512 devices in a mesh: kv: 64 (over z, y), tp: 8 (over x, core).
Axes of the slice: x: 4, y: 4, z: 16, core: 2. Of those that a mesh axis runs over, the one named last changes fastest.
Arguments:
- tokens: bfloat16 [16384, 2048], P('kv'), may hold values from -72 to 72
- w_query: bfloat16 [2048, 1024], P(None, 'tp'), may hold values from -0.125 to 0.125
- w_key: bfloat16 [2048, 1024], P(None, 'tp'), may hold values from -0.125 to 0.125
- w_value: bfloat16 [2048, 1024], P(None, 'tp'), may hold values from -0.125 to 0.125
- w_out: bfloat16 [1024, 2048], P('tp'), may hold values from -0.1875 to 0.1875
- chosen: int32 [256, 16], replicated, may hold values from -1 to 255, as said below
Outputs:
- mixed: bfloat16 [16384, 2048], P(('kv', 'tp'))
- log_sums: float32 [16, 16384], P('tp', 'kv')
The draws below stay inside these ranges and needn't reach their ends.
Inputs may be any that keep to these rules, and one draw needn't show every extreme that they name: `chosen`: row b begins with b itself, then lists distinct key blocks at most b, then holds -1 in its remaining entries. Taken together, the rows of the query blocks of one index of kv list at most 2 distinct blocks of the positions of any other index of kv, and exactly 2 for some pairs of indices in every draw.
All inputs are finite; a program needn't handle non-finite values.
Results may differ from the reference program's by a relative error of at most 0.03.
Values may be sent and summed in bfloat16 or wider, within the bound.
A program may use at most 64 MiB of HBM per device.

```python
import jax
import jax.numpy as jnp
from jax import lax

D = 2048
HEADS = 16
HEAD_DIM = 64
BLK = 64
SEL = 16
CAP = 2
TOK_DEV = 256
ATT = 1024
TOKENS = 16384
NBLK = 256
N_TP = 8


def draw_tokens(key, part):
    values = jnp.clip(jax.random.normal(key, (TOKENS, D), jnp.float32), -6.0, 6.0)
    return values.astype(jnp.bfloat16)


def draw_chosen(key, part):
    per_dev = TOK_DEV // BLK
    devices = NBLK // per_dev
    pair_key = jax.random.fold_in(key, 11)
    hot_key = jax.random.fold_in(key, 12)
    rank_key = jax.random.fold_in(key, 13)
    order_bits = jax.random.randint(pair_key, (devices, devices, per_dev), 0, 1 << 20) * per_dev + jnp.arange(per_dev)
    ordering = jnp.argsort(order_bits, axis=-1)[..., :CAP]
    picked_blocks = jnp.arange(devices)[None, :, None] * per_dev + ordering
    hotness = jax.random.randint(hot_key, (devices,), 0, 4)
    blocks = jnp.arange(NBLK)
    query_block = blocks[:, None]
    target = blocks[None, :]
    query_dev = query_block // per_dev
    target_dev = target // per_dev
    pair_table = jnp.any(picked_blocks[:, blocks // per_dev, :] == blocks[None, :, None], axis=-1)
    in_pair = pair_table[blocks // per_dev] & (target_dev < query_dev)
    same_dev = (target_dev == query_dev) & (target <= query_block)
    near_dev = (target_dev == query_dev - 1) | (target_dev == query_dev - devices // 2)
    tier_level = jnp.where(target == query_block, 3, jnp.where(same_dev | in_pair & near_dev, 2, 1))
    jitter = jax.random.randint(rank_key, (NBLK, NBLK), 0, 1 << 12)
    rating = ((tier_level * 4 + hotness[target_dev]) * 4096 + jitter) * NBLK + target
    rating = jnp.where(same_dev | in_pair, rating, -1 - target)
    values, position = lax.top_k(rating, SEL)
    return jnp.where(values >= 0, position, -1).astype(jnp.int32)


def level_of(stream_key, extent, split, smallest, high):
    gain = 1.0
    for dim, blocks in split:
        steps = jax.random.uniform(jax.random.fold_in(jax.random.fold_in(stream_key, 6), dim), (blocks,), jnp.float32, smallest / len(split), high / len(split))
        gain = gain * jnp.repeat(jnp.exp(steps), extent[dim] // blocks).reshape((-1,) + (1,) * (len(extent) - 1 - dim))
    return gain


def normal_values(stream_key, shape, deviation, reach, cuts=(), held_as=jnp.bfloat16):
    result = deviation * jax.random.normal(stream_key, shape, jnp.float32)
    if cuts:
        result = result * level_of(stream_key, shape, cuts, -0.22, 0.18)
    return jnp.clip(result, -reach, reach).astype(held_as)


def setup_inputs(seed: int = 0) -> dict:
    keys = jax.random.split(jax.random.key(seed), 7)
    tokens = draw_tokens(jax.random.fold_in(keys[6], 71), 0)
    w_query = normal_values(keys[1], (D, ATT), D ** -0.5, 0.125, ((1, 8),))
    w_key = normal_values(keys[2], (D, ATT), D ** -0.5, 0.125, ((1, 8),))
    w_value = normal_values(keys[3], (D, ATT), D ** -0.5, 0.125, ((1, 8),))
    w_out = normal_values(keys[4], (ATT, D), ATT ** -0.5, 0.1875, ((0, 8),))
    chosen = draw_chosen(jax.random.fold_in(keys[6], 71), 0)
    return dict(tokens=tokens, w_query=w_query, w_key=w_key, w_value=w_value, w_out=w_out, chosen=chosen)


rotary_base = 500000.0
masked_score = -1e30


def rotate(values, positions, head_count, head_size):
    half_size = head_size // 2
    inverse = rotary_base ** (-jnp.arange(half_size, dtype=jnp.float32) / half_size)
    angles = positions.astype(jnp.float32)[:, None, None] * inverse[None, None, :]
    cos_part = jnp.cos(angles)
    sin_part = jnp.sin(angles)
    grouped = values.reshape(values.shape[0], head_count, head_size)
    first_half = grouped[..., :half_size]
    second_half = grouped[..., half_size:]
    turned = jnp.concatenate([first_half * cos_part - second_half * sin_part, second_half * cos_part + first_half * sin_part], axis=-1)
    return turned.reshape(values.shape)


def reference(tokens, w_query, w_key, w_value, w_out, chosen):
    positions = jnp.arange(TOKENS)
    query = rotate(jnp.dot(tokens, w_query, preferred_element_type=jnp.float32), positions, HEADS, HEAD_DIM).astype(jnp.bfloat16)
    keys_all = rotate(jnp.dot(tokens, w_key, preferred_element_type=jnp.float32), positions, HEADS, HEAD_DIM).astype(jnp.bfloat16)
    values_all = jnp.dot(tokens, w_value, preferred_element_type=jnp.float32).astype(jnp.bfloat16)
    key_blocks = keys_all.reshape(NBLK, BLK, HEADS, HEAD_DIM)
    value_blocks = values_all.reshape(NBLK, BLK, HEADS, HEAD_DIM)
    query_blocks = query.reshape(NBLK, BLK, HEADS, HEAD_DIM)
    scaling = HEAD_DIM ** -0.5

    def one_block(inputs):
        query_rows, listed = inputs
        usable = listed >= 0
        safe_rows = jnp.maximum(listed, 0)
        picked_keys = key_blocks[safe_rows].reshape(SEL * BLK, HEADS, HEAD_DIM)
        picked_values = value_blocks[safe_rows].reshape(SEL * BLK, HEADS, HEAD_DIM)
        scores = jnp.einsum('qhd,khd->hqk', query_rows.astype(jnp.float32), picked_keys.astype(jnp.float32)) * scaling
        key_mask = jnp.broadcast_to(usable[:, None], (SEL, BLK)).reshape(SEL * BLK)
        scores = jnp.where(key_mask[None, None, :], scores, masked_score)
        row_max = jnp.max(scores, axis=-1)
        weights = jnp.where(key_mask[None, None, :], jnp.exp(scores - row_max[..., None]), 0.0)
        totals = jnp.sum(weights, axis=-1)
        rounded = lax.optimization_barrier(weights.astype(jnp.bfloat16)).astype(jnp.float32)
        summed = jnp.einsum('hqk,khd->qhd', rounded, picked_values.astype(jnp.float32))
        mixed_rows = (summed / jnp.transpose(totals)[:, :, None]).reshape(BLK, HEADS * HEAD_DIM).astype(jnp.bfloat16)
        return mixed_rows, row_max + jnp.log(totals)

    mixed_all, log_blocks = lax.map(one_block, (query_blocks, chosen))
    attended = mixed_all.reshape(TOKENS, HEADS * HEAD_DIM)
    log_sums = jnp.transpose(log_blocks, (1, 0, 2)).reshape(HEADS, TOKENS)
    group_width = HEADS * HEAD_DIM // N_TP
    output = jnp.zeros((TOKENS, D), jnp.float32)
    for group_index in range(N_TP):
        lower = group_index * group_width
        partial_sum = jnp.dot(attended[:, lower:lower + group_width], w_out[lower:lower + group_width], preferred_element_type=jnp.float32)
        output = output + lax.optimization_barrier(partial_sum.astype(jnp.bfloat16)).astype(jnp.float32)
    return output.astype(jnp.bfloat16), log_sums
```

```python
import functools

import jax
import jax.numpy as jnp
from jax import lax
from jax.experimental import pallas as pl
from jax.experimental.pallas import tpu as pltpu
from jax.sharding import PartitionSpec as P

HEAD_DIM = 64
BLK = 64
SEL = 16
NY = 4
ROTARY_BASE = 500000.0
MASKED = -1e30
MESH = pl.DeviceIdType.MESH


def rotary_tables(positions, width):
    half = HEAD_DIM // 2
    lane = jnp.arange(width)
    inverse = ROTARY_BASE ** (-(lane % half).astype(jnp.float32) / half)
    angles = positions.astype(jnp.float32)[:, None] * inverse[None, :]
    sign = jnp.where(lane % HEAD_DIM < half, -1.0, 1.0)
    return jnp.cos(angles), jnp.sin(angles) * sign[None, :]


def turn(values, cos_part, sin_part):
    width = values.shape[1]
    half = HEAD_DIM // 2
    lane = lax.broadcasted_iota(jnp.int32, values.shape, 1)
    ahead = pltpu.roll(values, width - half, 1)
    behind = pltpu.roll(values, half, 1)
    partner = jnp.where(lane % HEAD_DIM < half, ahead, behind)
    return values * cos_part + partner * sin_part


def project(tokens_ref, wq_ref, wk_ref, wv_ref, cos_ref, sin_ref, kv_ref, q_ref):
    blocks = kv_ref.shape[0]
    width = wk_ref.shape[1]
    cos_part, sin_part = cos_ref[...], sin_ref[...]
    tokens = tokens_ref[...]
    keys = jnp.dot(tokens, wk_ref[...], preferred_element_type=jnp.float32)
    keys = turn(keys, cos_part, sin_part).astype(jnp.bfloat16)
    kv_ref[:, :, :width] = keys.reshape(blocks, BLK, width)
    values = jnp.dot(tokens, wv_ref[...], preferred_element_type=jnp.float32).astype(jnp.bfloat16)
    kv_ref[:, :, width:] = values.reshape(blocks, BLK, width)
    query = jnp.dot(tokens, wq_ref[...], preferred_element_type=jnp.float32)
    query = turn(query, cos_part, sin_part).astype(jnp.bfloat16).astype(jnp.float32)
    query = query * HEAD_DIM ** (-0.5)
    lane = lax.broadcasted_iota(jnp.int32, query.shape, 1)
    for head in range(width // HEAD_DIM):
        mine = jnp.where(lane // HEAD_DIM == head, query, 0.0).astype(jnp.bfloat16)
        q_ref[:, head * BLK : (head + 1) * BLK, :] = mine.reshape(blocks, BLK, width)


def attend(
    nz,
    ntp,
    kv_ref,
    q_ref,
    w_ref,
    bias_ref,
    sel_ref,
    idx_ref,
    out_ref,
    lse_ref,
    pool,
    to_right,
    to_left,
    picked,
    wall,
    att,
    abuf,
    up_send,
    up_recv,
    dn_send,
    dn_recv,
    rs_send,
    rs_recv,
    ls_send,
    ls_recv,
    rf_send,
    rf_recv,
    lf_send,
    lf_recv,
    w_send,
    w_recv,
    a_send,
    a_recv,
):
    kv = lax.axis_index("kv")
    tp = lax.axis_index("tp")
    z, y = kv // NY, kv % NY
    nx = ntp // 2
    x, core = tp // 2, tp % 2
    up = ((z + 1) % nz) * NY + y
    down = ((z + nz - 1) % nz) * NY + y
    right = z * NY + (y + 1) % NY
    left = z * NY + (y + NY - 1) % NY
    x_right = ((x + 1) % nx) * 2 + core
    x_left = ((x + nx - 1) % nx) * 2 + core
    partner = x * 2 + (1 - core)
    blocks = kv_ref.shape[0]
    width = w_ref.shape[0]
    left_base = nz * blocks
    right_base = left_base + 3 * nz
    far0_base = right_base + 3 * nz
    far1_base = far0_base + nz
    rows = att.shape[0] // ntp

    barrier = pltpu.get_barrier_semaphore()
    for peer in (up, down, right, left):
        pl.semaphore_signal(barrier, inc=1, device_id=(peer, tp), device_id_type=MESH)
    for step in range(1, ntp):
        pl.semaphore_signal(
            barrier, inc=1, device_id=(kv, (tp + step) % ntp), device_id_type=MESH
        )
    pl.semaphore_wait(barrier, 4 + ntp - 1)

    def remote(src, dst, send, recv, device):
        return pltpu.make_async_remote_copy(
            src_ref=src,
            dst_ref=dst,
            send_sem=send,
            recv_sem=recv,
            device_id=device,
            device_id_type=MESH,
        )

    ups = (nz - 1 + 1) // 2
    downs = nz - 1 - ups

    def plane(p):
        return pool.at[pl.ds(p * blocks, blocks)]

    def up_copy(step):
        p = (z + nz - step) % nz
        src = kv_ref if step == 0 else plane(p)
        return remote(src, plane(p), up_send.at[step], up_recv.at[step], (up, tp))

    def down_copy(step):
        p = (z + step) % nz
        src = kv_ref if step == 0 else plane(p)
        return remote(src, plane(p), dn_send.at[step], dn_recv.at[step], (down, tp))

    def right_copy(p):
        dst = pool.at[pl.ds(left_base + 3 * p, 3)]
        return remote(to_right.at[p], dst, rs_send.at[p], rs_recv.at[p], (right, tp))

    def left_copy(p):
        dst = pool.at[pl.ds(right_base + 3 * p, 3)]
        return remote(to_left.at[p], dst, ls_send.at[p], ls_recv.at[p], (left, tp))

    def right_relay(p):
        src = pool.at[left_base + 3 * p + 2]
        return remote(src, pool.at[far0_base + p], rf_send.at[p], rf_recv.at[p], (right, tp))

    def left_relay(p):
        src = pool.at[right_base + 3 * p + 2]
        return remote(src, pool.at[far1_base + p], lf_send.at[p], lf_recv.at[p], (left, tp))

    def exchange(p):
        here = [pool[p * blocks + b] for b in range(blocks)]

        def pick(ahead, c):
            which = sel_ref[(p * 3 + ahead - 1) * 2 + c]
            found = here[blocks - 1]
            for b in range(blocks - 1):
                found = jnp.where(which == b, here[b], found)
            return found

        to_right[p, 0] = pick(1, 0)
        to_right[p, 1] = pick(1, 1)
        to_right[p, 2] = pick(2, 0)
        right_copy(p).start()
        to_left[p, 0] = pick(3, 0)
        to_left[p, 1] = pick(3, 1)
        to_left[p, 2] = pick(2, 1)
        left_copy(p).start()

    def relay(p):
        right_copy(p).wait_recv()
        right_relay(p).start()
        left_copy(p).wait_recv()
        left_relay(p).start()

    def settle(p):
        right_relay(p).wait()
        left_relay(p).wait()
        right_copy(p).wait_send()
        left_copy(p).wait_send()

    half = width // 2

    def w_ring(side):
        src = w_ref
        peer = x_right if side == 0 else x_left
        return remote(src, wall.at[tp], w_send.at[side], w_recv.at[side], (kv, peer))

    def w_half(side):
        origin = x_left if side == 0 else x_right
        peer = x_right if side == 0 else x_left
        part = wall.at[origin, pl.ds(side * half, half)]
        return remote(part, part, w_send.at[2 + side], w_recv.at[2 + side], (kv, peer))

    def w_pair(which):
        far = ((x + 2) % nx) * 2 + core
        owner = (tp, x_left, x_right, far)[which]
        src = w_ref if which == 0 else wall.at[owner]
        return remote(src, wall.at[owner], w_send.at[4 + which], w_recv.at[4 + which], (kv, partner))

    up_copy(0).start()
    down_copy(0).start()
    w_ring(0).start()
    w_ring(1).start()
    w_pair(0).start()
    pool[pl.ds(z * blocks, blocks)] = kv_ref[...]
    wall[tp] = w_ref[...]
    exchange(z)

    order = [[(z, None)]]
    for step in range(ups):
        up_copy(step).wait_recv()
        if step + 1 < ups:
            up_copy(step + 1).start()
        if step < downs:
            down_copy(step).wait_recv()
            if step + 1 < downs:
                down_copy(step + 1).start()
        now = []
        above = z - 1 - step
        now.append((above, above >= 0))
        if step < downs:
            below = z + 1 + step - nz
            now.append((below, below >= 0))
        for p, there in now:
            pl.when(there)(functools.partial(exchange, p))
        order.append(now)
        if step == 3 or step == ups - 2 and ups < 5:
            w_ring(0).wait_recv()
            w_half(0).start()
            w_pair(1).start()
            w_ring(1).wait_recv()
            w_half(1).start()
            w_pair(2).start()
        if step == 5 or step == ups - 1 and ups < 6:
            w_half(0).wait_recv()
            w_half(1).wait_recv()
            w_pair(3).start()
        if step >= 1:
            for p, there in order[step - 1]:
                if there is None:
                    relay(p)
                else:
                    pl.when(there)(functools.partial(relay, p))
    for now in order[ups - 1 :]:
        for p, there in now:
            if there is None:
                relay(p)
            else:
                pl.when(there)(functools.partial(relay, p))
    for step in range(ups):
        up_copy(step).wait_send()
    for step in range(downs):
        down_copy(step).wait_send()
    for side in range(2):
        w_ring(side).wait_send()
        w_half(side).wait_send()
    for which in range(4):
        w_pair(which).wait()
    for now in order:
        for p, there in now:
            if there is None:
                settle(p)
            else:
                pl.when(there)(functools.partial(settle, p))

    def part_copy(to):
        src = att.at[pl.ds(to * rows, rows)]
        dst = abuf.at[:, pl.ds(pl.multiple_of(tp * width, width), width)]
        return remote(src, dst, a_send.at[to], a_recv.at[tp], (kv, to))

    def part_arrival(source):
        src = att.at[pl.ds(0, rows)]
        dst = abuf.at[:, pl.ds(source * width, width)]
        return remote(src, dst, a_send.at[source], a_recv.at[source], (kv, source))

    heads = width // HEAD_DIM
    per_block = ntp // blocks
    lane = lax.broadcasted_iota(jnp.int32, (BLK, width), 1)
    row_id = lax.broadcasted_iota(jnp.int32, (heads * BLK, heads * BLK), 0)
    col_id = lax.broadcasted_iota(jnp.int32, (heads * BLK, heads * BLK), 1)
    logs = []
    for i in range(blocks):
        for j in range(SEL):
            picked[j * BLK : (j + 1) * BLK, :] = pool[idx_ref[i * SEL + j]]
        scores = lax.dot_general(
            q_ref[i],
            picked[:, :width],
            (((1,), (1,)), ((), ())),
            preferred_element_type=jnp.float32,
        )
        scores = scores + bias_ref[i : i + 1, :]
        top = jnp.max(scores, axis=1, keepdims=True)
        weights = jnp.exp(scores - top)
        total = jnp.sum(weights, axis=1, keepdims=True)
        summed = jnp.dot(
            weights.astype(jnp.bfloat16), picked[:, width:], preferred_element_type=jnp.float32
        )
        summed = summed / total
        mixed = summed[:BLK]
        for head in range(1, heads):
            mixed = jnp.where(
                lane // HEAD_DIM == head, summed[head * BLK : (head + 1) * BLK], mixed
            )
        att[i * BLK : (i + 1) * BLK, :] = mixed.astype(jnp.bfloat16)
        for to in range(i * per_block, (i + 1) * per_block):
            @pl.when(to != tp)
            def _():
                part_copy(to).start()

            @pl.when(to == tp)
            def _():
                abuf[:, pl.ds(pl.multiple_of(tp * width, width), width)] = att[
                    to * rows : (to + 1) * rows, :
                ]
        column = top + jnp.log(total)
        logs.append(jnp.sum(jnp.where(row_id == col_id, column, 0.0), axis=0, keepdims=True))
    for head in range(heads):
        lse_ref[head : head + 1, :] = jnp.concatenate(
            [row[:, head * BLK : (head + 1) * BLK] for row in logs], axis=1
        )
    for other in range(ntp):
        @pl.when(other != tp)
        def _():
            part_arrival(other).wait_recv()
            part_copy(other).wait_send()
    total_width = out_ref.shape[1]
    chunk = min(512, total_width)
    for c in range(total_width // chunk):
        cols = slice(c * chunk, (c + 1) * chunk)
        acc = jnp.zeros((rows, chunk), jnp.float32)
        for t in range(ntp):
            acc += jnp.dot(
                abuf[:, t * width : (t + 1) * width],
                wall[t, :, cols],
                preferred_element_type=jnp.float32,
            )
        out_ref[:, cols] = acc.astype(jnp.bfloat16)


def local(nkv, ntp, tokens, w_query, w_key, w_value, w_out, chosen):
    local_rows = tokens.shape[0]
    width = w_query.shape[1]
    heads = width // HEAD_DIM
    blocks = local_rows // BLK
    nz = nkv // NY
    device = lax.axis_index("kv")
    z, y = device // NY, device % NY
    vmem = pl.BlockSpec(memory_space=pltpu.VMEM)
    smem = pl.BlockSpec(memory_space=pltpu.SMEM)
    positions = device * local_rows + jnp.arange(local_rows)
    cos_part, sin_part = rotary_tables(positions, width)
    kv_here, query = pl.pallas_call(
        project,
        out_shape=(
            jax.ShapeDtypeStruct((blocks, BLK, 2 * width), jnp.bfloat16),
            jax.ShapeDtypeStruct((blocks, heads * BLK, width), jnp.bfloat16),
        ),
        in_specs=[vmem] * 6,
        out_specs=(vmem, vmem),
        compiler_params=pltpu.CompilerParams(vmem_limit_bytes=24 * 1024 * 1024),
    )(tokens, w_query, w_key, w_value, cos_part, sin_part)

    plane_lists = lax.dynamic_slice_in_dim(chosen, z * NY * blocks, NY * blocks, 0)
    plane_lists = plane_lists.reshape(NY, blocks * SEL)
    every = jnp.arange(chosen.shape[0])
    wanted = jnp.any(plane_lists[:, :, None] == every[None, None, :], axis=1)
    wanted = wanted.reshape(NY, nz, NY, blocks)
    order = jnp.arange(blocks)
    lowest = jnp.min(jnp.where(wanted, order, blocks - 1), axis=-1)
    highest = jnp.max(jnp.where(wanted, order, 0), axis=-1)
    table = jnp.stack([lowest, highest], axis=-1)
    dest = (y + 1 + jnp.arange(NY - 1)) % NY
    sent = jnp.take(jnp.take(table, y, axis=2), dest, axis=0)
    sel = jnp.transpose(sent, (1, 0, 2)).reshape(-1)

    own_lists = lax.dynamic_slice_in_dim(chosen, device * blocks, blocks, 0)
    usable = own_lists >= 0
    entry = jnp.where(usable, own_lists, device * blocks)
    source = entry // blocks
    from_z, from_y, block = source // NY, source % NY, entry % blocks
    low_mine = jnp.take(lowest, y, axis=0)
    second = (block != low_mine[from_z, from_y]).astype(jnp.int32)
    ahead = (from_y - y) % NY
    left_base = nz * blocks
    right_base = left_base + 3 * nz
    far_base = right_base + 3 * nz
    place = jnp.where(
        ahead == 0,
        from_z * blocks + block,
        jnp.where(
            ahead == NY - 1,
            left_base + 3 * from_z + second,
            jnp.where(ahead == 1, right_base + 3 * from_z + second, far_base + second * nz + from_z),
        ),
    )
    idx = place.reshape(-1).astype(jnp.int32)
    bias = jnp.where(usable, 0.0, MASKED)
    bias = jnp.broadcast_to(bias[:, :, None], (blocks, SEL, BLK)).reshape(blocks, SEL * BLK)

    ups = nz // 2
    out_rows = local_rows // ntp
    dma = pltpu.SemaphoreType.DMA
    pool_size = far_base + 2 * nz
    return pl.pallas_call(
        functools.partial(attend, nz, ntp),
        out_shape=(
            jax.ShapeDtypeStruct((out_rows, w_out.shape[1]), jnp.bfloat16),
            jax.ShapeDtypeStruct((heads, local_rows), jnp.float32),
        ),
        in_specs=[vmem] * 4 + [smem] * 2,
        out_specs=(vmem, vmem),
        scratch_shapes=[
            pltpu.VMEM((pool_size, BLK, 2 * width), jnp.bfloat16),
            pltpu.VMEM((nz, 3, BLK, 2 * width), jnp.bfloat16),
            pltpu.VMEM((nz, 3, BLK, 2 * width), jnp.bfloat16),
            pltpu.VMEM((SEL * BLK, 2 * width), jnp.bfloat16),
            pltpu.VMEM((ntp, width, w_out.shape[1]), jnp.bfloat16),
            pltpu.VMEM((local_rows, width), jnp.bfloat16),
            pltpu.VMEM((out_rows, ntp * width), jnp.bfloat16),
            dma((ups,)),
            dma((ups,)),
            dma((ups,)),
            dma((ups,)),
        ]
        + [dma((nz,))] * 8
        + [dma((8,))] * 2
        + [dma((ntp,))] * 2,
        compiler_params=pltpu.CompilerParams(
            collective_id=0, has_side_effects=True, vmem_limit_bytes=48 * 1024 * 1024
        ),
    )(kv_here, query, w_out, bias, sel, idx)


def solution(mesh):
    placed = (P("kv", None), P(None, "tp"), P(None, "tp"), P(None, "tp"), P("tp", None), P())
    return jax.shard_map(
        functools.partial(local, mesh.shape["kv"], mesh.shape["tp"]),
        mesh=mesh,
        in_specs=placed,
        out_specs=(P(("kv", "tp"), None), P("tp", "kv")),
        check_vma=False,
    )
```

```python
import functools

import jax
import jax.numpy as jnp
from jax import lax
from jax.experimental import pallas as pl
from jax.experimental.pallas import tpu as pltpu
from jax.sharding import PartitionSpec as P

HEAD_DIM = 64
BLK = 64
SEL = 16
NY = 4
ROTARY_BASE = 500000.0
MASKED = -1e30
MESH = pl.DeviceIdType.MESH


def rotary_tables(positions, width):
    half = HEAD_DIM // 2
    lane = jnp.arange(width)
    inverse = ROTARY_BASE ** (-(lane % half).astype(jnp.float32) / half)
    angles = positions.astype(jnp.float32)[:, None] * inverse[None, :]
    sign = jnp.where(lane % HEAD_DIM < half, -1.0, 1.0)
    return jnp.cos(angles), jnp.sin(angles) * sign[None, :]


def turn(values, cos_part, sin_part):
    width = values.shape[1]
    half = HEAD_DIM // 2
    lane = lax.broadcasted_iota(jnp.int32, values.shape, 1)
    ahead = pltpu.roll(values, width - half, 1)
    behind = pltpu.roll(values, half, 1)
    partner = jnp.where(lane % HEAD_DIM < half, ahead, behind)
    return values * cos_part + partner * sin_part


def make_tables(nz, blocks, kv, chosen_ref, table):
    z, y = kv // NY, kv % NY
    row = lax.broadcasted_iota(jnp.int32, table.shape[1:], 0)
    lane = lax.broadcasted_iota(jnp.int32, table.shape[1:], 1)
    found = jnp.zeros(table.shape[1:], jnp.int32)
    target = lax.broadcasted_iota(jnp.int32, (nz, SEL), 0) * (NY * blocks) + y * blocks
    for ahead in range(1, NY):
        dest = z * NY + (y + ahead) % NY
        rows = [chosen_ref[pl.ds(dest * blocks + r, 1), :] for r in range(blocks)]
        low = jnp.full((nz, 1), blocks - 1, jnp.int32)
        high = jnp.zeros((nz, 1), jnp.int32)
        hits = []
        for b in range(blocks):
            hit = jnp.zeros((nz, SEL), jnp.int32)
            for entries in rows:
                hit = jnp.where(entries == target + b, 1, hit)
            hits.append(jnp.max(hit, axis=1, keepdims=True))
        for b in range(blocks):
            high = jnp.where(hits[b] > 0, b, high)
            low = jnp.where(hits[blocks - 1 - b] > 0, blocks - 1 - b, low)
        found = jnp.where(lane == (ahead - 1) * 2, low, found)
        found = jnp.where(lane == (ahead - 1) * 2 + 1, high, found)
    table[0] = found
    size = blocks * SEL
    mine = jnp.concatenate(
        [chosen_ref[pl.ds(kv * blocks + r, 1), :] for r in range(blocks)], axis=1
    )
    mine = jnp.where(mine >= 0, mine, kv * blocks)
    across = jnp.broadcast_to(mine, (size, size))
    diagonal = lax.broadcasted_iota(jnp.int32, (size, size), 0) == lax.broadcasted_iota(
        jnp.int32, (size, size), 1
    )
    down = jnp.sum(jnp.where(diagonal, across, 0), axis=1, keepdims=True)
    lower = (down // blocks == across // blocks) & (down < across)
    second = jnp.max(jnp.where(lower, 1, 0), axis=0, keepdims=True)
    source = mine // blocks
    from_z, ahead = source // NY, (source % NY - y + NY) % NY
    left_base = nz * blocks
    right_base = left_base + 3 * nz
    far_base = right_base + 3 * nz
    place = jnp.where(
        ahead == 0,
        mine % blocks + from_z * blocks,
        jnp.where(
            ahead == NY - 1,
            left_base + 3 * from_z + second,
            jnp.where(ahead == 1, right_base + 3 * from_z + second, far_base + second * nz + from_z),
        ),
    )
    full = jnp.concatenate([place, jnp.zeros((1, table.shape[2] - size), jnp.int32)], axis=1)
    table[1] = jnp.broadcast_to(full, table.shape[1:])


def attend(
    nz,
    ntp,
    tokens_hbm,
    wq_hbm,
    wk_hbm,
    wv_hbm,
    w_hbm,
    chosen_ref,
    cos_ref,
    sin_ref,
    out_ref,
    lse_ref,
    tokens_ref,
    wq_ref,
    wk_ref,
    wv_ref,
    q_ref,
    table,
    sel_ref,
    idx_ref,
    local_sem,
    pool,
    to_right,
    to_left,
    picked,
    wall,
    att,
    abuf,
    up_send,
    up_recv,
    dn_send,
    dn_recv,
    rs_send,
    rs_recv,
    ls_send,
    ls_recv,
    rf_send,
    rf_recv,
    lf_send,
    lf_recv,
    w_send,
    w_recv,
    a_send,
    a_recv,
):
    kv = lax.axis_index("kv")
    tp = lax.axis_index("tp")
    z, y = kv // NY, kv % NY
    nx = ntp // 2
    x, core = tp // 2, tp % 2
    up = ((z + 1) % nz) * NY + y
    down = ((z + nz - 1) % nz) * NY + y
    right = z * NY + (y + 1) % NY
    left = z * NY + (y + NY - 1) % NY
    x_right = ((x + 1) % nx) * 2 + core
    x_left = ((x + nx - 1) % nx) * 2 + core
    partner = x * 2 + (1 - core)
    width = wk_ref.shape[1]
    blocks = att.shape[0] // BLK
    heads = width // HEAD_DIM
    left_base = nz * blocks
    right_base = left_base + 3 * nz
    far0_base = right_base + 3 * nz
    far1_base = far0_base + nz
    rows = att.shape[0] // ntp

    def load(which, src, dst):
        return pltpu.make_async_copy(src, dst, local_sem.at[which])

    loads = [
        load(0, tokens_hbm, tokens_ref),
        load(1, wk_hbm, wk_ref),
        load(2, wv_hbm, wv_ref),
        load(3, w_hbm, wall.at[tp]),
        load(4, wq_hbm, wq_ref),
    ]
    for copy in loads:
        copy.start()

    barrier = pltpu.get_barrier_semaphore()
    for peer in (up, down, right, left):
        pl.semaphore_signal(barrier, inc=1, device_id=(peer, tp), device_id_type=MESH)
    for step in range(1, ntp):
        pl.semaphore_signal(
            barrier, inc=1, device_id=(kv, (tp + step) % ntp), device_id_type=MESH
        )
    make_tables(nz, blocks, kv, chosen_ref, table)
    to_smem = [load(5, table.at[0], sel_ref), load(6, table.at[1, pl.ds(0, 8)], idx_ref)]
    for copy in to_smem:
        copy.start()
    pl.semaphore_wait(barrier, 4 + ntp - 1)

    def remote(src, dst, send, recv, device):
        return pltpu.make_async_remote_copy(
            src_ref=src,
            dst_ref=dst,
            send_sem=send,
            recv_sem=recv,
            device_id=device,
            device_id_type=MESH,
        )

    ups = (nz - 1 + 1) // 2
    downs = nz - 1 - ups

    def up_copy(step, b):
        at = pool.at[(z + nz - step) % nz * blocks + b]
        sem = step * blocks + b
        return remote(at, at, up_send.at[sem], up_recv.at[sem], (up, tp))

    def down_copy(step, b):
        at = pool.at[(z + step) % nz * blocks + b]
        sem = step * blocks + b
        return remote(at, at, dn_send.at[sem], dn_recv.at[sem], (down, tp))

    def right_copy(p):
        dst = pool.at[pl.ds(left_base + 3 * p, 3)]
        return remote(to_right.at[p], dst, rs_send.at[p], rs_recv.at[p], (right, tp))

    def left_copy(p):
        dst = pool.at[pl.ds(right_base + 3 * p, 3)]
        return remote(to_left.at[p], dst, ls_send.at[p], ls_recv.at[p], (left, tp))

    def right_relay(p):
        src = pool.at[left_base + 3 * p + 2]
        return remote(src, pool.at[far0_base + p], rf_send.at[p], rf_recv.at[p], (right, tp))

    def left_relay(p):
        src = pool.at[right_base + 3 * p + 2]
        return remote(src, pool.at[far1_base + p], lf_send.at[p], lf_recv.at[p], (left, tp))

    def exchange(p):
        here = [pool[p * blocks + b] for b in range(blocks)]

        def pick(ahead, c):
            which = sel_ref[p, (ahead - 1) * 2 + c]
            found = here[blocks - 1]
            for b in range(blocks - 1):
                found = jnp.where(which == b, here[b], found)
            return found

        to_right[p, 0] = pick(1, 0)
        to_right[p, 1] = pick(1, 1)
        to_right[p, 2] = pick(2, 0)
        right_copy(p).start()
        to_left[p, 0] = pick(3, 0)
        to_left[p, 1] = pick(3, 1)
        to_left[p, 2] = pick(2, 1)
        left_copy(p).start()

    def relay(p):
        right_copy(p).wait_recv()
        right_relay(p).start()
        left_copy(p).wait_recv()
        left_relay(p).start()

    def settle(p):
        right_relay(p).wait()
        left_relay(p).wait()
        right_copy(p).wait_send()
        left_copy(p).wait_send()

    half = width // 2

    def w_ring(side):
        peer = x_right if side == 0 else x_left
        return remote(wall.at[tp], wall.at[tp], w_send.at[side], w_recv.at[side], (kv, peer))

    def w_half(side):
        origin = x_left if side == 0 else x_right
        peer = x_right if side == 0 else x_left
        part = wall.at[origin, pl.ds(side * half, half)]
        return remote(part, part, w_send.at[2 + side], w_recv.at[2 + side], (kv, peer))

    def w_pair(which):
        far = ((x + 2) % nx) * 2 + core
        owner = (tp, x_left, x_right, far)[which]
        return remote(wall.at[owner], wall.at[owner], w_send.at[4 + which], w_recv.at[4 + which], (kv, partner))

    loads[0].wait()
    loads[1].wait()
    cos_part, sin_part = cos_ref[...], sin_ref[...]
    keys = jnp.dot(tokens_ref[...], wk_ref[...], preferred_element_type=jnp.float32)
    keys = turn(keys, cos_part, sin_part).astype(jnp.bfloat16)
    pool[pl.ds(z * blocks, blocks), :, :width] = keys.reshape(blocks, BLK, width)
    loads[2].wait()
    values = jnp.dot(tokens_ref[...], wv_ref[...], preferred_element_type=jnp.float32)
    values = values.astype(jnp.bfloat16)
    pool[pl.ds(z * blocks, blocks), :, width:] = values.reshape(blocks, BLK, width)
    for b in range(blocks):
        up_copy(0, b).start()
        down_copy(0, b).start()
    for copy in to_smem:
        copy.wait()
    exchange(z)
    loads[3].wait()
    w_ring(0).start()
    w_ring(1).start()
    w_pair(0).start()
    loads[4].wait()
    query = jnp.dot(tokens_ref[...], wq_ref[...], preferred_element_type=jnp.float32)
    query = turn(query, cos_part, sin_part).astype(jnp.bfloat16).astype(jnp.float32)
    query = query * HEAD_DIM ** (-0.5)
    channel = lax.broadcasted_iota(jnp.int32, query.shape, 1)
    for head in range(heads):
        mine = jnp.where(channel // HEAD_DIM == head, query, 0.0).astype(jnp.bfloat16)
        q_ref[:, head * BLK : (head + 1) * BLK, :] = mine.reshape(blocks, BLK, width)

    order = [[(z, None)]]
    for step in range(ups):
        for b in range(blocks):
            up_copy(step, b).wait_recv()
            if step + 1 < ups:
                up_copy(step + 1, b).start()
            if step < downs:
                down_copy(step, b).wait_recv()
                if step + 1 < downs:
                    down_copy(step + 1, b).start()
        now = []
        above = z - 1 - step
        now.append((above, above >= 0))
        if step < downs:
            below = z + 1 + step - nz
            now.append((below, below >= 0))
        for p, there in now:
            pl.when(there)(functools.partial(exchange, p))
        order.append(now)
        if step == 3 or step == ups - 2 and ups < 5:
            w_ring(0).wait_recv()
            w_half(0).start()
            w_pair(1).start()
            w_ring(1).wait_recv()
            w_half(1).start()
            w_pair(2).start()
        if step == 5 or step == ups - 1 and ups < 6:
            w_half(0).wait_recv()
            w_half(1).wait_recv()
            w_pair(3).start()
        if step >= 1:
            for p, there in order[step - 1]:
                if there is None:
                    relay(p)
                else:
                    pl.when(there)(functools.partial(relay, p))
    for now in order[ups - 1 :]:
        for p, there in now:
            if there is None:
                relay(p)
            else:
                pl.when(there)(functools.partial(relay, p))
    for b in range(blocks):
        for step in range(ups):
            up_copy(step, b).wait_send()
        for step in range(downs):
            down_copy(step, b).wait_send()
    for side in range(2):
        w_ring(side).wait_send()
        w_half(side).wait_send()
    for which in range(4):
        w_pair(which).wait()
    for now in order:
        for p, there in now:
            if there is None:
                settle(p)
            else:
                pl.when(there)(functools.partial(settle, p))

    def part_copy(to):
        src = att.at[pl.ds(to * rows, rows)]
        dst = abuf.at[:, pl.ds(pl.multiple_of(tp * width, width), width)]
        return remote(src, dst, a_send.at[to], a_recv.at[tp], (kv, to))

    def part_arrival(source):
        src = att.at[pl.ds(0, rows)]
        dst = abuf.at[:, pl.ds(source * width, width)]
        return remote(src, dst, a_send.at[source], a_recv.at[source], (kv, source))

    per_block = ntp // blocks
    lane = lax.broadcasted_iota(jnp.int32, (BLK, width), 1)
    row_id = lax.broadcasted_iota(jnp.int32, (heads * BLK, heads * BLK), 0)
    col_id = lax.broadcasted_iota(jnp.int32, (heads * BLK, heads * BLK), 1)
    key_id = lax.broadcasted_iota(jnp.int32, (1, SEL * BLK), 1)
    logs = []
    for i in range(blocks):
        for j in range(SEL):
            picked[j * BLK : (j + 1) * BLK, :] = pool[idx_ref[0, i * SEL + j]]
        scores = lax.dot_general(
            q_ref[i],
            picked[:, :width],
            (((1,), (1,)), ((), ())),
            preferred_element_type=jnp.float32,
        )
        listed = chosen_ref[pl.ds(kv * blocks + i, 1), :]
        count = jnp.sum((listed >= 0).astype(jnp.int32), axis=1, keepdims=True)
        scores = jnp.where(key_id < count * BLK, scores, MASKED)
        top = jnp.max(scores, axis=1, keepdims=True)
        weights = jnp.exp(scores - top)
        total = jnp.sum(weights, axis=1, keepdims=True)
        summed = jnp.dot(
            weights.astype(jnp.bfloat16), picked[:, width:], preferred_element_type=jnp.float32
        )
        summed = summed / total
        mixed = summed[:BLK]
        for head in range(1, heads):
            mixed = jnp.where(
                lane // HEAD_DIM == head, summed[head * BLK : (head + 1) * BLK], mixed
            )
        att[i * BLK : (i + 1) * BLK, :] = mixed.astype(jnp.bfloat16)
        for to in range(i * per_block, (i + 1) * per_block):
            @pl.when(to != tp)
            def _():
                part_copy(to).start()

            @pl.when(to == tp)
            def _():
                abuf[:, pl.ds(pl.multiple_of(tp * width, width), width)] = att[
                    to * rows : (to + 1) * rows, :
                ]
        column = top + jnp.log(total)
        logs.append(jnp.sum(jnp.where(row_id == col_id, column, 0.0), axis=0, keepdims=True))
    for head in range(heads):
        lse_ref[head : head + 1, :] = jnp.concatenate(
            [row[:, head * BLK : (head + 1) * BLK] for row in logs], axis=1
        )
    for other in range(ntp):
        @pl.when(other != tp)
        def _():
            part_arrival(other).wait_recv()
            part_copy(other).wait_send()
    total_width = out_ref.shape[1]
    chunk = min(512, total_width)
    for c in range(total_width // chunk):
        cols = slice(c * chunk, (c + 1) * chunk)
        acc = jnp.zeros((rows, chunk), jnp.float32)
        for t in range(ntp):
            acc += jnp.dot(
                abuf[:, t * width : (t + 1) * width],
                wall[t, :, cols],
                preferred_element_type=jnp.float32,
            )
        out_ref[:, cols] = acc.astype(jnp.bfloat16)


def local(nkv, ntp, tokens, w_query, w_key, w_value, w_out, chosen):
    local_rows = tokens.shape[0]
    width = w_query.shape[1]
    heads = width // HEAD_DIM
    blocks = local_rows // BLK
    nz = nkv // NY
    device = lax.axis_index("kv")
    vmem = pl.BlockSpec(memory_space=pltpu.VMEM)
    hbm = pl.BlockSpec(memory_space=pl.ANY)
    positions = device * local_rows + jnp.arange(local_rows)
    cos_part, sin_part = rotary_tables(positions, width)
    ups = nz // 2
    out_rows = local_rows // ntp
    dma = pltpu.SemaphoreType.DMA
    pool_size = nz * (blocks + 8)
    return pl.pallas_call(
        functools.partial(attend, nz, ntp),
        out_shape=(
            jax.ShapeDtypeStruct((out_rows, w_out.shape[1]), jnp.bfloat16),
            jax.ShapeDtypeStruct((heads, local_rows), jnp.float32),
        ),
        in_specs=[hbm] * 5 + [vmem] * 3,
        out_specs=(vmem, vmem),
        scratch_shapes=[
            pltpu.VMEM(tokens.shape, jnp.bfloat16),
            pltpu.VMEM(w_query.shape, jnp.bfloat16),
            pltpu.VMEM(w_key.shape, jnp.bfloat16),
            pltpu.VMEM(w_value.shape, jnp.bfloat16),
            pltpu.VMEM((blocks, heads * BLK, width), jnp.bfloat16),
            pltpu.VMEM((2, nz, 128), jnp.int32),
            pltpu.SMEM((nz, 128), jnp.int32),
            pltpu.SMEM((8, 128), jnp.int32),
            dma((7,)),
            pltpu.VMEM((pool_size, BLK, 2 * width), jnp.bfloat16),
            pltpu.VMEM((nz, 3, BLK, 2 * width), jnp.bfloat16),
            pltpu.VMEM((nz, 3, BLK, 2 * width), jnp.bfloat16),
            pltpu.VMEM((SEL * BLK, 2 * width), jnp.bfloat16),
            pltpu.VMEM((ntp, width, w_out.shape[1]), jnp.bfloat16),
            pltpu.VMEM((local_rows, width), jnp.bfloat16),
            pltpu.VMEM((out_rows, ntp * width), jnp.bfloat16),
        ]
        + [dma((ups * blocks,))] * 4
        + [dma((nz,))] * 8
        + [dma((8,))] * 2
        + [dma((ntp,))] * 2,
        compiler_params=pltpu.CompilerParams(
            collective_id=0, has_side_effects=True, vmem_limit_bytes=56 * 1024 * 1024
        ),
    )(tokens, w_query, w_key, w_value, w_out, chosen, cos_part, sin_part)


def solution(mesh):
    placed = (P("kv", None), P(None, "tp"), P(None, "tp"), P(None, "tp"), P("tp", None), P())
    return jax.shard_map(
        functools.partial(local, mesh.shape["kv"], mesh.shape["tp"]),
        mesh=mesh,
        in_specs=placed,
        out_specs=(P(("kv", "tp"), None), P("tp", "kv")),
        check_vma=False,
    )
```

```python
import functools

import jax
import jax.numpy as jnp
from jax import lax
from jax.experimental import pallas as pl
from jax.experimental.pallas import tpu as pltpu
from jax.sharding import PartitionSpec as P

HEAD_DIM = 64
BLK = 64
SEL = 16
NY = 4
ROTARY_BASE = 500000.0
MASKED = -1e30
MESH = pl.DeviceIdType.MESH


def rotary_pieces(first, width):
    half = HEAD_DIM // 2
    lane = jnp.arange(width)
    inverse = ROTARY_BASE ** (-(lane % half).astype(jnp.float32) / half)
    row = jnp.arange(40)
    position = jnp.where(row < 16, 16 * row, jnp.where(row < 32, row - 16, first))
    angles = position.astype(jnp.float32)[:, None] * inverse[None, :]
    return jnp.cos(angles), jnp.sin(angles)


def rotary_tables(cos_piece, sin_piece, cos_ref, sin_ref):
    half = HEAD_DIM // 2
    cos_first, sin_first = cos_piece[32:33, :], sin_piece[32:33, :]
    cos_tens, sin_tens = cos_piece[:16, :], sin_piece[:16, :]
    cos_ones, sin_ones = cos_piece[16:32, :], sin_piece[16:32, :]
    lane = lax.broadcasted_iota(jnp.int32, cos_ones.shape, 1)
    sign = jnp.where(lane % HEAD_DIM < half, -1.0, 1.0)
    cos_row = cos_first * cos_tens - sin_first * sin_tens
    sin_row = sin_first * cos_tens + cos_first * sin_tens
    for t in range(cos_ref.shape[0] // 16):
        c, n = cos_row[t : t + 1, :], sin_row[t : t + 1, :]
        cos_ref[t * 16 : (t + 1) * 16, :] = c * cos_ones - n * sin_ones
        sin_ref[t * 16 : (t + 1) * 16, :] = (n * cos_ones + c * sin_ones) * sign


def turn(values, cos_part, sin_part):
    width = values.shape[1]
    half = HEAD_DIM // 2
    lane = lax.broadcasted_iota(jnp.int32, values.shape, 1)
    ahead = pltpu.roll(values, width - half, 1)
    behind = pltpu.roll(values, half, 1)
    partner = jnp.where(lane % HEAD_DIM < half, ahead, behind)
    return values * cos_part + partner * sin_part


def make_tables(nz, blocks, kv, chosen_ref, table):
    z, y = kv // NY, kv % NY
    row = lax.broadcasted_iota(jnp.int32, table.shape[1:], 0)
    lane = lax.broadcasted_iota(jnp.int32, table.shape[1:], 1)
    found = jnp.zeros(table.shape[1:], jnp.int32)
    target = lax.broadcasted_iota(jnp.int32, (nz, SEL), 0) * (NY * blocks) + y * blocks
    for ahead in range(1, NY):
        dest = z * NY + (y + ahead) % NY
        rows = [chosen_ref[pl.ds(dest * blocks + r, 1), :] for r in range(blocks)]
        low = jnp.full((nz, 1), blocks - 1, jnp.int32)
        high = jnp.zeros((nz, 1), jnp.int32)
        hits = []
        for b in range(blocks):
            hit = jnp.zeros((nz, SEL), jnp.int32)
            for entries in rows:
                hit = jnp.where(entries == target + b, 1, hit)
            hits.append(jnp.max(hit, axis=1, keepdims=True))
        for b in range(blocks):
            high = jnp.where(hits[b] > 0, b, high)
            low = jnp.where(hits[blocks - 1 - b] > 0, blocks - 1 - b, low)
        found = jnp.where(lane == (ahead - 1) * 2, low, found)
        found = jnp.where(lane == (ahead - 1) * 2 + 1, high, found)
    table[0] = found
    size = blocks * SEL
    mine = jnp.concatenate(
        [chosen_ref[pl.ds(kv * blocks + r, 1), :] for r in range(blocks)], axis=1
    )
    mine = jnp.where(mine >= 0, mine, kv * blocks)
    across = jnp.broadcast_to(mine, (size, size))
    diagonal = lax.broadcasted_iota(jnp.int32, (size, size), 0) == lax.broadcasted_iota(
        jnp.int32, (size, size), 1
    )
    down = jnp.sum(jnp.where(diagonal, across, 0), axis=1, keepdims=True)
    lower = (down // blocks == across // blocks) & (down < across)
    second = jnp.max(jnp.where(lower, 1, 0), axis=0, keepdims=True)
    source = mine // blocks
    from_z, ahead = source // NY, (source % NY - y + NY) % NY
    left_base = nz * blocks
    right_base = left_base + 3 * nz
    far_base = right_base + 3 * nz
    place = jnp.where(
        ahead == 0,
        mine % blocks + from_z * blocks,
        jnp.where(
            ahead == NY - 1,
            left_base + 3 * from_z + second,
            jnp.where(ahead == 1, right_base + 3 * from_z + second, far_base + second * nz + from_z),
        ),
    )
    full = jnp.concatenate([place, jnp.zeros((1, table.shape[2] - size), jnp.int32)], axis=1)
    table[1] = jnp.broadcast_to(full, table.shape[1:])


def attend(
    nz,
    ntp,
    tokens_hbm,
    wq_hbm,
    wk_hbm,
    wv_hbm,
    w_hbm,
    chosen_hbm,
    cos_piece,
    sin_piece,
    out_ref,
    lse_ref,
    tokens_ref,
    wq_ref,
    wk_ref,
    wv_ref,
    q_ref,
    chosen_across,
    chosen_ref,
    cos_ref,
    sin_ref,
    table,
    sel_ref,
    idx_ref,
    local_sem,
    pool,
    to_right,
    to_left,
    picked,
    wall,
    att,
    abuf,
    z_send,
    z_recv,
    y_send,
    y_recv,
    relay_recv,
    w_send,
    w_recv,
    a_send,
    a_recv,
):
    kv = lax.axis_index("kv")
    tp = lax.axis_index("tp")
    z, y = kv // NY, kv % NY
    nx = ntp // 2
    x, core = tp // 2, tp % 2
    up = ((z + 1) % nz) * NY + y
    down = ((z + nz - 1) % nz) * NY + y
    right = z * NY + (y + 1) % NY
    left = z * NY + (y + NY - 1) % NY
    x_right = ((x + 1) % nx) * 2 + core
    x_left = ((x + nx - 1) % nx) * 2 + core
    partner = x * 2 + (1 - core)
    width = wk_ref.shape[1]
    blocks = att.shape[0] // BLK
    heads = width // HEAD_DIM
    left_base = nz * blocks
    right_base = left_base + 3 * nz
    far0_base = right_base + 3 * nz
    far1_base = far0_base + nz
    rows = att.shape[0] // ntp

    def load(which, src, dst):
        return pltpu.make_async_copy(src, dst, local_sem.at[which])

    loads = [
        load(0, tokens_hbm, tokens_ref),
        load(1, wk_hbm, wk_ref),
        load(2, wv_hbm, wv_ref),
        load(3, w_hbm, wall.at[tp]),
        load(4, wq_hbm, wq_ref),
    ]
    listing = load(7, chosen_hbm, chosen_across)
    listing.start()
    for copy in loads:
        copy.start()

    barrier = pltpu.get_barrier_semaphore()
    for peer in (up, down, right, left):
        pl.semaphore_signal(barrier, inc=1, device_id=(peer, tp), device_id_type=MESH)
    for step in range(1, ntp):
        pl.semaphore_signal(
            barrier, inc=1, device_id=(kv, (tp + step) % ntp), device_id_type=MESH
        )
    rotary_tables(cos_piece, sin_piece, cos_ref, sin_ref)
    listing.wait()
    chosen_ref[...] = jnp.transpose(chosen_across[...])
    make_tables(nz, blocks, kv, chosen_ref, table)
    to_smem = [load(5, table.at[0], sel_ref), load(6, table.at[1, pl.ds(0, 8)], idx_ref)]
    for copy in to_smem:
        copy.start()
    pl.semaphore_wait(barrier, 4 + ntp - 1)

    def remote(src, dst, send, recv, device):
        return pltpu.make_async_remote_copy(
            src_ref=src,
            dst_ref=dst,
            send_sem=send,
            recv_sem=recv,
            device_id=device,
            device_id_type=MESH,
        )

    ups = (nz - 1 + 1) // 2
    downs = nz - 1 - ups

    part = blocks // 2
    parts = blocks // part

    def up_copy(step, b):
        at = pool.at[pl.ds((z + nz - step) % nz * blocks + b * part, part)]
        return remote(at, at, z_send, z_recv.at[step * parts + b], (up, tp))

    def down_copy(step, b):
        at = pool.at[pl.ds((z + step) % nz * blocks + b * part, part)]
        return remote(at, at, z_send, z_recv.at[step * parts + b], (down, tp))

    def stretch(size):
        return pool.at[pl.ds(0, size)]

    def arrived(size, sem):
        remote(stretch(size), stretch(size), z_send, sem, (up, tp)).wait_recv()

    def left_off(size, sem):
        remote(stretch(size), stretch(size), sem, relay_recv, (up, tp)).wait_send()

    def right_copy(p):
        dst = pool.at[pl.ds(left_base + 3 * p, 3)]
        return remote(to_right.at[p], dst, y_send, y_recv.at[p], (right, tp))

    def left_copy(p):
        dst = pool.at[pl.ds(right_base + 3 * p, 3)]
        return remote(to_left.at[p], dst, y_send, y_recv.at[p], (left, tp))

    def right_relay(p):
        src = pool.at[left_base + 3 * p + 2]
        return remote(src, pool.at[far0_base + p], y_send, relay_recv, (right, tp))

    def left_relay(p):
        src = pool.at[right_base + 3 * p + 2]
        return remote(src, pool.at[far1_base + p], y_send, relay_recv, (left, tp))

    def exchange(p):
        here = [pool[p * blocks + b] for b in range(blocks)]

        def pick(ahead, c):
            which = sel_ref[p, (ahead - 1) * 2 + c]
            found = here[blocks - 1]
            for b in range(blocks - 1):
                found = jnp.where(which == b, here[b], found)
            return found

        to_right[p, 0] = pick(1, 0)
        to_right[p, 1] = pick(1, 1)
        to_right[p, 2] = pick(2, 0)
        right_copy(p).start()
        to_left[p, 0] = pick(3, 0)
        to_left[p, 1] = pick(3, 1)
        to_left[p, 2] = pick(2, 1)
        left_copy(p).start()

    def relay(p):
        arrived(6, y_recv.at[p])
        right_relay(p).start()
        left_relay(p).start()

    half = width // 2

    def w_ring(side):
        peer = x_right if side == 0 else x_left
        return remote(wall.at[tp], wall.at[tp], w_send, w_recv.at[side], (kv, peer))

    def w_half(side):
        origin = x_left if side == 0 else x_right
        peer = x_right if side == 0 else x_left
        piece = wall.at[origin, pl.ds(side * half, half)]
        return remote(piece, piece, w_send, w_recv.at[2], (kv, peer))

    def w_arrived(size, sem):
        remote(wall.at[pl.ds(0, size)], wall.at[pl.ds(0, size)], w_send, sem, (kv, partner)).wait_recv()

    def w_pair(which):
        far = ((x + 2) % nx) * 2 + core
        owner = (tp, x_left, x_right, far)[which]
        return remote(wall.at[owner], wall.at[owner], w_send, w_recv.at[3], (kv, partner))

    loads[0].wait()
    loads[1].wait()
    cos_part, sin_part = cos_ref[...], sin_ref[...]
    keys = jnp.dot(tokens_ref[...], wk_ref[...], preferred_element_type=jnp.float32)
    keys = turn(keys, cos_part, sin_part).astype(jnp.bfloat16)
    pool[pl.ds(z * blocks, blocks), :, :width] = keys.reshape(blocks, BLK, width)
    loads[2].wait()
    values = jnp.dot(tokens_ref[...], wv_ref[...], preferred_element_type=jnp.float32)
    values = values.astype(jnp.bfloat16)
    pool[pl.ds(z * blocks, blocks), :, width:] = values.reshape(blocks, BLK, width)
    for b in range(parts):
        up_copy(0, b).start()
        down_copy(0, b).start()
    for copy in to_smem:
        copy.wait()
    exchange(z)
    loads[3].wait()
    w_ring(0).start()
    w_ring(1).start()
    w_pair(0).start()
    loads[4].wait()
    query = jnp.dot(tokens_ref[...], wq_ref[...], preferred_element_type=jnp.float32)
    query = turn(query, cos_part, sin_part).astype(jnp.bfloat16).astype(jnp.float32)
    query = query * HEAD_DIM ** (-0.5)
    channel = lax.broadcasted_iota(jnp.int32, query.shape, 1)
    for head in range(heads):
        mine = jnp.where(channel // HEAD_DIM == head, query, 0.0).astype(jnp.bfloat16)
        q_ref[:, head * BLK : (head + 1) * BLK, :] = mine.reshape(blocks, BLK, width)

    order = [[(z, None)]]
    for step in range(ups):
        for b in range(parts):
            both = 2 if step < downs else 1
            arrived(both * part, z_recv.at[step * parts + b])
            if step + 1 < ups:
                up_copy(step + 1, b).start()
            if step + 1 < downs:
                down_copy(step + 1, b).start()
        now = []
        above = z - 1 - step
        now.append((above, above >= 0))
        if step < downs:
            below = z + 1 + step - nz
            now.append((below, below >= 0))
        for p, there in now:
            pl.when(there)(functools.partial(exchange, p))
        order.append(now)
        if step == 3 or step == ups - 2 and ups < 5:
            w_ring(0).wait_recv()
            w_half(0).start()
            w_pair(1).start()
            w_ring(1).wait_recv()
            w_half(1).start()
            w_pair(2).start()
        if step == 5 or step == ups - 1 and ups < 6:
            w_arrived(1, w_recv.at[2])
            w_pair(3).start()
        if step >= 1:
            for p, there in order[step - 1]:
                if there is None:
                    relay(p)
                else:
                    pl.when(there)(functools.partial(relay, p))
    for now in order[ups - 1 :]:
        for p, there in now:
            if there is None:
                relay(p)
            else:
                pl.when(there)(functools.partial(relay, p))
    left_off((ups + downs) * blocks, z_send)
    w_arrived(4, w_recv.at[3])
    sent = wall.at[pl.ds(0, ntp - 1)]
    remote(sent, sent, w_send, w_recv.at[3], (kv, partner)).wait_send()
    for k in range(nz):
        @pl.when(z == k)
        def _():
            left_off(8 * (k + 1), y_send)
            arrived(2 * (k + 1), relay_recv)

    def part_copy(to):
        src = att.at[pl.ds(to * rows, rows)]
        dst = abuf.at[:, pl.ds(pl.multiple_of(tp * width, width), width)]
        return remote(src, dst, a_send, a_recv, (kv, to))

    per_block = ntp // blocks
    lane = lax.broadcasted_iota(jnp.int32, (BLK, width), 1)
    row_id = lax.broadcasted_iota(jnp.int32, (heads * BLK, heads * BLK), 0)
    col_id = lax.broadcasted_iota(jnp.int32, (heads * BLK, heads * BLK), 1)
    key_id = lax.broadcasted_iota(jnp.int32, (1, SEL * BLK), 1)
    logs = []
    for i in range(blocks):
        for j in range(SEL):
            picked[j * BLK : (j + 1) * BLK, :] = pool[idx_ref[0, i * SEL + j]]
        scores = lax.dot_general(
            q_ref[i],
            picked[:, :width],
            (((1,), (1,)), ((), ())),
            preferred_element_type=jnp.float32,
        )
        listed = chosen_ref[pl.ds(kv * blocks + i, 1), :]
        count = jnp.sum((listed >= 0).astype(jnp.int32), axis=1, keepdims=True)
        scores = jnp.where(key_id < count * BLK, scores, MASKED)
        top = jnp.max(scores, axis=1, keepdims=True)
        weights = jnp.exp(scores - top)
        total = jnp.sum(weights, axis=1, keepdims=True)
        summed = jnp.dot(
            weights.astype(jnp.bfloat16), picked[:, width:], preferred_element_type=jnp.float32
        )
        summed = summed / total
        mixed = summed[:BLK]
        for head in range(1, heads):
            mixed = jnp.where(
                lane // HEAD_DIM == head, summed[head * BLK : (head + 1) * BLK], mixed
            )
        att[i * BLK : (i + 1) * BLK, :] = mixed.astype(jnp.bfloat16)
        for to in range(i * per_block, (i + 1) * per_block):
            @pl.when(to != tp)
            def _():
                part_copy(to).start()

            @pl.when(to == tp)
            def _():
                abuf[:, pl.ds(pl.multiple_of(tp * width, width), width)] = att[
                    to * rows : (to + 1) * rows, :
                ]
        column = top + jnp.log(total)
        logs.append(jnp.sum(jnp.where(row_id == col_id, column, 0.0), axis=0, keepdims=True))
    for head in range(heads):
        lse_ref[head : head + 1, :] = jnp.concatenate(
            [row[:, head * BLK : (head + 1) * BLK] for row in logs], axis=1
        )
    others = abuf.at[:, pl.ds(0, (ntp - 1) * width)]
    remote(others, others, a_send, a_recv, (kv, partner)).wait()
    total_width = out_ref.shape[1]
    chunk = min(512, total_width)
    for c in range(total_width // chunk):
        cols = slice(c * chunk, (c + 1) * chunk)
        acc = jnp.zeros((rows, chunk), jnp.float32)
        for t in range(ntp):
            acc += jnp.dot(
                abuf[:, t * width : (t + 1) * width],
                wall[t, :, cols],
                preferred_element_type=jnp.float32,
            )
        out_ref[:, cols] = acc.astype(jnp.bfloat16)


def finish(mixed_ref, log_ref, mixed_out, log_out, sem):
    first = pltpu.make_async_copy(mixed_ref, mixed_out, sem.at[0])
    second = pltpu.make_async_copy(log_ref, log_out, sem.at[1])
    first.start()
    second.start()
    first.wait()
    second.wait()


def local(nkv, ntp, tokens, w_query, w_key, w_value, w_out, chosen):
    local_rows = tokens.shape[0]
    width = w_query.shape[1]
    heads = width // HEAD_DIM
    blocks = local_rows // BLK
    nz = nkv // NY
    device = lax.axis_index("kv")
    vmem = pl.BlockSpec(memory_space=pltpu.VMEM)
    hbm = pl.BlockSpec(memory_space=pltpu.HBM)
    cos_piece, sin_piece = rotary_pieces(device * local_rows, width)
    ups = nz // 2
    out_rows = local_rows // ntp
    dma = pltpu.SemaphoreType.DMA
    pool_size = nz * (blocks + 8)
    mixed, log_sums = pl.pallas_call(
        functools.partial(attend, nz, ntp),
        out_shape=(
            jax.ShapeDtypeStruct((out_rows, w_out.shape[1]), jnp.bfloat16),
            jax.ShapeDtypeStruct((heads, local_rows), jnp.float32),
        ),
        in_specs=[hbm] * 6 + [vmem] * 2,
        out_specs=(vmem, vmem),
        scratch_shapes=[
            pltpu.VMEM(tokens.shape, jnp.bfloat16),
            pltpu.VMEM(w_query.shape, jnp.bfloat16),
            pltpu.VMEM(w_key.shape, jnp.bfloat16),
            pltpu.VMEM(w_value.shape, jnp.bfloat16),
            pltpu.VMEM((blocks, heads * BLK, width), jnp.bfloat16),
            pltpu.VMEM((SEL, chosen.shape[0]), jnp.int32),
            pltpu.VMEM((chosen.shape[0], SEL), jnp.int32),
            pltpu.VMEM((local_rows, width), jnp.float32),
            pltpu.VMEM((local_rows, width), jnp.float32),
            pltpu.VMEM((2, nz, 128), jnp.int32),
            pltpu.SMEM((nz, 128), jnp.int32),
            pltpu.SMEM((8, 128), jnp.int32),
            dma((8,)),
            pltpu.VMEM((pool_size, BLK, 2 * width), jnp.bfloat16),
            pltpu.VMEM((nz, 3, BLK, 2 * width), jnp.bfloat16),
            pltpu.VMEM((nz, 3, BLK, 2 * width), jnp.bfloat16),
            pltpu.VMEM((SEL * BLK, 2 * width), jnp.bfloat16),
            pltpu.VMEM((ntp, width, w_out.shape[1]), jnp.bfloat16),
            pltpu.VMEM((local_rows, width), jnp.bfloat16),
            pltpu.VMEM((out_rows, ntp * width), jnp.bfloat16),
            dma,
            dma((2 * ups,)),
            dma,
            dma((nz,)),
            dma,
            dma,
            dma((4,)),
            dma,
            dma,
        ],
        compiler_params=pltpu.CompilerParams(
            collective_id=0, has_side_effects=True, vmem_limit_bytes=55000 * 1024
        ),
    )(tokens, w_query, w_key, w_value, w_out, chosen.T, cos_piece, sin_piece)
    return pl.pallas_call(
        finish,
        out_shape=(
            jax.ShapeDtypeStruct(mixed.shape, mixed.dtype),
            jax.ShapeDtypeStruct(log_sums.shape, log_sums.dtype),
        ),
        in_specs=[vmem, vmem],
        out_specs=(hbm, hbm),
        scratch_shapes=[dma((2,))],
        compiler_params=pltpu.CompilerParams(vmem_limit_bytes=1024 * 1024),
    )(mixed, log_sums)


def solution(mesh):
    placed = (P("kv", None), P(None, "tp"), P(None, "tp"), P(None, "tp"), P("tp", None), P())
    return jax.shard_map(
        functools.partial(local, mesh.shape["kv"], mesh.shape["tp"]),
        mesh=mesh,
        in_specs=placed,
        out_specs=(P(("kv", "tp"), None), P("tp", "kv")),
        check_vma=False,
    )
```

```python
import functools

import jax
import jax.numpy as jnp
from jax import lax
from jax.experimental import pallas as pl
from jax.experimental.pallas import tpu as pltpu
from jax.sharding import PartitionSpec as P

HEAD_DIM = 64
BLK = 64
SEL = 16
NY = 4
ROTARY_BASE = 500000.0
MASKED = -1e30
MESH = pl.DeviceIdType.MESH


def rotary_pieces(first, width):
    half = HEAD_DIM // 2
    lane = jnp.arange(width)
    inverse = ROTARY_BASE ** (-(lane % half).astype(jnp.float32) / half)
    row = jnp.arange(40)
    position = jnp.where(row < 16, 16 * row, jnp.where(row < 32, row - 16, first))
    angles = position.astype(jnp.float32)[:, None] * inverse[None, :]
    return jnp.cos(angles), jnp.sin(angles)


def rotary_tables(cos_piece, sin_piece, cos_ref, sin_ref):
    half = HEAD_DIM // 2
    cos_first, sin_first = cos_piece[32:33, :], sin_piece[32:33, :]
    cos_tens, sin_tens = cos_piece[:16, :], sin_piece[:16, :]
    cos_ones, sin_ones = cos_piece[16:32, :], sin_piece[16:32, :]
    lane = lax.broadcasted_iota(jnp.int32, cos_ones.shape, 1)
    sign = jnp.where(lane % HEAD_DIM < half, -1.0, 1.0)
    cos_row = cos_first * cos_tens - sin_first * sin_tens
    sin_row = sin_first * cos_tens + cos_first * sin_tens
    for t in range(cos_ref.shape[0] // 16):
        c, n = cos_row[t : t + 1, :], sin_row[t : t + 1, :]
        cos_ref[t * 16 : (t + 1) * 16, :] = c * cos_ones - n * sin_ones
        sin_ref[t * 16 : (t + 1) * 16, :] = (n * cos_ones + c * sin_ones) * sign


def turn(values, cos_part, sin_part):
    width = values.shape[1]
    half = HEAD_DIM // 2
    lane = lax.broadcasted_iota(jnp.int32, values.shape, 1)
    ahead = pltpu.roll(values, width - half, 1)
    behind = pltpu.roll(values, half, 1)
    partner = jnp.where(lane % HEAD_DIM < half, ahead, behind)
    return values * cos_part + partner * sin_part


def make_tables(nz, blocks, kv, dest_z, low, high, planes, chosen_ref, table, at):
    z, y = kv // NY, kv % NY
    lane = lax.broadcasted_iota(jnp.int32, table.shape[1:], 1)
    found = jnp.zeros(table.shape[1:], jnp.int32)
    target = lax.broadcasted_iota(jnp.int32, (nz, SEL), 0) * (NY * blocks) + y * blocks
    for ahead in range(1, NY):
        dest = dest_z * NY + (y + ahead) % NY
        rows = [chosen_ref[pl.ds(dest * blocks + r, 1), :] for r in range(blocks)]
        least = jnp.full((nz, 1), blocks - 1, jnp.int32)
        most = jnp.zeros((nz, 1), jnp.int32)
        hits = []
        for b in range(blocks):
            hit = jnp.zeros((nz, SEL), jnp.int32)
            for entries in rows:
                hit = jnp.where(entries == target + b, 1, hit)
            hits.append(jnp.max(hit, axis=1, keepdims=True))
        for b in range(blocks):
            most = jnp.where(hits[b] > 0, b, most)
            least = jnp.where(hits[blocks - 1 - b] > 0, blocks - 1 - b, least)
        found = jnp.where(lane == (ahead - 1) * 2, least, found)
        found = jnp.where(lane == (ahead - 1) * 2 + 1, most, found)
    table[at] = found
    size = blocks * SEL
    first_row = (dest_z * NY + y) * blocks
    mine = jnp.concatenate([chosen_ref[pl.ds(first_row + r, 1), :] for r in range(blocks)], axis=1)
    across = jnp.broadcast_to(mine, (size, size))
    diagonal = lax.broadcasted_iota(jnp.int32, (size, size), 0) == lax.broadcasted_iota(
        jnp.int32, (size, size), 1
    )
    down = jnp.sum(jnp.where(diagonal, across, 0), axis=1, keepdims=True)
    lower = (down // blocks == across // blocks) & (down >= 0) & (down < across)
    second = jnp.max(jnp.where(lower, 1, 0), axis=0, keepdims=True)
    source = jnp.maximum(mine, 0) // blocks
    from_z, ahead = source // NY, (source % NY - y + NY) % NY
    served = (mine >= 0) & (from_z >= low) & (from_z <= high)
    here = (ahead == 0) | (served == False)
    column = jnp.where(served, from_z * blocks + jnp.maximum(mine, 0) % blocks, z * blocks)
    column = jnp.where(here, column, 0)
    along = jnp.where(
        ahead == NY - 1,
        3 * from_z + second,
        jnp.where(
            ahead == 1,
            3 * planes + 3 * from_z + second,
            6 * planes + second * planes + from_z,
        ),
    )
    along = jnp.where(here, 0, along)
    blank = jnp.zeros((1, table.shape[2] - size), jnp.int32)
    full = [jnp.concatenate([v, blank], axis=1) for v in (column, along, here.astype(jnp.int32))]
    row = lax.broadcasted_iota(jnp.int32, table.shape[1:], 0)
    table[at + 1] = jnp.where(row == 0, full[0], jnp.where(row == 1, full[1], full[2]))


def attend(
    nz,
    ntp,
    tokens_hbm,
    wq_hbm,
    wk_hbm,
    wv_hbm,
    w_hbm,
    chosen_hbm,
    cos_piece,
    sin_piece,
    out_ref,
    lse_ref,
    tokens_ref,
    wq_ref,
    wk_ref,
    wv_ref,
    q_ref,
    q_far,
    chosen_across,
    chosen_ref,
    cos_ref,
    sin_ref,
    table,
    sel_ref,
    idx_ref,
    far_sel_ref,
    far_idx_ref,
    pool,
    own_pool,
    far_pool,
    to_right,
    to_left,
    picked,
    wall,
    mixed_ref,
    wide_ref,
    help_out,
    help_log_out,
    help_in,
    help_log_in,
    att,
    abuf,
    local_sem,
    z_send,
    up_recv,
    down_recv,
    y_send,
    y_recv,
    far_recv,
    relay_recv,
    w_send,
    w_recv,
    help_send,
    help_recv,
    a_send,
    a_recv,
):
    kv = lax.axis_index("kv")
    tp = lax.axis_index("tp")
    z, y = kv // NY, kv % NY
    nx = ntp // 2
    x, core = tp // 2, tp % 2
    up = ((z + 1) % nz) * NY + y
    down = ((z + nz - 1) % nz) * NY + y
    mirror_z = nz - 1 - z
    mirror = mirror_z * NY + y
    right = z * NY + (y + 1) % NY
    left = z * NY + (y + NY - 1) % NY
    x_right = ((x + 1) % nx) * 2 + core
    x_left = ((x + nx - 1) % nx) * 2 + core
    partner = x * 2 + (1 - core)
    width = wk_ref.shape[1]
    blocks = att.shape[0] // BLK
    heads = width // HEAD_DIM
    rows = att.shape[0] // ntp
    ups = nz // 2
    last_far = ups - 2 - z

    def load(which, src, dst):
        return pltpu.make_async_copy(src, dst, local_sem.at[which])

    loads = [
        load(0, tokens_hbm, tokens_ref),
        load(1, wk_hbm, wk_ref),
        load(2, wv_hbm, wv_ref),
        load(3, w_hbm, wall.at[tp]),
        load(4, wq_hbm, wq_ref),
    ]
    listing = load(5, chosen_hbm, chosen_across)
    listing.start()
    for copy in loads:
        copy.start()

    barrier = pltpu.get_barrier_semaphore()
    for peer in (mirror, up, down, right, left):
        pl.semaphore_signal(barrier, inc=1, device_id=(peer, tp), device_id_type=MESH)
    for step in range(1, ntp):
        pl.semaphore_signal(barrier, inc=1, device_id=(kv, (tp + step) % ntp), device_id_type=MESH)
    rotary_tables(cos_piece, sin_piece, cos_ref, sin_ref)
    listing.wait()
    chosen_ref[...] = jnp.transpose(chosen_across[...])
    make_tables(nz, blocks, kv, z, z - ups, nz, nz, chosen_ref, table, 0)
    make_tables(nz, blocks, kv, mirror_z, 0, last_far, nz // 2, chosen_ref, table, 2)
    to_smem = [
        load(5, table.at[0], sel_ref),
        load(6, table.at[1, pl.ds(0, 8)], idx_ref),
        load(7, table.at[2], far_sel_ref),
        load(8, table.at[3, pl.ds(0, 8)], far_idx_ref),
    ]
    for copy in to_smem:
        copy.start()
    pl.semaphore_wait(barrier, 5 + ntp - 1)

    def remote(src, dst, send, recv, device):
        return pltpu.make_async_remote_copy(
            src_ref=src,
            dst_ref=dst,
            send_sem=send,
            recv_sem=recv,
            device_id=device,
            device_id_type=MESH,
        )

    part = blocks // 2
    parts = blocks // part

    def up_copy(step, b):
        at = pool.at[(z + nz - step) % nz * blocks + b]
        return remote(at, at, z_send, up_recv.at[step * blocks + b], (up, tp))

    def down_copy(step, b):
        at = pool.at[pl.ds((z + step) % nz * blocks + b * part, part)]
        return remote(at, at, z_send, down_recv.at[step * parts + b], (down, tp))

    def stretch(size):
        return own_pool.at[pl.ds(0, size)]

    def arrived(size, sem):
        remote(stretch(size), stretch(size), z_send, sem, (up, tp)).wait_recv()

    def left_off(size, sem):
        remote(stretch(size), stretch(size), sem, relay_recv.at[0], (up, tp)).wait_send()

    class Route:
        def __init__(self, kind):
            self.kind = kind
            self.pool = (own_pool, far_pool)[kind]
            self.planes = (nz, nz // 2)[kind]
            self.stage = (0, nz)[kind]
            self.sel = (sel_ref, far_sel_ref)[kind]
            self.recv = (y_recv, far_recv)[kind]

        def right_copy(self, k, p):
            dst = self.pool.at[pl.ds(3 * p, 3)]
            return remote(to_right.at[self.stage + p], dst, y_send, self.recv.at[k], (right, tp))

        def left_copy(self, k, p):
            dst = self.pool.at[pl.ds(3 * self.planes + 3 * p, 3)]
            return remote(to_left.at[self.stage + p], dst, y_send, self.recv.at[k], (left, tp))

        def right_relay(self, p):
            src = self.pool.at[3 * p + 2]
            dst = self.pool.at[6 * self.planes + p]
            return remote(src, dst, y_send, relay_recv.at[self.kind], (right, tp))

        def left_relay(self, p):
            src = self.pool.at[3 * self.planes + 3 * p + 2]
            dst = self.pool.at[7 * self.planes + p]
            return remote(src, dst, y_send, relay_recv.at[self.kind], (left, tp))

        def exchange(self, k, p):
            here = [pool[p * blocks + b] for b in range(blocks)]
            at = self.stage + p

            def pick(ahead, c):
                which = self.sel[p, (ahead - 1) * 2 + c]
                found = here[blocks - 1]
                for b in range(blocks - 1):
                    found = jnp.where(which == b, here[b], found)
                return found

            to_right[at, 0] = pick(1, 0)
            to_right[at, 1] = pick(1, 1)
            to_right[at, 2] = pick(2, 0)
            self.right_copy(k, p).start()
            to_left[at, 0] = pick(3, 0)
            to_left[at, 1] = pick(3, 1)
            to_left[at, 2] = pick(2, 1)
            self.left_copy(k, p).start()

        def relay(self, k, p):
            arrived(6, self.recv.at[k])
            self.right_relay(p).start()
            self.left_relay(p).start()

    routes = (Route(0), Route(1))

    half = width // 2

    def w_ring(side):
        peer = x_right if side == 0 else x_left
        return remote(wall.at[tp], wall.at[tp], w_send, w_recv.at[side], (kv, peer))

    def w_half(side):
        origin = x_left if side == 0 else x_right
        peer = x_right if side == 0 else x_left
        piece = wall.at[origin, pl.ds(side * half, half)]
        return remote(piece, piece, w_send, w_recv.at[2], (kv, peer))

    def w_arrived(size, sem):
        at = wall.at[pl.ds(0, size)]
        remote(at, at, w_send, sem, (kv, partner)).wait_recv()

    def w_pair(which):
        far = ((x + 2) % nx) * 2 + core
        owner = (tp, x_left, x_right, far)[which]
        return remote(wall.at[owner], wall.at[owner], w_send, w_recv.at[3], (kv, partner))

    def w_first():
        w_ring(0).wait_recv()
        w_half(0).start()
        w_pair(1).start()
        w_ring(1).wait_recv()
        w_half(1).start()
        w_pair(2).start()

    def w_second():
        w_arrived(1, w_recv.at[2])
        w_pair(3).start()

    q_copy = remote(q_ref, q_far, help_send.at[0], help_recv.at[0], (mirror, tp))
    o_copy = remote(help_out, help_in, help_send.at[1], help_recv.at[1], (mirror, tp))
    log_copy = remote(help_log_out, help_log_in, help_send.at[2], help_recv.at[2], (mirror, tp))
    helper = last_far >= 0
    helped = mirror_z <= ups - 2

    loads[0].wait()
    loads[1].wait()
    cos_part, sin_part = cos_ref[...], sin_ref[...]
    keys = jnp.dot(tokens_ref[...], wk_ref[...], preferred_element_type=jnp.float32)
    keys = turn(keys, cos_part, sin_part).astype(jnp.bfloat16)
    pool[pl.ds(z * blocks, blocks), :, :width] = keys.reshape(blocks, BLK, width)
    loads[2].wait()
    values = jnp.dot(tokens_ref[...], wv_ref[...], preferred_element_type=jnp.float32)
    values = values.astype(jnp.bfloat16)
    pool[pl.ds(z * blocks, blocks), :, width:] = values.reshape(blocks, BLK, width)

    @pl.when(z < nz - 1)
    def _():
        for b in range(blocks):
            up_copy(0, b).start()

    goes_down = (z >= 1) & (z <= ups - 2)

    @pl.when(goes_down)
    def _():
        for b in range(parts):
            down_copy(0, b).start()

    for copy in to_smem:
        copy.wait()
    pl.when(z <= last_far)(lambda: routes[1].exchange(0, z))
    routes[0].exchange(0, z)
    loads[4].wait()
    query = jnp.dot(tokens_ref[...], wq_ref[...], preferred_element_type=jnp.float32)
    query = turn(query, cos_part, sin_part).astype(jnp.bfloat16).astype(jnp.float32)
    q_ref[...] = (query * HEAD_DIM ** (-0.5)).astype(jnp.bfloat16)
    pl.when(helped)(lambda: q_copy.start())
    loads[3].wait()
    w_ring(0).start()
    w_ring(1).start()
    w_pair(0).start()

    def own_there(k):
        return z - k >= 0

    def far_below(k):
        return (z - k >= 0) & (z - k <= last_far)

    def far_above(step):
        return z + 1 + step <= last_far

    def relay_step(k):
        pl.when(far_below(k))(lambda: routes[1].relay(k, z - k))
        if 1 <= k <= ups - 2:
            pl.when(far_above(k - 1))(lambda: routes[1].relay(ups + k - 1, z + k))
        pl.when(own_there(k))(lambda: routes[0].relay(k, z - k))

    for step in range(ups):
        k = step + 1

        @pl.when(own_there(k))
        def _():
            for b in range(blocks):
                remote(pool.at[b], pool.at[b], z_send, up_recv.at[step * blocks + b], (up, tp)).wait_recv()
                if step + 1 < ups:
                    pl.when(z < nz - 1)(lambda: up_copy(step + 1, b).start())
            pl.when(z - k <= last_far)(lambda: routes[1].exchange(k, z - k))
            routes[0].exchange(k, z - k)

        if step <= ups - 3:

            @pl.when(z + 1 + step <= ups - 2)
            def _():
                for b in range(parts):
                    arrived(part, down_recv.at[step * parts + b])

                    if step <= ups - 4:

                        @pl.when(z >= 1)
                        def _():
                            down_copy(step + 1, b).start()

                pl.when(far_above(step))(lambda: routes[1].exchange(ups + step, z + k))

        if step == 3:
            w_first()
        if step == 5:
            w_second()
        if step >= 1:
            relay_step(step - 1)
    relay_step(ups - 1)
    relay_step(ups)

    def plane_counts(c):
        own = min(c, ups) + 1
        far = max(0, ups - 1 - c)
        ups_sent = min(c, ups - 1) + 1 if c < nz - 1 else 0
        downs_sent = ups - 1 - c if 1 <= c <= ups - 2 else 0
        return own, far, (ups_sent + downs_sent) * blocks

    lane = lax.broadcasted_iota(jnp.int32, (BLK, width), 1)
    wide_lane = lax.broadcasted_iota(jnp.int32, (heads * BLK, width), 1)
    wide_row = lax.broadcasted_iota(jnp.int32, (heads * BLK, width), 0)
    eye = lax.broadcasted_iota(jnp.int32, (heads * BLK, heads * BLK), 0) == lax.broadcasted_iota(
        jnp.int32, (heads * BLK, heads * BLK), 1
    )
    key_block = lax.broadcasted_iota(jnp.int32, (1, SEL * BLK), 1) // BLK

    def by_head(stacked):
        result = stacked[:BLK]
        for head in range(1, heads):
            result = jnp.where(lane // HEAD_DIM == head, stacked[head * BLK : (head + 1) * BLK], result)
        return result

    def attention(i, queries, places, along, dest, low, high):
        for j in range(SEL):
            n = i * SEL + j
            picked[j * BLK : (j + 1) * BLK, :] = jnp.where(
                places[2, n] > 0, pool[places[0, n]], along[places[1, n]]
            )
        rows_here = queries[i * BLK : (i + 1) * BLK, :].astype(jnp.float32)
        stacked = jnp.concatenate([rows_here] * heads, axis=0)
        stacked = jnp.where(wide_lane // HEAD_DIM == wide_row // BLK, stacked, 0.0)
        scores = lax.dot_general(
            stacked.astype(jnp.bfloat16),
            picked[:, :width],
            (((1,), (1,)), ((), ())),
            preferred_element_type=jnp.float32,
        )
        listed = chosen_ref[pl.ds(dest * blocks + i, 1), :]
        block_of = jnp.zeros((1, SEL * BLK), jnp.int32)
        for j in range(SEL):
            block_of = jnp.where(key_block == j, listed[:, j : j + 1], block_of)
        scores = jnp.where((block_of >= low) & (block_of < high), scores, MASKED)
        top = jnp.max(scores, axis=1, keepdims=True)
        weights = jnp.exp(scores - top)
        total = jnp.sum(weights, axis=1, keepdims=True)
        summed = jnp.dot(
            weights.astype(jnp.bfloat16), picked[:, width:], preferred_element_type=jnp.float32
        )
        return by_head(summed / total), top + jnp.log(total)

    first = jnp.maximum(z - ups, 0) * NY * blocks

    def own_attention():
        for c in range(nz):
            pl.when(z == c)(lambda: arrived(2 * plane_counts(c)[0], relay_recv.at[0]))
        for i in range(blocks):
            result, column = attention(i, q_ref, idx_ref, own_pool, kv, first, nz * NY * blocks)
            mixed_ref[i * BLK : (i + 1) * BLK, :] = result
            wide_ref[i * BLK : (i + 1) * BLK, :] = by_head(
                jnp.broadcast_to(column, (heads * BLK, width))
            )

    early = z <= 1
    pl.when(early)(own_attention)

    @pl.when(helper)
    def _():
        for c in range(ups - 1):

            @pl.when(z == c)
            def _():
                arrived(2 * plane_counts(c)[1], relay_recv.at[1])

        q_copy.wait_recv()
        help_log_out[...] = jnp.zeros(help_log_out.shape, jnp.float32)
        limit = (last_far + 1) * NY * blocks
        for i in range(blocks):
            result, column = attention(i, q_far, far_idx_ref, far_pool, mirror, 0, limit)
            help_out[i * BLK : (i + 1) * BLK, :] = result.astype(jnp.bfloat16)
            help_log_out[i : i + 1, :] = jnp.sum(jnp.where(eye, column, 0.0), axis=0, keepdims=True)
        o_copy.start()
        log_copy.start()

    pl.when(z > 1)(own_attention)

    @pl.when(helped)
    def _():
        o_copy.wait_recv()
        log_copy.wait_recv()
        for i in range(blocks):
            at = slice(i * BLK, (i + 1) * BLK)
            row = jnp.broadcast_to(help_log_in[i : i + 1, :], (heads * BLK, width))
            column = jnp.sum(jnp.where(eye, row, 0.0), axis=1, keepdims=True)
            theirs = by_head(jnp.broadcast_to(column, (heads * BLK, width)))
            mine = wide_ref[at, :]
            top = jnp.maximum(mine, theirs)
            share, other = jnp.exp(mine - top), jnp.exp(theirs - top)
            total = share + other
            extra = help_in[at, :].astype(jnp.float32)
            mixed_ref[at, :] = (mixed_ref[at, :] * share + extra * other) / total
            wide_ref[at, :] = top + jnp.log(total)

    def part_copy(to):
        src = att.at[pl.ds(to * rows, rows)]
        dst = abuf.at[:, pl.ds(pl.multiple_of(tp * width, width), width)]
        return remote(src, dst, a_send, a_recv, (kv, to))

    per_block = ntp // blocks
    for i in range(blocks):
        at = slice(i * BLK, (i + 1) * BLK)
        att[at, :] = mixed_ref[at, :].astype(jnp.bfloat16)
        for to in range(i * per_block, (i + 1) * per_block):

            @pl.when(to != tp)
            def _():
                part_copy(to).start()

            @pl.when(to == tp)
            def _():
                abuf[:, pl.ds(pl.multiple_of(tp * width, width), width)] = att[
                    to * rows : (to + 1) * rows, :
                ]

    for head in range(heads):
        cols = slice(head * HEAD_DIM, (head + 1) * HEAD_DIM)
        lse_ref[head : head + 1, :] = jnp.concatenate(
            [
                jnp.sum(
                    jnp.where(
                        eye[:BLK, :HEAD_DIM], wide_ref[i * BLK : (i + 1) * BLK, cols], 0.0
                    ),
                    axis=0,
                    keepdims=True,
                )
                for i in range(blocks)
            ],
            axis=1,
        )

    for c in range(nz):

        @pl.when(z == c)
        def _():
            own, far, sent = plane_counts(c)
            left_off(8 * (own + far), y_send)
            if sent:
                left_off(sent, z_send)

    @pl.when(helper)
    def _():
        o_copy.wait_send()
        log_copy.wait_send()

    pl.when(helped)(lambda: q_copy.wait_send())
    w_arrived(4, w_recv.at[3])
    sent_w = wall.at[pl.ds(0, ntp - 1)]
    remote(sent_w, sent_w, w_send, w_recv.at[3], (kv, partner)).wait_send()
    others = abuf.at[:, pl.ds(0, (ntp - 1) * width)]
    remote(others, others, a_send, a_recv, (kv, partner)).wait()
    total_width = out_ref.shape[1]
    chunk = min(512, total_width)
    for c in range(total_width // chunk):
        cols = slice(c * chunk, (c + 1) * chunk)
        acc = jnp.zeros((rows, chunk), jnp.float32)
        for t in range(ntp):
            acc += jnp.dot(
                abuf[:, t * width : (t + 1) * width],
                wall[t, :, cols],
                preferred_element_type=jnp.float32,
            )
        out_ref[:, cols] = acc.astype(jnp.bfloat16)


def finish(mixed_ref, log_ref, mixed_out, log_out, sem):
    first = pltpu.make_async_copy(mixed_ref, mixed_out, sem.at[0])
    second = pltpu.make_async_copy(log_ref, log_out, sem.at[1])
    first.start()
    second.start()
    first.wait()
    second.wait()


def local(nkv, ntp, tokens, w_query, w_key, w_value, w_out, chosen):
    local_rows = tokens.shape[0]
    width = w_query.shape[1]
    heads = width // HEAD_DIM
    blocks = local_rows // BLK
    nz = nkv // NY
    device = lax.axis_index("kv")
    vmem = pl.BlockSpec(memory_space=pltpu.VMEM)
    hbm = pl.BlockSpec(memory_space=pltpu.HBM)
    cos_piece, sin_piece = rotary_pieces(device * local_rows, width)
    ups = nz // 2
    out_rows = local_rows // ntp
    dma = pltpu.SemaphoreType.DMA
    stage = (nz + ups, 3, BLK, 2 * width)
    bf16, f32, i32 = jnp.bfloat16, jnp.float32, jnp.int32
    mixed, log_sums = pl.pallas_call(
        functools.partial(attend, nz, ntp),
        out_shape=(
            jax.ShapeDtypeStruct((out_rows, w_out.shape[1]), bf16),
            jax.ShapeDtypeStruct((heads, local_rows), f32),
        ),
        in_specs=[hbm] * 6 + [vmem] * 2,
        out_specs=(vmem, vmem),
        scratch_shapes=[
            pltpu.VMEM(tokens.shape, bf16),
            pltpu.VMEM(w_query.shape, bf16),
            pltpu.VMEM(w_key.shape, bf16),
            pltpu.VMEM(w_value.shape, bf16),
            pltpu.VMEM((local_rows, width), bf16),
            pltpu.VMEM((local_rows, width), bf16),
            pltpu.VMEM((SEL, chosen.shape[0]), i32),
            pltpu.VMEM((chosen.shape[0], SEL), i32),
            pltpu.VMEM((local_rows, width), f32),
            pltpu.VMEM((local_rows, width), f32),
            pltpu.VMEM((4, nz, 128), i32),
            pltpu.SMEM((nz, 128), i32),
            pltpu.SMEM((8, 128), i32),
            pltpu.SMEM((nz, 128), i32),
            pltpu.SMEM((8, 128), i32),
            pltpu.VMEM((nz * blocks, BLK, 2 * width), bf16),
            pltpu.VMEM((nz * 8, BLK, 2 * width), bf16),
            pltpu.VMEM((ups * 8, BLK, 2 * width), bf16),
            pltpu.VMEM(stage, bf16),
            pltpu.VMEM(stage, bf16),
            pltpu.VMEM((SEL * BLK, 2 * width), bf16),
            pltpu.VMEM((ntp, width, w_out.shape[1]), bf16),
            pltpu.VMEM((local_rows, width), f32),
            pltpu.VMEM((local_rows, width), f32),
            pltpu.VMEM((local_rows, width), bf16),
            pltpu.VMEM((8, heads * BLK), f32),
            pltpu.VMEM((local_rows, width), bf16),
            pltpu.VMEM((8, heads * BLK), f32),
            pltpu.VMEM((local_rows, width), bf16),
            pltpu.VMEM((out_rows, ntp * width), bf16),
            dma((9,)),
            dma,
            dma((blocks * ups,)),
            dma((2 * (ups - 2),)),
            dma,
            dma((ups + 1,)),
            dma((2 * ups - 2,)),
            dma((2,)),
            dma,
            dma((4,)),
            dma((3,)),
            dma((3,)),
            dma,
            dma,
        ],
        compiler_params=pltpu.CompilerParams(
            collective_id=0, has_side_effects=True, vmem_limit_bytes=55000 * 1024
        ),
    )(tokens, w_query, w_key, w_value, w_out, chosen.T, cos_piece, sin_piece)
    return pl.pallas_call(
        finish,
        out_shape=(
            jax.ShapeDtypeStruct(mixed.shape, mixed.dtype),
            jax.ShapeDtypeStruct(log_sums.shape, log_sums.dtype),
        ),
        in_specs=[vmem, vmem],
        out_specs=(hbm, hbm),
        scratch_shapes=[dma((2,))],
        compiler_params=pltpu.CompilerParams(vmem_limit_bytes=1024 * 1024),
    )(mixed, log_sums)


def solution(mesh):
    placed = (P("kv", None), P(None, "tp"), P(None, "tp"), P(None, "tp"), P("tp", None), P())
    return jax.shard_map(
        functools.partial(local, mesh.shape["kv"], mesh.shape["tp"]),
        mesh=mesh,
        in_specs=placed,
        out_specs=(P(("kv", "tp"), None), P("tp", "kv")),
        check_vma=False,
    )
```

```python
import functools

import jax
import jax.numpy as jnp
from jax import lax
from jax.experimental import pallas as pl
from jax.experimental.pallas import tpu as pltpu
from jax.sharding import PartitionSpec as P

HEAD_DIM = 64
BLK = 64
SEL = 16
NY = 4
ROTARY_BASE = 500000.0
MASKED = -1e30
MESH = pl.DeviceIdType.MESH


def rotary_pieces(first, width):
    half = HEAD_DIM // 2
    lane = jnp.arange(width)
    inverse = ROTARY_BASE ** (-(lane % half).astype(jnp.float32) / half)
    row = jnp.arange(40)
    position = jnp.where(row < 16, 16 * row, jnp.where(row < 32, row - 16, first))
    angles = position.astype(jnp.float32)[:, None] * inverse[None, :]
    return jnp.cos(angles), jnp.sin(angles)


def rotary_tables(cos_piece, sin_piece, cos_ref, sin_ref):
    half = HEAD_DIM // 2
    cos_first, sin_first = cos_piece[32:33, :], sin_piece[32:33, :]
    cos_tens, sin_tens = cos_piece[:16, :], sin_piece[:16, :]
    cos_ones, sin_ones = cos_piece[16:32, :], sin_piece[16:32, :]
    lane = lax.broadcasted_iota(jnp.int32, cos_ones.shape, 1)
    sign = jnp.where(lane % HEAD_DIM < half, -1.0, 1.0)
    cos_row = cos_first * cos_tens - sin_first * sin_tens
    sin_row = sin_first * cos_tens + cos_first * sin_tens
    for t in range(cos_ref.shape[0] // 16):
        c, n = cos_row[t : t + 1, :], sin_row[t : t + 1, :]
        cos_ref[t * 16 : (t + 1) * 16, :] = c * cos_ones - n * sin_ones
        sin_ref[t * 16 : (t + 1) * 16, :] = (n * cos_ones + c * sin_ones) * sign


def turn(values, cos_part, sin_part):
    width = values.shape[1]
    half = HEAD_DIM // 2
    lane = lax.broadcasted_iota(jnp.int32, values.shape, 1)
    ahead = pltpu.roll(values, width - half, 1)
    behind = pltpu.roll(values, half, 1)
    partner = jnp.where(lane % HEAD_DIM < half, ahead, behind)
    return values * cos_part + partner * sin_part


def make_tables(nz, blocks, kv, dest_z, low, high, planes, chosen_ref, table, at):
    z, y = kv // NY, kv % NY
    lane = lax.broadcasted_iota(jnp.int32, table.shape[1:], 1)
    found = jnp.zeros(table.shape[1:], jnp.int32)
    target = lax.broadcasted_iota(jnp.int32, (nz, SEL), 0) * (NY * blocks) + y * blocks
    for ahead in range(1, NY):
        dest = dest_z * NY + (y + ahead) % NY
        rows = [chosen_ref[pl.ds(dest * blocks + r, 1), :] for r in range(blocks)]
        least = jnp.full((nz, 1), blocks - 1, jnp.int32)
        most = jnp.zeros((nz, 1), jnp.int32)
        hits = []
        for b in range(blocks):
            hit = jnp.zeros((nz, SEL), jnp.int32)
            for entries in rows:
                hit = jnp.where(entries == target + b, 1, hit)
            hits.append(jnp.max(hit, axis=1, keepdims=True))
        for b in range(blocks):
            most = jnp.where(hits[b] > 0, b, most)
            least = jnp.where(hits[blocks - 1 - b] > 0, blocks - 1 - b, least)
        found = jnp.where(lane == (ahead - 1) * 2, least, found)
        found = jnp.where(lane == (ahead - 1) * 2 + 1, most, found)
    table[at] = found
    size = blocks * SEL
    first_row = (dest_z * NY + y) * blocks
    mine = jnp.concatenate([chosen_ref[pl.ds(first_row + r, 1), :] for r in range(blocks)], axis=1)
    across = jnp.broadcast_to(mine, (size, size))
    diagonal = lax.broadcasted_iota(jnp.int32, (size, size), 0) == lax.broadcasted_iota(
        jnp.int32, (size, size), 1
    )
    down = jnp.sum(jnp.where(diagonal, across, 0), axis=1, keepdims=True)
    lower = (down // blocks == across // blocks) & (down >= 0) & (down < across)
    second = jnp.max(jnp.where(lower, 1, 0), axis=0, keepdims=True)
    source = jnp.maximum(mine, 0) // blocks
    from_z, ahead = source // NY, (source % NY - y + NY) % NY
    served = (mine >= 0) & (from_z >= low) & (from_z <= high)
    here = (ahead == 0) | (served == False)
    column = jnp.where(served, from_z * blocks + jnp.maximum(mine, 0) % blocks, z * blocks)
    column = jnp.where(here, column, 0)
    along = jnp.where(
        ahead == NY - 1,
        3 * from_z + second,
        jnp.where(
            ahead == 1,
            3 * planes + 3 * from_z + second,
            6 * planes + second * planes + from_z,
        ),
    )
    along = jnp.where(here, 0, along)
    blank = jnp.zeros((1, table.shape[2] - size), jnp.int32)
    full = [jnp.concatenate([v, blank], axis=1) for v in (column, along, here.astype(jnp.int32))]
    row = lax.broadcasted_iota(jnp.int32, table.shape[1:], 0)
    table[at + 1] = jnp.where(row == 0, full[0], jnp.where(row == 1, full[1], full[2]))


def attend(
    nz,
    ntp,
    tokens_hbm,
    wq_hbm,
    wk_hbm,
    wv_hbm,
    w_hbm,
    chosen_hbm,
    cos_piece,
    sin_piece,
    out_ref,
    lse_ref,
    tokens_ref,
    wq_ref,
    wk_ref,
    wv_ref,
    q_ref,
    q_far,
    chosen_across,
    chosen_ref,
    cos_ref,
    sin_ref,
    table,
    sel_ref,
    idx_ref,
    far_sel_ref,
    far_idx_ref,
    pool,
    own_pool,
    far_pool,
    to_right,
    to_left,
    picked,
    wall,
    mixed_ref,
    wide_ref,
    help_out,
    help_log_out,
    help_in,
    help_log_in,
    att,
    abuf,
    local_sem,
    z_send,
    up_recv,
    down_recv,
    y_send,
    y_recv,
    far_recv,
    relay_recv,
    w_send,
    w_recv,
    help_send,
    help_recv,
    a_send,
    a_recv,
):
    kv = lax.axis_index("kv")
    tp = lax.axis_index("tp")
    z, y = kv // NY, kv % NY
    nx = ntp // 2
    x, core = tp // 2, tp % 2
    up = ((z + 1) % nz) * NY + y
    down = ((z + nz - 1) % nz) * NY + y
    mirror_z = nz - 1 - z
    mirror = mirror_z * NY + y
    right = z * NY + (y + 1) % NY
    left = z * NY + (y + NY - 1) % NY
    x_right = ((x + 1) % nx) * 2 + core
    x_left = ((x + nx - 1) % nx) * 2 + core
    partner = x * 2 + (1 - core)
    width = wk_ref.shape[1]
    blocks = att.shape[0] // BLK
    heads = width // HEAD_DIM
    rows = att.shape[0] // ntp
    ups = nz // 2
    last_far = ups - 2 - z

    def load(which, src, dst):
        return pltpu.make_async_copy(src, dst, local_sem.at[which])

    loads = [
        load(0, tokens_hbm, tokens_ref),
        load(1, wk_hbm, wk_ref),
        load(2, wv_hbm, wv_ref),
        load(3, w_hbm, wall.at[tp]),
        load(4, wq_hbm, wq_ref),
    ]
    listing = load(5, chosen_hbm, chosen_across)
    listing.start()
    for copy in loads:
        copy.start()

    barrier = pltpu.get_barrier_semaphore()
    for peer in (mirror, up, down, right, left):
        pl.semaphore_signal(barrier, inc=1, device_id=(peer, tp), device_id_type=MESH)
    for step in range(1, ntp):
        pl.semaphore_signal(barrier, inc=1, device_id=(kv, (tp + step) % ntp), device_id_type=MESH)
    rotary_tables(cos_piece, sin_piece, cos_ref, sin_ref)
    listing.wait()
    chosen_ref[...] = jnp.transpose(chosen_across[...])
    make_tables(nz, blocks, kv, z, z - ups, nz, nz, chosen_ref, table, 0)
    make_tables(nz, blocks, kv, mirror_z, 0, last_far, nz // 2, chosen_ref, table, 2)
    to_smem = [
        load(5, table.at[0], sel_ref),
        load(6, table.at[1, pl.ds(0, 8)], idx_ref),
        load(7, table.at[2], far_sel_ref),
        load(8, table.at[3, pl.ds(0, 8)], far_idx_ref),
    ]
    for copy in to_smem:
        copy.start()

    def remote(src, dst, send, recv, device):
        return pltpu.make_async_remote_copy(
            src_ref=src,
            dst_ref=dst,
            send_sem=send,
            recv_sem=recv,
            device_id=device,
            device_id_type=MESH,
        )

    part = 1
    parts = blocks

    def up_copy(step, b):
        at = pool.at[(z + nz - step) % nz * blocks + b]
        return remote(at, at, z_send, up_recv.at[step * blocks + b], (up, tp))

    def down_copy(step, b):
        at = pool.at[pl.ds((z + step) % nz * blocks + b, 1)]
        return remote(at, at, z_send, down_recv.at[step * parts + b], (down, tp))

    def stretch(size):
        return own_pool.at[pl.ds(0, size)]

    def arrived(size, sem):
        remote(stretch(size), stretch(size), z_send, sem, (up, tp)).wait_recv()

    def left_off(size, sem):
        remote(stretch(size), stretch(size), sem, relay_recv.at[0], (up, tp)).wait_send()

    class Route:
        def __init__(self, kind):
            self.kind = kind
            self.pool = (own_pool, far_pool)[kind]
            self.planes = (nz, nz // 2)[kind]
            self.stage = (0, nz)[kind]
            self.sel = (sel_ref, far_sel_ref)[kind]
            self.recv = (y_recv, far_recv)[kind]

        def right_copy(self, p):
            src, dst = to_right.at[self.stage + p, pl.ds(0, 2)], self.pool.at[pl.ds(3 * p, 2)]
            return remote(src, dst, y_send, relay_recv.at[self.kind], (right, tp))

        def left_copy(self, p):
            src = to_left.at[self.stage + p, pl.ds(0, 2)]
            dst = self.pool.at[pl.ds(3 * self.planes + 3 * p, 2)]
            return remote(src, dst, y_send, relay_recv.at[self.kind], (left, tp))

        def right_ahead(self, k, p):
            src, dst = to_right.at[self.stage + p, 2], self.pool.at[3 * p + 2]
            return remote(src, dst, y_send, self.recv.at[k], (right, tp))

        def left_ahead(self, k, p):
            src, dst = to_left.at[self.stage + p, 2], self.pool.at[3 * self.planes + 3 * p + 2]
            return remote(src, dst, y_send, self.recv.at[k], (left, tp))

        def right_relay(self, p):
            src = self.pool.at[3 * p + 2]
            dst = self.pool.at[6 * self.planes + p]
            return remote(src, dst, y_send, relay_recv.at[self.kind], (right, tp))

        def left_relay(self, p):
            src = self.pool.at[3 * self.planes + 3 * p + 2]
            dst = self.pool.at[7 * self.planes + p]
            return remote(src, dst, y_send, relay_recv.at[self.kind], (left, tp))

        def exchange(self, k, p):
            here = [pool[p * blocks + b] for b in range(blocks)]
            at = self.stage + p

            def pick(ahead, c):
                which = self.sel[p, (ahead - 1) * 2 + c]
                found = here[blocks - 1]
                for b in range(blocks - 1):
                    found = jnp.where(which == b, here[b], found)
                return found

            to_right[at, 2] = pick(2, 0)
            self.right_ahead(k, p).start()
            to_left[at, 2] = pick(2, 1)
            self.left_ahead(k, p).start()
            to_right[at, 0] = pick(1, 0)
            to_right[at, 1] = pick(1, 1)
            self.right_copy(p).start()
            to_left[at, 0] = pick(3, 0)
            to_left[at, 1] = pick(3, 1)
            self.left_copy(p).start()

        def relay(self, k, p):
            arrived(2, self.recv.at[k])
            self.right_relay(p).start()
            self.left_relay(p).start()

    routes = (Route(0), Route(1))

    half = width // 2

    def w_ring(side):
        peer = x_right if side == 0 else x_left
        return remote(wall.at[tp], wall.at[tp], w_send, w_recv.at[side], (kv, peer))

    def w_half(side):
        origin = x_left if side == 0 else x_right
        peer = x_right if side == 0 else x_left
        piece = wall.at[origin, pl.ds(side * half, half)]
        return remote(piece, piece, w_send, w_recv.at[2], (kv, peer))

    def w_arrived(size, sem):
        at = wall.at[pl.ds(0, size)]
        remote(at, at, w_send, sem, (kv, partner)).wait_recv()

    def w_pair(which):
        far = ((x + 2) % nx) * 2 + core
        owner = (tp, x_left, x_right, far)[which]
        return remote(wall.at[owner], wall.at[owner], w_send, w_recv.at[3], (kv, partner))

    def w_first():
        w_ring(0).wait_recv()
        w_half(0).start()
        w_pair(1).start()
        w_ring(1).wait_recv()
        w_half(1).start()
        w_pair(2).start()

    def w_second():
        w_arrived(1, w_recv.at[2])
        w_pair(3).start()

    q_copy = remote(q_ref, q_far, help_send.at[0], help_recv.at[0], (mirror, tp))
    o_copy = remote(help_out, help_in, help_send.at[1], help_recv.at[1], (mirror, tp))
    log_copy = remote(help_log_out, help_log_in, help_send.at[2], help_recv.at[2], (mirror, tp))
    helper = last_far >= 0
    helped = mirror_z <= ups - 2

    loads[0].wait()
    loads[1].wait()
    cos_part, sin_part = cos_ref[...], sin_ref[...]
    keys = jnp.dot(tokens_ref[...], wk_ref[...], preferred_element_type=jnp.float32)
    keys = turn(keys, cos_part, sin_part).astype(jnp.bfloat16)
    pool[pl.ds(z * blocks, blocks), :, :width] = keys.reshape(blocks, BLK, width)
    loads[2].wait()
    values = jnp.dot(tokens_ref[...], wv_ref[...], preferred_element_type=jnp.float32)
    values = values.astype(jnp.bfloat16)
    pool[pl.ds(z * blocks, blocks), :, width:] = values.reshape(blocks, BLK, width)

    pl.semaphore_wait(barrier, 5 + ntp - 1)

    @pl.when(z < nz - 1)
    def _():
        for b in range(blocks):
            up_copy(0, b).start()

    goes_down = (z >= 1) & (z <= ups - 2)

    @pl.when(goes_down)
    def _():
        for b in range(parts):
            down_copy(0, b).start()

    for copy in to_smem:
        copy.wait()
    pl.when(z <= last_far)(lambda: routes[1].exchange(0, z))
    routes[0].exchange(0, z)
    loads[4].wait()
    query = jnp.dot(tokens_ref[...], wq_ref[...], preferred_element_type=jnp.float32)
    query = turn(query, cos_part, sin_part).astype(jnp.bfloat16).astype(jnp.float32)
    q_ref[...] = (query * HEAD_DIM ** (-0.5)).astype(jnp.bfloat16)
    pl.when(helped)(lambda: q_copy.start())
    loads[3].wait()
    w_ring(0).start()
    w_ring(1).start()
    w_pair(0).start()

    def own_there(k):
        return z - k >= 0

    def far_below(k):
        return (z - k >= 0) & (z - k <= last_far)

    def far_above(step):
        return z + 1 + step <= last_far

    def relay_step(k):
        pl.when(far_below(k))(lambda: routes[1].relay(k, z - k))
        if 1 <= k <= ups - 2:
            pl.when(far_above(k - 1))(lambda: routes[1].relay(ups + k - 1, z + k))
        pl.when(own_there(k))(lambda: routes[0].relay(k, z - k))

    for step in range(ups):
        k = step + 1

        @pl.when(own_there(k))
        def _():
            for b in range(blocks):
                remote(pool.at[b], pool.at[b], z_send, up_recv.at[step * blocks + b], (up, tp)).wait_recv()
                if step + 1 < ups:
                    pl.when(z < nz - 1)(lambda: up_copy(step + 1, b).start())
            pl.when(z - k <= last_far)(lambda: routes[1].exchange(k, z - k))
            routes[0].exchange(k, z - k)

        if step <= ups - 3:

            @pl.when(z + 1 + step <= ups - 2)
            def _():
                for b in range(parts):
                    arrived(part, down_recv.at[step * parts + b])

                    if step <= ups - 4:

                        @pl.when(z >= 1)
                        def _():
                            down_copy(step + 1, b).start()

                pl.when(far_above(step))(lambda: routes[1].exchange(ups + step, z + k))

        if step == 3:
            w_first()
        if step == 5:
            w_second()
        if step >= 1:
            relay_step(step - 1)
    relay_step(ups - 1)
    relay_step(ups)

    def plane_counts(c):
        own = min(c, ups) + 1
        far = max(0, ups - 1 - c)
        ups_sent = min(c, ups - 1) + 1 if c < nz - 1 else 0
        downs_sent = ups - 1 - c if 1 <= c <= ups - 2 else 0
        return own, far, (ups_sent + downs_sent) * blocks

    lane = lax.broadcasted_iota(jnp.int32, (BLK, width), 1)
    wide_lane = lax.broadcasted_iota(jnp.int32, (heads * BLK, width), 1)
    wide_row = lax.broadcasted_iota(jnp.int32, (heads * BLK, width), 0)
    eye = lax.broadcasted_iota(jnp.int32, (heads * BLK, heads * BLK), 0) == lax.broadcasted_iota(
        jnp.int32, (heads * BLK, heads * BLK), 1
    )
    key_block = lax.broadcasted_iota(jnp.int32, (1, SEL * BLK), 1) // BLK

    def by_head(stacked):
        result = stacked[:BLK]
        for head in range(1, heads):
            result = jnp.where(lane // HEAD_DIM == head, stacked[head * BLK : (head + 1) * BLK], result)
        return result

    def attention(i, queries, places, along, dest, low, high):
        for j in range(SEL):
            n = i * SEL + j
            picked[i, j * BLK : (j + 1) * BLK, :] = jnp.where(
                places[2, n] > 0, pool[places[0, n]], along[places[1, n]]
            )
        rows_here = queries[i * BLK : (i + 1) * BLK, :].astype(jnp.float32)
        stacked = jnp.concatenate([rows_here] * heads, axis=0)
        stacked = jnp.where(wide_lane // HEAD_DIM == wide_row // BLK, stacked, 0.0)
        scores = lax.dot_general(
            stacked.astype(jnp.bfloat16),
            picked[i, :, :width],
            (((1,), (1,)), ((), ())),
            preferred_element_type=jnp.float32,
        )
        listed = chosen_ref[pl.ds(dest * blocks + i, 1), :]
        block_of = jnp.zeros((1, SEL * BLK), jnp.int32)
        for j in range(SEL):
            block_of = jnp.where(key_block == j, listed[:, j : j + 1], block_of)
        scores = jnp.where((block_of >= low) & (block_of < high), scores, MASKED)
        top = jnp.max(scores, axis=1, keepdims=True)
        weights = jnp.exp(scores - top)
        total = jnp.sum(weights, axis=1, keepdims=True)
        summed = jnp.dot(
            weights.astype(jnp.bfloat16), picked[i, :, width:], preferred_element_type=jnp.float32
        )
        return by_head(summed / total), top + jnp.log(total)

    first = jnp.maximum(z - ups, 0) * NY * blocks

    def own_attention():
        for c in range(nz):
            pl.when(z == c)(lambda: arrived(6 * plane_counts(c)[0], relay_recv.at[0]))
        for i in range(blocks):
            result, column = attention(i, q_ref, idx_ref, own_pool, kv, first, nz * NY * blocks)
            mixed_ref[i * BLK : (i + 1) * BLK, :] = result
            wide_ref[i * BLK : (i + 1) * BLK, :] = by_head(
                jnp.broadcast_to(column, (heads * BLK, width))
            )

    def part_copy(to):
        src = att.at[pl.ds(to * rows, rows)]
        dst = abuf.at[:, pl.ds(pl.multiple_of(tp * width, width), width)]
        return remote(src, dst, a_send, a_recv, (kv, to))

    def emit():
        per_block = ntp // blocks
        for i in range(blocks):
            at = slice(i * BLK, (i + 1) * BLK)
            att[at, :] = mixed_ref[at, :].astype(jnp.bfloat16)
            for to in range(i * per_block, (i + 1) * per_block):

                @pl.when(to != tp)
                def _():
                    part_copy(to).start()

                @pl.when(to == tp)
                def _():
                    abuf[:, pl.ds(pl.multiple_of(tp * width, width), width)] = att[
                        to * rows : (to + 1) * rows, :
                    ]

        for head in range(heads):
            cols = slice(head * HEAD_DIM, (head + 1) * HEAD_DIM)
            lse_ref[head : head + 1, :] = jnp.concatenate(
                [
                    jnp.sum(
                        jnp.where(
                            eye[:BLK, :HEAD_DIM], wide_ref[i * BLK : (i + 1) * BLK, cols], 0.0
                        ),
                        axis=0,
                        keepdims=True,
                    )
                    for i in range(blocks)
                ],
                axis=1,
            )

    early = z <= 1

    @pl.when(early)
    def _():
        own_attention()
        emit()

    @pl.when(helper)
    def _():
        for c in range(ups - 1):

            @pl.when(z == c)
            def _():
                arrived(6 * plane_counts(c)[1], relay_recv.at[1])

        q_copy.wait_recv()
        help_log_out[...] = jnp.zeros(help_log_out.shape, jnp.float32)
        limit = (last_far + 1) * NY * blocks
        for i in range(blocks):
            result, column = attention(i, q_far, far_idx_ref, far_pool, mirror, 0, limit)
            help_out[i * BLK : (i + 1) * BLK, :] = result.astype(jnp.bfloat16)
            help_log_out[i : i + 1, :] = jnp.sum(jnp.where(eye, column, 0.0), axis=0, keepdims=True)
        o_copy.start()
        log_copy.start()

    pl.when(z > 1)(own_attention)

    @pl.when(helped)
    def _():
        o_copy.wait_recv()
        log_copy.wait_recv()
        for i in range(blocks):
            at = slice(i * BLK, (i + 1) * BLK)
            row = jnp.broadcast_to(help_log_in[i : i + 1, :], (heads * BLK, width))
            column = jnp.sum(jnp.where(eye, row, 0.0), axis=1, keepdims=True)
            theirs = by_head(jnp.broadcast_to(column, (heads * BLK, width)))
            mine = wide_ref[at, :]
            top = jnp.maximum(mine, theirs)
            share, other = jnp.exp(mine - top), jnp.exp(theirs - top)
            total = share + other
            extra = help_in[at, :].astype(jnp.float32)
            mixed_ref[at, :] = (mixed_ref[at, :] * share + extra * other) / total
            wide_ref[at, :] = top + jnp.log(total)

    pl.when(z > 1)(emit)

    for c in range(nz):

        @pl.when(z == c)
        def _():
            own, far, sent = plane_counts(c)
            left_off(8 * (own + far), y_send)
            if sent:
                left_off(sent, z_send)

    @pl.when(helper)
    def _():
        o_copy.wait_send()
        log_copy.wait_send()

    pl.when(helped)(lambda: q_copy.wait_send())
    w_arrived(4, w_recv.at[3])
    sent_w = wall.at[pl.ds(0, ntp - 1)]
    remote(sent_w, sent_w, w_send, w_recv.at[3], (kv, partner)).wait_send()
    others = abuf.at[:, pl.ds(0, (ntp - 1) * width)]
    remote(others, others, a_send, a_recv, (kv, partner)).wait()
    total_width = out_ref.shape[1]
    chunk = min(512, total_width)
    for c in range(total_width // chunk):
        cols = slice(c * chunk, (c + 1) * chunk)
        acc = jnp.zeros((rows, chunk), jnp.float32)
        for t in range(ntp):
            acc += jnp.dot(
                abuf[:, t * width : (t + 1) * width],
                wall[t, :, cols],
                preferred_element_type=jnp.float32,
            )
        out_ref[:, cols] = acc.astype(jnp.bfloat16)


def finish(mixed_ref, log_ref, mixed_out, log_out, sem):
    first = pltpu.make_async_copy(mixed_ref, mixed_out, sem.at[0])
    second = pltpu.make_async_copy(log_ref, log_out, sem.at[1])
    first.start()
    second.start()
    first.wait()
    second.wait()


def local(nkv, ntp, tokens, w_query, w_key, w_value, w_out, chosen):
    local_rows = tokens.shape[0]
    width = w_query.shape[1]
    heads = width // HEAD_DIM
    blocks = local_rows // BLK
    nz = nkv // NY
    device = lax.axis_index("kv")
    vmem = pl.BlockSpec(memory_space=pltpu.VMEM)
    hbm = pl.BlockSpec(memory_space=pltpu.HBM)
    cos_piece, sin_piece = rotary_pieces(device * local_rows, width)
    ups = nz // 2
    out_rows = local_rows // ntp
    dma = pltpu.SemaphoreType.DMA
    stage = (nz + ups, 3, BLK, 2 * width)
    bf16, f32, i32 = jnp.bfloat16, jnp.float32, jnp.int32
    mixed, log_sums = pl.pallas_call(
        functools.partial(attend, nz, ntp),
        out_shape=(
            jax.ShapeDtypeStruct((out_rows, w_out.shape[1]), bf16),
            jax.ShapeDtypeStruct((heads, local_rows), f32),
        ),
        in_specs=[hbm] * 6 + [vmem] * 2,
        out_specs=(vmem, vmem),
        scratch_shapes=[
            pltpu.VMEM(tokens.shape, bf16),
            pltpu.VMEM(w_query.shape, bf16),
            pltpu.VMEM(w_key.shape, bf16),
            pltpu.VMEM(w_value.shape, bf16),
            pltpu.VMEM((local_rows, width), bf16),
            pltpu.VMEM((local_rows, width), bf16),
            pltpu.VMEM((SEL, chosen.shape[0]), i32),
            pltpu.VMEM((chosen.shape[0], SEL), i32),
            pltpu.VMEM((local_rows, width), f32),
            pltpu.VMEM((local_rows, width), f32),
            pltpu.VMEM((4, nz, 128), i32),
            pltpu.SMEM((nz, 128), i32),
            pltpu.SMEM((8, 128), i32),
            pltpu.SMEM((nz, 128), i32),
            pltpu.SMEM((8, 128), i32),
            pltpu.VMEM((nz * blocks, BLK, 2 * width), bf16),
            pltpu.VMEM((nz * 8, BLK, 2 * width), bf16),
            pltpu.VMEM((ups * 8, BLK, 2 * width), bf16),
            pltpu.VMEM(stage, bf16),
            pltpu.VMEM(stage, bf16),
            pltpu.VMEM((blocks, SEL * BLK, 2 * width), bf16),
            pltpu.VMEM((ntp, width, w_out.shape[1]), bf16),
            pltpu.VMEM((local_rows, width), f32),
            pltpu.VMEM((local_rows, width), f32),
            pltpu.VMEM((local_rows, width), bf16),
            pltpu.VMEM((8, heads * BLK), f32),
            pltpu.VMEM((local_rows, width), bf16),
            pltpu.VMEM((8, heads * BLK), f32),
            pltpu.VMEM((local_rows, width), bf16),
            pltpu.VMEM((out_rows, ntp * width), bf16),
            dma((9,)),
            dma,
            dma((blocks * ups,)),
            dma((blocks * (ups - 2),)),
            dma,
            dma((ups + 1,)),
            dma((2 * ups - 2,)),
            dma((2,)),
            dma,
            dma((4,)),
            dma((3,)),
            dma((3,)),
            dma,
            dma,
        ],
        compiler_params=pltpu.CompilerParams(
            collective_id=0, has_side_effects=True, vmem_limit_bytes=55000 * 1024
        ),
    )(tokens, w_query, w_key, w_value, w_out, chosen.T, cos_piece, sin_piece)
    return pl.pallas_call(
        finish,
        out_shape=(
            jax.ShapeDtypeStruct(mixed.shape, mixed.dtype),
            jax.ShapeDtypeStruct(log_sums.shape, log_sums.dtype),
        ),
        in_specs=[vmem, vmem],
        out_specs=(hbm, hbm),
        scratch_shapes=[dma((2,))],
        compiler_params=pltpu.CompilerParams(vmem_limit_bytes=1024 * 1024),
    )(mixed, log_sums)


def solution(mesh):
    placed = (P("kv", None), P(None, "tp"), P(None, "tp"), P(None, "tp"), P("tp", None), P())
    return jax.shard_map(
        functools.partial(local, mesh.shape["kv"], mesh.shape["tp"]),
        mesh=mesh,
        in_specs=placed,
        out_specs=(P(("kv", "tp"), None), P("tp", "kv")),
        check_vma=False,
    )
```

```python
import functools

import jax
import jax.numpy as jnp
from jax import lax
from jax.experimental import pallas as pl
from jax.experimental.pallas import tpu as pltpu
from jax.sharding import PartitionSpec as P

HEAD_DIM = 64
BLK = 64
SEL = 16
NY = 4
ROTARY_BASE = 500000.0
MASKED = -1e30
MESH = pl.DeviceIdType.MESH


def rotary_pieces(first, width):
    half = HEAD_DIM // 2
    lane = jnp.arange(width)
    inverse = ROTARY_BASE ** (-(lane % half).astype(jnp.float32) / half)
    row = jnp.arange(40)
    position = jnp.where(row < 16, 16 * row, jnp.where(row < 32, row - 16, first))
    angles = position.astype(jnp.float32)[:, None] * inverse[None, :]
    return jnp.cos(angles), jnp.sin(angles)


def rotary_tables(cos_piece, sin_piece, cos_ref, sin_ref):
    half = HEAD_DIM // 2
    cos_first, sin_first = cos_piece[32:33, :], sin_piece[32:33, :]
    cos_tens, sin_tens = cos_piece[:16, :], sin_piece[:16, :]
    cos_ones, sin_ones = cos_piece[16:32, :], sin_piece[16:32, :]
    lane = lax.broadcasted_iota(jnp.int32, cos_ones.shape, 1)
    sign = jnp.where(lane % HEAD_DIM < half, -1.0, 1.0)
    cos_row = cos_first * cos_tens - sin_first * sin_tens
    sin_row = sin_first * cos_tens + cos_first * sin_tens
    for t in range(cos_ref.shape[0] // 16):
        c, n = cos_row[t : t + 1, :], sin_row[t : t + 1, :]
        cos_ref[t * 16 : (t + 1) * 16, :] = c * cos_ones - n * sin_ones
        sin_ref[t * 16 : (t + 1) * 16, :] = (n * cos_ones + c * sin_ones) * sign


def turn(values, cos_part, sin_part):
    width = values.shape[1]
    half = HEAD_DIM // 2
    lane = lax.broadcasted_iota(jnp.int32, values.shape, 1)
    ahead = pltpu.roll(values, width - half, 1)
    behind = pltpu.roll(values, half, 1)
    partner = jnp.where(lane % HEAD_DIM < half, ahead, behind)
    return values * cos_part + partner * sin_part


def make_tables(nz, blocks, kv, dest_z, low, high, planes, chosen_ref, table, at):
    z, y = kv // NY, kv % NY
    lane = lax.broadcasted_iota(jnp.int32, table.shape[1:], 1)
    found = jnp.zeros(table.shape[1:], jnp.int32)
    target = lax.broadcasted_iota(jnp.int32, (nz, SEL), 0) * (NY * blocks) + y * blocks
    for ahead in range(1, NY):
        dest = dest_z * NY + (y + ahead) % NY
        rows = [chosen_ref[pl.ds(dest * blocks + r, 1), :] for r in range(blocks)]
        least = jnp.full((nz, 1), blocks - 1, jnp.int32)
        most = jnp.zeros((nz, 1), jnp.int32)
        hits = []
        for b in range(blocks):
            hit = jnp.zeros((nz, SEL), jnp.int32)
            for entries in rows:
                hit = jnp.where(entries == target + b, 1, hit)
            hits.append(jnp.max(hit, axis=1, keepdims=True))
        for b in range(blocks):
            most = jnp.where(hits[b] > 0, b, most)
            least = jnp.where(hits[blocks - 1 - b] > 0, blocks - 1 - b, least)
        found = jnp.where(lane == (ahead - 1) * 2, least, found)
        found = jnp.where(lane == (ahead - 1) * 2 + 1, most, found)
    table[at] = found
    size = blocks * SEL
    first_row = (dest_z * NY + y) * blocks
    mine = jnp.concatenate([chosen_ref[pl.ds(first_row + r, 1), :] for r in range(blocks)], axis=1)
    across = jnp.broadcast_to(mine, (size, size))
    diagonal = lax.broadcasted_iota(jnp.int32, (size, size), 0) == lax.broadcasted_iota(
        jnp.int32, (size, size), 1
    )
    down = jnp.sum(jnp.where(diagonal, across, 0), axis=1, keepdims=True)
    lower = (down // blocks == across // blocks) & (down >= 0) & (down < across)
    second = jnp.max(jnp.where(lower, 1, 0), axis=0, keepdims=True)
    source = jnp.maximum(mine, 0) // blocks
    from_z, ahead = source // NY, (source % NY - y + NY) % NY
    served = (mine >= 0) & (from_z >= low) & (from_z <= high)
    here = (ahead == 0) | (served == False)
    column = jnp.where(served, from_z * blocks + jnp.maximum(mine, 0) % blocks, z * blocks)
    column = jnp.where(here, column, 0)
    along = jnp.where(
        ahead == NY - 1,
        3 * from_z + second,
        jnp.where(
            ahead == 1,
            3 * planes + 3 * from_z + second,
            6 * planes + second * planes + from_z,
        ),
    )
    along = jnp.where(here, 0, along)
    blank = jnp.zeros((1, table.shape[2] - size), jnp.int32)
    full = [jnp.concatenate([v, blank], axis=1) for v in (column, along, here.astype(jnp.int32))]
    row = lax.broadcasted_iota(jnp.int32, table.shape[1:], 0)
    table[at + 1] = jnp.where(row == 0, full[0], jnp.where(row == 1, full[1], full[2]))


def attend(
    nz,
    ntp,
    tokens_hbm,
    wq_hbm,
    wk_hbm,
    wv_hbm,
    w_hbm,
    chosen_hbm,
    cos_piece,
    sin_piece,
    out_ref,
    lse_ref,
    tokens_ref,
    wq_ref,
    wkv_ref,
    q_ref,
    q_far,
    chosen_across,
    chosen_ref,
    cos_ref,
    sin_ref,
    table,
    sel_ref,
    idx_ref,
    far_sel_ref,
    far_idx_ref,
    pool,
    own_pool,
    far_pool,
    to_right,
    to_left,
    picked,
    wall,
    mixed_ref,
    wide_ref,
    help_out,
    help_log_out,
    help_in,
    help_log_in,
    att,
    abuf,
    local_sem,
    z_send,
    up_recv,
    down_recv,
    y_send,
    y_recv,
    far_recv,
    relay_recv,
    w_send,
    w_recv,
    help_send,
    help_recv,
    a_send,
    a_recv,
):
    kv = lax.axis_index("kv")
    tp = lax.axis_index("tp")
    z, y = kv // NY, kv % NY
    nx = ntp // 2
    x, core = tp // 2, tp % 2
    up = ((z + 1) % nz) * NY + y
    down = ((z + nz - 1) % nz) * NY + y
    outer, place_in = (z // 4 + 1) // 2 % 2, z % 4
    mirror_z = (3 - z // 4) * 4
    mirror_z += outer * (3 - place_in) + (1 - outer) * (place_in + 1 - 2 * (place_in % 2))
    mirror = mirror_z * NY + y
    right = z * NY + (y + 1) % NY
    left = z * NY + (y + NY - 1) % NY
    x_right = ((x + 1) % nx) * 2 + core
    x_left = ((x + nx - 1) % nx) * 2 + core
    partner = x * 2 + (1 - core)
    width = wq_ref.shape[1]
    blocks = att.shape[0] // BLK
    heads = width // HEAD_DIM
    rows = att.shape[0] // ntp
    ups = nz // 2
    last_far = mirror_z - ups - 1

    def load(which, src, dst):
        return pltpu.make_async_copy(src, dst, local_sem.at[which])

    loads = [
        load(0, tokens_hbm, tokens_ref),
        load(1, wk_hbm, wkv_ref.at[:, pl.ds(0, width)]),
        load(2, wv_hbm, wkv_ref.at[:, pl.ds(width, width)]),
        load(3, w_hbm, wall.at[tp]),
        load(4, wq_hbm, wq_ref),
    ]
    listing = load(5, chosen_hbm, chosen_across)
    listing.start()
    for copy in loads:
        copy.start()

    barrier = pltpu.get_barrier_semaphore()
    for peer in (mirror, up, down, right, left):
        pl.semaphore_signal(barrier, inc=1, device_id=(peer, tp), device_id_type=MESH)
    for step in range(1, ntp):
        pl.semaphore_signal(barrier, inc=1, device_id=(kv, (tp + step) % ntp), device_id_type=MESH)
    rotary_tables(cos_piece, sin_piece, cos_ref, sin_ref)
    listing.wait()
    chosen_ref[...] = jnp.transpose(chosen_across[...])
    make_tables(nz, blocks, kv, z, z - ups, nz, nz, chosen_ref, table, 0)
    make_tables(nz, blocks, kv, mirror_z, 0, last_far, nz // 2, chosen_ref, table, 2)
    to_smem = [
        load(5, table.at[0], sel_ref),
        load(6, table.at[1, pl.ds(0, 8)], idx_ref),
        load(7, table.at[2], far_sel_ref),
        load(8, table.at[3, pl.ds(0, 8)], far_idx_ref),
    ]
    for copy in to_smem:
        copy.start()

    def remote(src, dst, send, recv, device):
        return pltpu.make_async_remote_copy(
            src_ref=src,
            dst_ref=dst,
            send_sem=send,
            recv_sem=recv,
            device_id=device,
            device_id_type=MESH,
        )

    part = 1
    parts = blocks

    def up_copy(step, b):
        at = pool.at[(z + nz - step) % nz * blocks + b // 2, pl.ds(b % 2 * (BLK // 2), BLK // 2)]
        return remote(at, at, z_send, up_recv.at[step * 2 * blocks + b], (up, tp))

    def down_copy(step, b):
        at = pool.at[pl.ds((z + step) % nz * blocks + b, 1)]
        return remote(at, at, z_send, down_recv.at[step * parts + b], (down, tp))

    def stretch(size):
        return own_pool.at[pl.ds(0, size)]

    def arrived(size, sem):
        remote(stretch(size), stretch(size), z_send, sem, (up, tp)).wait_recv()

    def left_off(size, sem):
        remote(stretch(size), stretch(size), sem, relay_recv.at[0], (up, tp)).wait_send()

    class Route:
        def __init__(self, kind):
            self.kind = kind
            self.pool = (own_pool, far_pool)[kind]
            self.planes = (nz, nz // 2)[kind]
            self.stage = (0, nz)[kind]
            self.sel = (sel_ref, far_sel_ref)[kind]
            self.recv = (y_recv, far_recv)[kind]

        def right_copy(self, p):
            src, dst = to_right.at[self.stage + p, pl.ds(0, 2)], self.pool.at[pl.ds(3 * p, 2)]
            return remote(src, dst, y_send, relay_recv.at[self.kind], (right, tp))

        def left_copy(self, p):
            src = to_left.at[self.stage + p, pl.ds(0, 2)]
            dst = self.pool.at[pl.ds(3 * self.planes + 3 * p, 2)]
            return remote(src, dst, y_send, relay_recv.at[self.kind], (left, tp))

        def right_ahead(self, k, p):
            src, dst = to_right.at[self.stage + p, 2], self.pool.at[3 * p + 2]
            return remote(src, dst, y_send, self.recv.at[k], (right, tp))

        def left_ahead(self, k, p):
            src, dst = to_left.at[self.stage + p, 2], self.pool.at[3 * self.planes + 3 * p + 2]
            return remote(src, dst, y_send, self.recv.at[k], (left, tp))

        def right_relay(self, p):
            src = self.pool.at[3 * p + 2]
            dst = self.pool.at[6 * self.planes + p]
            return remote(src, dst, y_send, relay_recv.at[self.kind], (right, tp))

        def left_relay(self, p):
            src = self.pool.at[3 * self.planes + 3 * p + 2]
            dst = self.pool.at[7 * self.planes + p]
            return remote(src, dst, y_send, relay_recv.at[self.kind], (left, tp))

        def exchange(self, k, p):
            here = [pool[p * blocks + b] for b in range(blocks)]
            at = self.stage + p

            def pick(ahead, c):
                which = self.sel[p, (ahead - 1) * 2 + c]
                found = here[blocks - 1]
                for b in range(blocks - 1):
                    found = jnp.where(which == b, here[b], found)
                return found

            to_right[at, 2] = pick(2, 0)
            self.right_ahead(k, p).start()
            to_left[at, 2] = pick(2, 1)
            self.left_ahead(k, p).start()
            to_right[at, 0] = pick(1, 0)
            to_right[at, 1] = pick(1, 1)
            self.right_copy(p).start()
            to_left[at, 0] = pick(3, 0)
            to_left[at, 1] = pick(3, 1)
            self.left_copy(p).start()

        def relay(self, k, p):
            arrived(2, self.recv.at[k])
            self.right_relay(p).start()
            self.left_relay(p).start()

    routes = (Route(0), Route(1))

    half = width // 2

    def w_ring(side):
        peer = x_right if side == 0 else x_left
        return remote(wall.at[tp], wall.at[tp], w_send, w_recv.at[side], (kv, peer))

    def w_half(side):
        origin = x_left if side == 0 else x_right
        peer = x_right if side == 0 else x_left
        piece = wall.at[origin, pl.ds(side * half, half)]
        return remote(piece, piece, w_send, w_recv.at[2], (kv, peer))

    def w_arrived(size, sem):
        at = wall.at[pl.ds(0, size)]
        remote(at, at, w_send, sem, (kv, partner)).wait_recv()

    def w_pair(which):
        far = ((x + 2) % nx) * 2 + core
        owner = (tp, x_left, x_right, far)[which]
        return remote(wall.at[owner], wall.at[owner], w_send, w_recv.at[3], (kv, partner))

    def w_first():
        w_ring(0).wait_recv()
        w_half(0).start()
        w_pair(1).start()
        w_ring(1).wait_recv()
        w_half(1).start()
        w_pair(2).start()

    def w_second():
        w_arrived(1, w_recv.at[2])
        w_pair(3).start()

    q_copy = remote(q_ref, q_far, help_send.at[0], help_recv.at[0], (mirror, tp))
    o_copy = remote(help_out, help_in, help_send.at[1], help_recv.at[1], (mirror, tp))
    log_copy = remote(help_log_out, help_log_in, help_send.at[2], help_recv.at[2], (mirror, tp))
    helper = last_far >= 0
    helped = z >= ups + 1

    loads[0].wait()
    loads[1].wait()
    cos_part, sin_part = cos_ref[...], sin_ref[...]
    loads[2].wait()
    both = jnp.dot(tokens_ref[...], wkv_ref[...], preferred_element_type=jnp.float32)
    keys = turn(both[:, :width], cos_part, sin_part).astype(jnp.bfloat16)
    pool[pl.ds(z * blocks, blocks), :, :width] = keys.reshape(blocks, BLK, width)
    values = both[:, width:].astype(jnp.bfloat16)
    pool[pl.ds(z * blocks, blocks), :, width:] = values.reshape(blocks, BLK, width)
    pl.semaphore_wait(barrier, 5 + ntp - 1)

    @pl.when(z < nz - 1)
    def _():
        for b in range(2 * blocks):
            up_copy(0, b).start()

    def from_above(r, p):
        return (p > r) & ((p <= 4) | ((r >= 2) & (p <= 6)))

    goes_down = (z >= 1) & (z <= 6)

    @pl.when(goes_down)
    def _():
        for b in range(parts):
            down_copy(0, b).start()

    for copy in to_smem:
        copy.wait()
    pl.when(z <= last_far)(lambda: routes[1].exchange(0, z))
    routes[0].exchange(0, z)
    loads[4].wait()
    query = jnp.dot(tokens_ref[...], wq_ref[...], preferred_element_type=jnp.float32)
    query = turn(query, cos_part, sin_part).astype(jnp.bfloat16).astype(jnp.float32)
    q_ref[...] = (query * HEAD_DIM ** (-0.5)).astype(jnp.bfloat16)
    pl.when(helped)(lambda: q_copy.start())
    loads[3].wait()
    w_ring(0).start()
    w_ring(1).start()
    w_pair(0).start()

    def own_there(k):
        return z - k >= 0

    def far_below(k):
        return (z - k >= 0) & (z - k <= last_far)

    def far_above(step):
        return z + 1 + step <= last_far

    def relay_step(k):
        pl.when(far_below(k))(lambda: routes[1].relay(k, z - k))
        if 1 <= k <= 4:
            pl.when(far_above(k - 1))(lambda: routes[1].relay(ups + k - 1, z + k))
        pl.when(own_there(k))(lambda: routes[0].relay(k, z - k))

    for step in range(ups):
        k = step + 1

        @pl.when(own_there(k))
        def _():
            for b in range(2 * blocks):
                up_copy(step, b).wait_recv()
                if step + 1 < ups:
                    pl.when(z < nz - 1)(lambda: up_copy(step + 1, b).start())
            pl.when(z - k <= last_far)(lambda: routes[1].exchange(k, z - k))
            routes[0].exchange(k, z - k)

        if step <= 3:

            @pl.when((z <= 5) & from_above(z, z + 1 + step))
            def _():
                for b in range(parts):
                    arrived(part, down_recv.at[step * parts + b])

                    if step <= 2:

                        @pl.when((z >= 1) & from_above(z - 1, z + 1 + step))
                        def _():
                            down_copy(step + 1, b).start()

                pl.when(far_above(step))(lambda: routes[1].exchange(ups + step, z + k))

        if step == 3:
            w_first()
        if step == 5:
            w_second()
        if step >= 2:
            relay_step(step - 2)
    relay_step(6)
    relay_step(7)
    relay_step(8)


    def plane_counts(c):
        own = min(c, ups) + 1
        far = (5, 4, 7, 6, 3, 2, 1)[c] if c <= 6 else 0
        ups_sent = min(c, ups - 1) + 1 if c < nz - 1 else 0
        downs_sent = (0, 4, 3, 4, 3, 2, 1)[c] if c <= 6 else 0
        return own, far, (ups_sent + downs_sent) * blocks

    lane = lax.broadcasted_iota(jnp.int32, (BLK, width), 1)
    wide_lane = lax.broadcasted_iota(jnp.int32, (heads * BLK, width), 1)
    wide_row = lax.broadcasted_iota(jnp.int32, (heads * BLK, width), 0)
    eye = lax.broadcasted_iota(jnp.int32, (heads * BLK, heads * BLK), 0) == lax.broadcasted_iota(
        jnp.int32, (heads * BLK, heads * BLK), 1
    )
    key_block = lax.broadcasted_iota(jnp.int32, (1, SEL * BLK), 1) // BLK

    def by_head(stacked):
        result = stacked[:BLK]
        for head in range(1, heads):
            result = jnp.where(lane // HEAD_DIM == head, stacked[head * BLK : (head + 1) * BLK], result)
        return result

    def attention(i, queries, places, along, dest, low, high):
        for j in range(SEL):
            n = i * SEL + j
            picked[i, j * BLK : (j + 1) * BLK, :] = jnp.where(
                places[2, n] > 0, pool[places[0, n]], along[places[1, n]]
            )
        rows_here = queries[i * BLK : (i + 1) * BLK, :].astype(jnp.float32)
        stacked = jnp.concatenate([rows_here] * heads, axis=0)
        stacked = jnp.where(wide_lane // HEAD_DIM == wide_row // BLK, stacked, 0.0)
        scores = lax.dot_general(
            stacked.astype(jnp.bfloat16),
            picked[i, :, :width],
            (((1,), (1,)), ((), ())),
            preferred_element_type=jnp.float32,
        )
        listed = chosen_ref[pl.ds(dest * blocks + i, 1), :]
        block_of = jnp.zeros((1, SEL * BLK), jnp.int32)
        for j in range(SEL):
            block_of = jnp.where(key_block == j, listed[:, j : j + 1], block_of)
        scores = jnp.where((block_of >= low) & (block_of < high), scores, MASKED)
        top = jnp.max(scores, axis=1, keepdims=True)
        weights = jnp.exp(scores - top)
        total = jnp.sum(weights, axis=1, keepdims=True)
        summed = jnp.dot(
            weights.astype(jnp.bfloat16), picked[i, :, width:], preferred_element_type=jnp.float32
        )
        return by_head(summed / total), top + jnp.log(total)

    first = jnp.maximum(z - ups, 0) * NY * blocks

    def own_attention():
        for c in range(nz):
            pl.when(z == c)(lambda: arrived(6 * plane_counts(c)[0], relay_recv.at[0]))
        for i in range(blocks):
            result, column = attention(i, q_ref, idx_ref, own_pool, kv, first, nz * NY * blocks)
            mixed_ref[i * BLK : (i + 1) * BLK, :] = result
            wide_ref[i * BLK : (i + 1) * BLK, :] = by_head(
                jnp.broadcast_to(column, (heads * BLK, width))
            )

    def part_copy(to):
        src = att.at[pl.ds(to * rows, rows)]
        dst = abuf.at[:, pl.ds(pl.multiple_of(tp * width, width), width)]
        return remote(src, dst, a_send, a_recv, (kv, to))

    def emit():
        per_block = ntp // blocks
        for i in range(blocks):
            at = slice(i * BLK, (i + 1) * BLK)
            att[at, :] = mixed_ref[at, :].astype(jnp.bfloat16)
            for to in range(i * per_block, (i + 1) * per_block):

                @pl.when(to != tp)
                def _():
                    part_copy(to).start()

                @pl.when(to == tp)
                def _():
                    abuf[:, pl.ds(pl.multiple_of(tp * width, width), width)] = att[
                        to * rows : (to + 1) * rows, :
                    ]

        for head in range(heads):
            cols = slice(head * HEAD_DIM, (head + 1) * HEAD_DIM)
            lse_ref[head : head + 1, :] = jnp.concatenate(
                [
                    jnp.sum(
                        jnp.where(
                            eye[:BLK, :HEAD_DIM], wide_ref[i * BLK : (i + 1) * BLK, cols], 0.0
                        ),
                        axis=0,
                        keepdims=True,
                    )
                    for i in range(blocks)
                ],
                axis=1,
            )

    early = z <= 1

    @pl.when(early)
    def _():
        own_attention()
        emit()

    @pl.when(helper)
    def _():
        for c in range(ups - 1):

            @pl.when(z == c)
            def _():
                arrived(6 * plane_counts(c)[1], relay_recv.at[1])

        q_copy.wait_recv()
        help_log_out[...] = jnp.zeros(help_log_out.shape, jnp.float32)
        limit = (last_far + 1) * NY * blocks
        for i in range(blocks):
            result, column = attention(i, q_far, far_idx_ref, far_pool, mirror, 0, limit)
            help_out[i * BLK : (i + 1) * BLK, :] = result.astype(jnp.bfloat16)
            help_log_out[i : i + 1, :] = jnp.sum(jnp.where(eye, column, 0.0), axis=0, keepdims=True)
        o_copy.start()
        log_copy.start()

    pl.when(z > 1)(own_attention)

    @pl.when(helped)
    def _():
        o_copy.wait_recv()
        log_copy.wait_recv()
        for i in range(blocks):
            at = slice(i * BLK, (i + 1) * BLK)
            row = jnp.broadcast_to(help_log_in[i : i + 1, :], (heads * BLK, width))
            column = jnp.sum(jnp.where(eye, row, 0.0), axis=1, keepdims=True)
            theirs = by_head(jnp.broadcast_to(column, (heads * BLK, width)))
            mine = wide_ref[at, :]
            top = jnp.maximum(mine, theirs)
            share, other = jnp.exp(mine - top), jnp.exp(theirs - top)
            total = share + other
            extra = help_in[at, :].astype(jnp.float32)
            mixed_ref[at, :] = (mixed_ref[at, :] * share + extra * other) / total
            wide_ref[at, :] = top + jnp.log(total)

    pl.when(z > 1)(emit)

    for c in range(nz):

        @pl.when(z == c)
        def _():
            own, far, sent = plane_counts(c)
            left_off(8 * (own + far), y_send)
            if sent:
                left_off(sent, z_send)

    @pl.when(helper)
    def _():
        o_copy.wait_send()
        log_copy.wait_send()

    pl.when(helped)(lambda: q_copy.wait_send())
    w_arrived(4, w_recv.at[3])
    sent_w = wall.at[pl.ds(0, ntp - 1)]
    remote(sent_w, sent_w, w_send, w_recv.at[3], (kv, partner)).wait_send()
    others = abuf.at[:, pl.ds(0, (ntp - 1) * width)]
    remote(others, others, a_send, a_recv, (kv, partner)).wait()
    total_width = out_ref.shape[1]
    chunk = min(512, total_width)
    for c in range(total_width // chunk):
        cols = slice(c * chunk, (c + 1) * chunk)
        acc = jnp.zeros((rows, chunk), jnp.float32)
        for t in range(ntp):
            acc += jnp.dot(
                abuf[:, t * width : (t + 1) * width],
                wall[t, :, cols],
                preferred_element_type=jnp.float32,
            )
        out_ref[:, cols] = acc.astype(jnp.bfloat16)


def finish(mixed_ref, log_ref, mixed_out, log_out, sem):
    first = pltpu.make_async_copy(mixed_ref, mixed_out, sem.at[0])
    second = pltpu.make_async_copy(log_ref, log_out, sem.at[1])
    first.start()
    second.start()
    first.wait()
    second.wait()


def local(nkv, ntp, tokens, w_query, w_key, w_value, w_out, chosen):
    local_rows = tokens.shape[0]
    width = w_query.shape[1]
    heads = width // HEAD_DIM
    blocks = local_rows // BLK
    nz = nkv // NY
    device = lax.axis_index("kv")
    vmem = pl.BlockSpec(memory_space=pltpu.VMEM)
    hbm = pl.BlockSpec(memory_space=pltpu.HBM)
    cos_piece, sin_piece = rotary_pieces(device * local_rows, width)
    ups = nz // 2
    out_rows = local_rows // ntp
    dma = pltpu.SemaphoreType.DMA
    stage = (nz + ups, 3, BLK, 2 * width)
    bf16, f32, i32 = jnp.bfloat16, jnp.float32, jnp.int32
    mixed, log_sums = pl.pallas_call(
        functools.partial(attend, nz, ntp),
        out_shape=(
            jax.ShapeDtypeStruct((out_rows, w_out.shape[1]), bf16),
            jax.ShapeDtypeStruct((heads, local_rows), f32),
        ),
        in_specs=[hbm] * 6 + [vmem] * 2,
        out_specs=(vmem, vmem),
        scratch_shapes=[
            pltpu.VMEM(tokens.shape, bf16),
            pltpu.VMEM(w_query.shape, bf16),
            pltpu.VMEM((w_key.shape[0], 2 * width), bf16),
            pltpu.VMEM((local_rows, width), bf16),
            pltpu.VMEM((local_rows, width), bf16),
            pltpu.VMEM((SEL, chosen.shape[0]), i32),
            pltpu.VMEM((chosen.shape[0], SEL), i32),
            pltpu.VMEM((local_rows, width), f32),
            pltpu.VMEM((local_rows, width), f32),
            pltpu.VMEM((4, nz, 128), i32),
            pltpu.SMEM((nz, 128), i32),
            pltpu.SMEM((8, 128), i32),
            pltpu.SMEM((nz, 128), i32),
            pltpu.SMEM((8, 128), i32),
            pltpu.VMEM((nz * blocks, BLK, 2 * width), bf16),
            pltpu.VMEM((nz * 8, BLK, 2 * width), bf16),
            pltpu.VMEM((ups * 8, BLK, 2 * width), bf16),
            pltpu.VMEM(stage, bf16),
            pltpu.VMEM(stage, bf16),
            pltpu.VMEM((blocks, SEL * BLK, 2 * width), bf16),
            pltpu.VMEM((ntp, width, w_out.shape[1]), bf16),
            pltpu.VMEM((local_rows, width), f32),
            pltpu.VMEM((local_rows, width), f32),
            pltpu.VMEM((local_rows, width), bf16),
            pltpu.VMEM((8, heads * BLK), f32),
            pltpu.VMEM((local_rows, width), bf16),
            pltpu.VMEM((8, heads * BLK), f32),
            pltpu.VMEM((local_rows, width), bf16),
            pltpu.VMEM((out_rows, ntp * width), bf16),
            dma((9,)),
            dma,
            dma((2 * blocks * ups,)),
            dma((blocks * 4,)),
            dma,
            dma((ups + 1,)),
            dma((ups + 4,)),
            dma((2,)),
            dma,
            dma((4,)),
            dma((3,)),
            dma((3,)),
            dma,
            dma,
        ],
        compiler_params=pltpu.CompilerParams(
            collective_id=0, has_side_effects=True, vmem_limit_bytes=55000 * 1024
        ),
    )(tokens, w_query, w_key, w_value, w_out, chosen.T, cos_piece, sin_piece)
    return pl.pallas_call(
        finish,
        out_shape=(
            jax.ShapeDtypeStruct(mixed.shape, mixed.dtype),
            jax.ShapeDtypeStruct(log_sums.shape, log_sums.dtype),
        ),
        in_specs=[vmem, vmem],
        out_specs=(hbm, hbm),
        scratch_shapes=[dma((2,))],
        compiler_params=pltpu.CompilerParams(vmem_limit_bytes=1024 * 1024),
    )(mixed, log_sums)


def solution(mesh):
    placed = (P("kv", None), P(None, "tp"), P(None, "tp"), P(None, "tp"), P("tp", None), P())
    return jax.shard_map(
        functools.partial(local, mesh.shape["kv"], mesh.shape["tp"]),
        mesh=mesh,
        in_specs=placed,
        out_specs=(P(("kv", "tp"), None), P("tp", "kv")),
        check_vma=False,
    )
```

```python
import functools

import jax
import jax.numpy as jnp
from jax import lax
from jax.experimental import pallas as pl
from jax.experimental.pallas import tpu as pltpu
from jax.sharding import PartitionSpec as P

HEAD_DIM = 64
BLK = 64
SEL = 16
NY = 4
ROTARY_BASE = 500000.0
MASKED = -1e30
MESH = pl.DeviceIdType.MESH


def rotary_pieces(first, width):
    half = HEAD_DIM // 2
    lane = jnp.arange(width)
    inverse = ROTARY_BASE ** (-(lane % half).astype(jnp.float32) / half)
    row = jnp.arange(40)
    position = jnp.where(row < 16, 16 * row, jnp.where(row < 32, row - 16, first))
    angles = position.astype(jnp.float32)[:, None] * inverse[None, :]
    return jnp.cos(angles), jnp.sin(angles)


def rotary_tables(cos_piece, sin_piece, cos_ref, sin_ref):
    half = HEAD_DIM // 2
    cos_first, sin_first = cos_piece[32:33, :], sin_piece[32:33, :]
    cos_tens, sin_tens = cos_piece[:16, :], sin_piece[:16, :]
    cos_ones, sin_ones = cos_piece[16:32, :], sin_piece[16:32, :]
    lane = lax.broadcasted_iota(jnp.int32, cos_ones.shape, 1)
    sign = jnp.where(lane % HEAD_DIM < half, -1.0, 1.0)
    cos_row = cos_first * cos_tens - sin_first * sin_tens
    sin_row = sin_first * cos_tens + cos_first * sin_tens
    for t in range(cos_ref.shape[0] // 16):
        c, n = cos_row[t : t + 1, :], sin_row[t : t + 1, :]
        cos_ref[t * 16 : (t + 1) * 16, :] = c * cos_ones - n * sin_ones
        sin_ref[t * 16 : (t + 1) * 16, :] = (n * cos_ones + c * sin_ones) * sign


def turn(values, cos_part, sin_part):
    width = values.shape[1]
    half = HEAD_DIM // 2
    lane = lax.broadcasted_iota(jnp.int32, values.shape, 1)
    ahead = pltpu.roll(values, width - half, 1)
    behind = pltpu.roll(values, half, 1)
    partner = jnp.where(lane % HEAD_DIM < half, ahead, behind)
    return values * cos_part + partner * sin_part


def make_tables(nz, blocks, kv, dest_z, low, high, planes, chosen_ref, table, at):
    z, y = kv // NY, kv % NY
    lane = lax.broadcasted_iota(jnp.int32, table.shape[1:], 1)
    found = jnp.zeros(table.shape[1:], jnp.int32)
    target = lax.broadcasted_iota(jnp.int32, (nz, SEL), 0) * (NY * blocks) + y * blocks
    for ahead in range(1, NY):
        dest = dest_z * NY + (y + ahead) % NY
        rows = [chosen_ref[pl.ds(dest * blocks + r, 1), :] for r in range(blocks)]
        least = jnp.full((nz, 1), blocks - 1, jnp.int32)
        most = jnp.zeros((nz, 1), jnp.int32)
        hits = []
        for b in range(blocks):
            hit = jnp.zeros((nz, SEL), jnp.int32)
            for entries in rows:
                hit = jnp.where(entries == target + b, 1, hit)
            hits.append(jnp.max(hit, axis=1, keepdims=True))
        for b in range(blocks):
            most = jnp.where(hits[b] > 0, b, most)
            least = jnp.where(hits[blocks - 1 - b] > 0, blocks - 1 - b, least)
        found = jnp.where(lane == (ahead - 1) * 2, least, found)
        found = jnp.where(lane == (ahead - 1) * 2 + 1, most, found)
    table[at] = found
    size = blocks * SEL
    first_row = (dest_z * NY + y) * blocks
    mine = jnp.concatenate([chosen_ref[pl.ds(first_row + r, 1), :] for r in range(blocks)], axis=1)
    across = jnp.broadcast_to(mine, (size, size))
    diagonal = lax.broadcasted_iota(jnp.int32, (size, size), 0) == lax.broadcasted_iota(
        jnp.int32, (size, size), 1
    )
    down = jnp.sum(jnp.where(diagonal, across, 0), axis=1, keepdims=True)
    lower = (down // blocks == across // blocks) & (down >= 0) & (down < across)
    second = jnp.max(jnp.where(lower, 1, 0), axis=0, keepdims=True)
    source = jnp.maximum(mine, 0) // blocks
    from_z, ahead = source // NY, (source % NY - y + NY) % NY
    served = (mine >= 0) & (from_z >= low) & (from_z <= high)
    here = (ahead == 0) | (served == False)
    column = jnp.where(served, from_z * blocks + jnp.maximum(mine, 0) % blocks, z * blocks)
    column = jnp.where(here, column, 0)
    along = jnp.where(
        ahead == NY - 1,
        3 * from_z + second,
        jnp.where(
            ahead == 1,
            3 * planes + 3 * from_z + second,
            6 * planes + second * planes + from_z,
        ),
    )
    along = jnp.where(here, 0, along)
    blank = jnp.zeros((1, table.shape[2] - size), jnp.int32)
    full = [jnp.concatenate([v, blank], axis=1) for v in (column, along, here.astype(jnp.int32))]
    row = lax.broadcasted_iota(jnp.int32, table.shape[1:], 0)
    table[at + 1] = jnp.where(row == 0, full[0], jnp.where(row == 1, full[1], full[2]))


def attend(
    nz,
    ntp,
    tokens_hbm,
    wq_hbm,
    wk_hbm,
    wv_hbm,
    w_hbm,
    chosen_hbm,
    cos_piece,
    sin_piece,
    out_ref,
    lse_ref,
    tokens_ref,
    wq_ref,
    wkv_ref,
    q_ref,
    q_far,
    chosen_across,
    chosen_ref,
    cos_ref,
    sin_ref,
    table,
    sel_ref,
    idx_ref,
    far_sel_ref,
    far_idx_ref,
    pool,
    own_pool,
    far_pool,
    to_right,
    to_left,
    picked,
    wall,
    mixed_ref,
    wide_ref,
    help_out,
    help_log_out,
    help_in,
    help_log_in,
    att,
    abuf,
    local_sem,
    z_send,
    up_recv,
    down_recv,
    y_send,
    y_recv,
    far_recv,
    relay_recv,
    w_send,
    w_recv,
    help_send,
    help_recv,
    a_send,
    a_recv,
):
    kv = lax.axis_index("kv")
    tp = lax.axis_index("tp")
    z, y = kv // NY, kv % NY
    nx = ntp // 2
    x, core = tp // 2, tp % 2
    up = ((z + 1) % nz) * NY + y
    down = ((z + nz - 1) % nz) * NY + y
    mirror_z = nz - 1 - z
    mirror = mirror_z * NY + y
    right = z * NY + (y + 1) % NY
    left = z * NY + (y + NY - 1) % NY
    x_right = ((x + 1) % nx) * 2 + core
    x_left = ((x + nx - 1) % nx) * 2 + core
    partner = x * 2 + (1 - core)
    width = wq_ref.shape[1]
    blocks = att.shape[0] // BLK
    heads = width // HEAD_DIM
    rows = att.shape[0] // ntp
    ups = nz // 2
    last_far = ups - 2 - z

    def load(which, src, dst):
        return pltpu.make_async_copy(src, dst, local_sem.at[which])

    loads = [
        load(0, tokens_hbm, tokens_ref),
        load(1, wk_hbm, wkv_ref.at[:, pl.ds(0, width)]),
        load(2, wv_hbm, wkv_ref.at[:, pl.ds(width, width)]),
        load(3, w_hbm, wall.at[tp]),
        load(4, wq_hbm, wq_ref),
    ]
    listing = load(5, chosen_hbm, chosen_across)
    listing.start()
    for copy in loads:
        copy.start()

    barrier = pltpu.get_barrier_semaphore()
    for peer in (mirror, up, down, right, left):
        pl.semaphore_signal(barrier, inc=1, device_id=(peer, tp), device_id_type=MESH)
    for step in range(1, ntp):
        pl.semaphore_signal(barrier, inc=1, device_id=(kv, (tp + step) % ntp), device_id_type=MESH)
    rotary_tables(cos_piece, sin_piece, cos_ref, sin_ref)
    listing.wait()
    chosen_ref[...] = jnp.transpose(chosen_across[...])
    make_tables(nz, blocks, kv, z, z - ups, nz, nz, chosen_ref, table, 0)
    make_tables(nz, blocks, kv, mirror_z, 0, last_far, nz // 2, chosen_ref, table, 2)
    to_smem = [
        load(5, table.at[0], sel_ref),
        load(6, table.at[1, pl.ds(0, 8)], idx_ref),
        load(7, table.at[2], far_sel_ref),
        load(8, table.at[3, pl.ds(0, 8)], far_idx_ref),
    ]
    for copy in to_smem:
        copy.start()

    def remote(src, dst, send, recv, device):
        return pltpu.make_async_remote_copy(
            src_ref=src,
            dst_ref=dst,
            send_sem=send,
            recv_sem=recv,
            device_id=device,
            device_id_type=MESH,
        )

    part = 1
    parts = blocks

    def up_copy(step, b):
        at = pool.at[(z + nz - step) % nz * blocks + b]
        return remote(at, at, z_send, up_recv.at[step * blocks + b], (up, tp))

    def down_copy(step, b):
        at = pool.at[pl.ds((z + step) % nz * blocks + b, 1)]
        return remote(at, at, z_send, down_recv.at[step * parts + b], (down, tp))

    def stretch(size):
        return own_pool.at[pl.ds(0, size)]

    def arrived(size, sem):
        remote(stretch(size), stretch(size), z_send, sem, (up, tp)).wait_recv()

    def left_off(size, sem):
        remote(stretch(size), stretch(size), sem, relay_recv.at[0], (up, tp)).wait_send()

    class Route:
        def __init__(self, kind):
            self.kind = kind
            self.pool = (own_pool, far_pool)[kind]
            self.planes = (nz, nz // 2)[kind]
            self.stage = (0, nz)[kind]
            self.sel = (sel_ref, far_sel_ref)[kind]
            self.recv = (y_recv, far_recv)[kind]

        def right_copy(self, p):
            src, dst = to_right.at[self.stage + p, pl.ds(0, 2)], self.pool.at[pl.ds(3 * p, 2)]
            return remote(src, dst, y_send, relay_recv.at[self.kind], (right, tp))

        def left_copy(self, p):
            src = to_left.at[self.stage + p, pl.ds(0, 2)]
            dst = self.pool.at[pl.ds(3 * self.planes + 3 * p, 2)]
            return remote(src, dst, y_send, relay_recv.at[self.kind], (left, tp))

        def right_ahead(self, k, p):
            src, dst = to_right.at[self.stage + p, 2], self.pool.at[3 * p + 2]
            return remote(src, dst, y_send, self.recv.at[k], (right, tp))

        def left_ahead(self, k, p):
            src, dst = to_left.at[self.stage + p, 2], self.pool.at[3 * self.planes + 3 * p + 2]
            return remote(src, dst, y_send, self.recv.at[k], (left, tp))

        def right_relay(self, p):
            src = self.pool.at[3 * p + 2]
            dst = self.pool.at[6 * self.planes + p]
            return remote(src, dst, y_send, relay_recv.at[self.kind], (right, tp))

        def left_relay(self, p):
            src = self.pool.at[3 * self.planes + 3 * p + 2]
            dst = self.pool.at[7 * self.planes + p]
            return remote(src, dst, y_send, relay_recv.at[self.kind], (left, tp))

        def exchange(self, k, p):
            here = [pool[p * blocks + b] for b in range(blocks)]
            at = self.stage + p

            def pick(ahead, c):
                which = self.sel[p, (ahead - 1) * 2 + c]
                found = here[blocks - 1]
                for b in range(blocks - 1):
                    found = jnp.where(which == b, here[b], found)
                return found

            to_right[at, 2] = pick(2, 0)
            self.right_ahead(k, p).start()
            to_left[at, 2] = pick(2, 1)
            self.left_ahead(k, p).start()
            to_right[at, 0] = pick(1, 0)
            to_right[at, 1] = pick(1, 1)
            self.right_copy(p).start()
            to_left[at, 0] = pick(3, 0)
            to_left[at, 1] = pick(3, 1)
            self.left_copy(p).start()

        def relay(self, k, p):
            arrived(2, self.recv.at[k])
            self.right_relay(p).start()
            self.left_relay(p).start()

    routes = (Route(0), Route(1))

    half = width // 2

    def w_ring(side):
        peer = x_right if side == 0 else x_left
        return remote(wall.at[tp], wall.at[tp], w_send, w_recv.at[side], (kv, peer))

    def w_half(side):
        origin = x_left if side == 0 else x_right
        peer = x_right if side == 0 else x_left
        piece = wall.at[origin, pl.ds(side * half, half)]
        return remote(piece, piece, w_send, w_recv.at[2], (kv, peer))

    def w_arrived(size, sem):
        at = wall.at[pl.ds(0, size)]
        remote(at, at, w_send, sem, (kv, partner)).wait_recv()

    def w_pair(which):
        far = ((x + 2) % nx) * 2 + core
        owner = (tp, x_left, x_right, far)[which]
        return remote(wall.at[owner], wall.at[owner], w_send, w_recv.at[3], (kv, partner))

    def w_first():
        w_ring(0).wait_recv()
        w_half(0).start()
        w_pair(1).start()
        w_ring(1).wait_recv()
        w_half(1).start()
        w_pair(2).start()

    def w_second():
        w_arrived(1, w_recv.at[2])
        w_pair(3).start()

    q_copy = remote(q_ref, q_far, help_send.at[0], help_recv.at[0], (mirror, tp))
    o_copy = remote(help_out, help_in, help_send.at[1], help_recv.at[1], (mirror, tp))
    log_copy = remote(help_log_out, help_log_in, help_send.at[2], help_recv.at[2], (mirror, tp))
    helper = last_far >= 0
    helped = mirror_z <= ups - 2

    loads[0].wait()
    loads[1].wait()
    cos_part, sin_part = cos_ref[...], sin_ref[...]
    loads[2].wait()
    both = jnp.dot(tokens_ref[...], wkv_ref[...], preferred_element_type=jnp.float32)
    keys = turn(both[:, :width], cos_part, sin_part).astype(jnp.bfloat16)
    pool[pl.ds(z * blocks, blocks), :, :width] = keys.reshape(blocks, BLK, width)
    values = both[:, width:].astype(jnp.bfloat16)
    pool[pl.ds(z * blocks, blocks), :, width:] = values.reshape(blocks, BLK, width)
    pl.semaphore_wait(barrier, 5 + ntp - 1)

    @pl.when(z < nz - 1)
    def _():
        for b in range(blocks):
            up_copy(0, b).start()

    goes_down = (z >= 1) & (z <= ups - 2)

    @pl.when(goes_down)
    def _():
        for b in range(parts):
            down_copy(0, b).start()

    for copy in to_smem:
        copy.wait()
    pl.when(z <= last_far)(lambda: routes[1].exchange(0, z))
    routes[0].exchange(0, z)
    loads[4].wait()
    query = jnp.dot(tokens_ref[...], wq_ref[...], preferred_element_type=jnp.float32)
    query = turn(query, cos_part, sin_part).astype(jnp.bfloat16).astype(jnp.float32)
    q_ref[...] = (query * HEAD_DIM ** (-0.5)).astype(jnp.bfloat16)
    pl.when(helped)(lambda: q_copy.start())
    loads[3].wait()
    w_ring(0).start()
    w_ring(1).start()
    w_pair(0).start()

    def own_there(k):
        return z - k >= 0

    def far_below(k):
        return (z - k >= 0) & (z - k <= last_far)

    def far_above(step):
        return z + 1 + step <= last_far

    def relay_step(k):
        pl.when(far_below(k))(lambda: routes[1].relay(k, z - k))
        if 1 <= k <= ups - 2:
            pl.when(far_above(k - 1))(lambda: routes[1].relay(ups + k - 1, z + k))
        pl.when(own_there(k))(lambda: routes[0].relay(k, z - k))

    for step in range(ups):
        k = step + 1

        @pl.when(own_there(k))
        def _():
            for b in range(blocks):
                remote(pool.at[b], pool.at[b], z_send, up_recv.at[step * blocks + b], (up, tp)).wait_recv()
                if step + 1 < ups:
                    pl.when(z < nz - 1)(lambda: up_copy(step + 1, b).start())
            pl.when(z - k <= last_far)(lambda: routes[1].exchange(k, z - k))
            routes[0].exchange(k, z - k)

        if step <= ups - 3:

            @pl.when(z + 1 + step <= ups - 2)
            def _():
                for b in range(parts):
                    arrived(part, down_recv.at[step * parts + b])

                    if step <= ups - 4:

                        @pl.when(z >= 1)
                        def _():
                            down_copy(step + 1, b).start()

                pl.when(far_above(step))(lambda: routes[1].exchange(ups + step, z + k))

        if step == 3:
            w_first()
        if step == 5:
            w_second()
        if step >= 1:
            relay_step(step - 1)
    relay_step(ups - 1)
    relay_step(ups)

    def plane_counts(c):
        own = min(c, ups) + 1
        far = max(0, ups - 1 - c)
        ups_sent = min(c, ups - 1) + 1 if c < nz - 1 else 0
        downs_sent = ups - 1 - c if 1 <= c <= ups - 2 else 0
        return own, far, (ups_sent + downs_sent) * blocks

    lane = lax.broadcasted_iota(jnp.int32, (BLK, width), 1)
    wide_lane = lax.broadcasted_iota(jnp.int32, (heads * BLK, width), 1)
    wide_row = lax.broadcasted_iota(jnp.int32, (heads * BLK, width), 0)
    eye = lax.broadcasted_iota(jnp.int32, (heads * BLK, heads * BLK), 0) == lax.broadcasted_iota(
        jnp.int32, (heads * BLK, heads * BLK), 1
    )
    key_block = lax.broadcasted_iota(jnp.int32, (1, SEL * BLK), 1) // BLK

    def by_head(stacked):
        result = stacked[:BLK]
        for head in range(1, heads):
            result = jnp.where(lane // HEAD_DIM == head, stacked[head * BLK : (head + 1) * BLK], result)
        return result

    def attention(i, queries, places, along, dest, low, high):
        for j in range(SEL):
            n = i * SEL + j
            picked[i, j * BLK : (j + 1) * BLK, :] = jnp.where(
                places[2, n] > 0, pool[places[0, n]], along[places[1, n]]
            )
        rows_here = queries[i * BLK : (i + 1) * BLK, :].astype(jnp.float32)
        stacked = jnp.concatenate([rows_here] * heads, axis=0)
        stacked = jnp.where(wide_lane // HEAD_DIM == wide_row // BLK, stacked, 0.0)
        scores = lax.dot_general(
            stacked.astype(jnp.bfloat16),
            picked[i, :, :width],
            (((1,), (1,)), ((), ())),
            preferred_element_type=jnp.float32,
        )
        listed = chosen_ref[pl.ds(dest * blocks + i, 1), :]
        block_of = jnp.zeros((1, SEL * BLK), jnp.int32)
        for j in range(SEL):
            block_of = jnp.where(key_block == j, listed[:, j : j + 1], block_of)
        scores = jnp.where((block_of >= low) & (block_of < high), scores, MASKED)
        top = jnp.max(scores, axis=1, keepdims=True)
        weights = jnp.exp(scores - top)
        total = jnp.sum(weights, axis=1, keepdims=True)
        summed = jnp.dot(
            weights.astype(jnp.bfloat16), picked[i, :, width:], preferred_element_type=jnp.float32
        )
        return by_head(summed / total), top + jnp.log(total)

    first = jnp.maximum(z - ups, 0) * NY * blocks

    def own_attention():
        for c in range(nz):
            pl.when(z == c)(lambda: arrived(6 * plane_counts(c)[0], relay_recv.at[0]))
        for i in range(blocks):
            result, column = attention(i, q_ref, idx_ref, own_pool, kv, first, nz * NY * blocks)
            mixed_ref[i * BLK : (i + 1) * BLK, :] = result
            wide_ref[i * BLK : (i + 1) * BLK, :] = by_head(
                jnp.broadcast_to(column, (heads * BLK, width))
            )

    def part_copy(to):
        src = att.at[pl.ds(to * rows, rows)]
        dst = abuf.at[:, pl.ds(pl.multiple_of(tp * width, width), width)]
        return remote(src, dst, a_send, a_recv, (kv, to))

    def emit():
        per_block = ntp // blocks
        for i in range(blocks):
            at = slice(i * BLK, (i + 1) * BLK)
            att[at, :] = mixed_ref[at, :].astype(jnp.bfloat16)
            for to in range(i * per_block, (i + 1) * per_block):

                @pl.when(to != tp)
                def _():
                    part_copy(to).start()

                @pl.when(to == tp)
                def _():
                    abuf[:, pl.ds(pl.multiple_of(tp * width, width), width)] = att[
                        to * rows : (to + 1) * rows, :
                    ]

        for head in range(heads):
            cols = slice(head * HEAD_DIM, (head + 1) * HEAD_DIM)
            lse_ref[head : head + 1, :] = jnp.concatenate(
                [
                    jnp.sum(
                        jnp.where(
                            eye[:BLK, :HEAD_DIM], wide_ref[i * BLK : (i + 1) * BLK, cols], 0.0
                        ),
                        axis=0,
                        keepdims=True,
                    )
                    for i in range(blocks)
                ],
                axis=1,
            )

    early = z <= 1

    @pl.when(early)
    def _():
        own_attention()
        emit()

    @pl.when(helper)
    def _():
        for c in range(ups - 1):

            @pl.when(z == c)
            def _():
                arrived(6 * plane_counts(c)[1], relay_recv.at[1])

        q_copy.wait_recv()
        help_log_out[...] = jnp.zeros(help_log_out.shape, jnp.float32)
        limit = (last_far + 1) * NY * blocks
        for i in range(blocks):
            result, column = attention(i, q_far, far_idx_ref, far_pool, mirror, 0, limit)
            help_out[i * BLK : (i + 1) * BLK, :] = result.astype(jnp.bfloat16)
            help_log_out[i : i + 1, :] = jnp.sum(jnp.where(eye, column, 0.0), axis=0, keepdims=True)
        o_copy.start()
        log_copy.start()

    pl.when(z > 1)(own_attention)

    @pl.when(helped)
    def _():
        o_copy.wait_recv()
        log_copy.wait_recv()
        for i in range(blocks):
            at = slice(i * BLK, (i + 1) * BLK)
            row = jnp.broadcast_to(help_log_in[i : i + 1, :], (heads * BLK, width))
            column = jnp.sum(jnp.where(eye, row, 0.0), axis=1, keepdims=True)
            theirs = by_head(jnp.broadcast_to(column, (heads * BLK, width)))
            mine = wide_ref[at, :]
            top = jnp.maximum(mine, theirs)
            share, other = jnp.exp(mine - top), jnp.exp(theirs - top)
            total = share + other
            extra = help_in[at, :].astype(jnp.float32)
            mixed_ref[at, :] = (mixed_ref[at, :] * share + extra * other) / total
            wide_ref[at, :] = top + jnp.log(total)

    pl.when(z > 1)(emit)

    for c in range(nz):

        @pl.when(z == c)
        def _():
            own, far, sent = plane_counts(c)
            left_off(8 * (own + far), y_send)
            if sent:
                left_off(sent, z_send)

    @pl.when(helper)
    def _():
        o_copy.wait_send()
        log_copy.wait_send()

    pl.when(helped)(lambda: q_copy.wait_send())
    w_arrived(4, w_recv.at[3])
    sent_w = wall.at[pl.ds(0, ntp - 1)]
    remote(sent_w, sent_w, w_send, w_recv.at[3], (kv, partner)).wait_send()
    others = abuf.at[:, pl.ds(0, (ntp - 1) * width)]
    remote(others, others, a_send, a_recv, (kv, partner)).wait()
    total_width = out_ref.shape[1]
    chunk = min(512, total_width)
    for c in range(total_width // chunk):
        cols = slice(c * chunk, (c + 1) * chunk)
        acc = jnp.zeros((rows, chunk), jnp.float32)
        for t in range(ntp):
            acc += jnp.dot(
                abuf[:, t * width : (t + 1) * width],
                wall[t, :, cols],
                preferred_element_type=jnp.float32,
            )
        out_ref[:, cols] = acc.astype(jnp.bfloat16)


def finish(mixed_ref, log_ref, mixed_out, log_out, sem):
    first = pltpu.make_async_copy(mixed_ref, mixed_out, sem.at[0])
    second = pltpu.make_async_copy(log_ref, log_out, sem.at[1])
    first.start()
    second.start()
    first.wait()
    second.wait()


def local(nkv, ntp, tokens, w_query, w_key, w_value, w_out, chosen):
    local_rows = tokens.shape[0]
    width = w_query.shape[1]
    heads = width // HEAD_DIM
    blocks = local_rows // BLK
    nz = nkv // NY
    device = lax.axis_index("kv")
    vmem = pl.BlockSpec(memory_space=pltpu.VMEM)
    hbm = pl.BlockSpec(memory_space=pltpu.HBM)
    cos_piece, sin_piece = rotary_pieces(device * local_rows, width)
    ups = nz // 2
    out_rows = local_rows // ntp
    dma = pltpu.SemaphoreType.DMA
    stage = (nz + ups, 3, BLK, 2 * width)
    bf16, f32, i32 = jnp.bfloat16, jnp.float32, jnp.int32
    mixed, log_sums = pl.pallas_call(
        functools.partial(attend, nz, ntp),
        out_shape=(
            jax.ShapeDtypeStruct((out_rows, w_out.shape[1]), bf16),
            jax.ShapeDtypeStruct((heads, local_rows), f32),
        ),
        in_specs=[hbm] * 6 + [vmem] * 2,
        out_specs=(vmem, vmem),
        scratch_shapes=[
            pltpu.VMEM(tokens.shape, bf16),
            pltpu.VMEM(w_query.shape, bf16),
            pltpu.VMEM((w_key.shape[0], 2 * width), bf16),
            pltpu.VMEM((local_rows, width), bf16),
            pltpu.VMEM((local_rows, width), bf16),
            pltpu.VMEM((SEL, chosen.shape[0]), i32),
            pltpu.VMEM((chosen.shape[0], SEL), i32),
            pltpu.VMEM((local_rows, width), f32),
            pltpu.VMEM((local_rows, width), f32),
            pltpu.VMEM((4, nz, 128), i32),
            pltpu.SMEM((nz, 128), i32),
            pltpu.SMEM((8, 128), i32),
            pltpu.SMEM((nz, 128), i32),
            pltpu.SMEM((8, 128), i32),
            pltpu.VMEM((nz * blocks, BLK, 2 * width), bf16),
            pltpu.VMEM((nz * 8, BLK, 2 * width), bf16),
            pltpu.VMEM((ups * 8, BLK, 2 * width), bf16),
            pltpu.VMEM(stage, bf16),
            pltpu.VMEM(stage, bf16),
            pltpu.VMEM((blocks, SEL * BLK, 2 * width), bf16),
            pltpu.VMEM((ntp, width, w_out.shape[1]), bf16),
            pltpu.VMEM((local_rows, width), f32),
            pltpu.VMEM((local_rows, width), f32),
            pltpu.VMEM((local_rows, width), bf16),
            pltpu.VMEM((8, heads * BLK), f32),
            pltpu.VMEM((local_rows, width), bf16),
            pltpu.VMEM((8, heads * BLK), f32),
            pltpu.VMEM((local_rows, width), bf16),
            pltpu.VMEM((out_rows, ntp * width), bf16),
            dma((9,)),
            dma,
            dma((blocks * ups,)),
            dma((blocks * (ups - 2),)),
            dma,
            dma((ups + 1,)),
            dma((2 * ups - 2,)),
            dma((2,)),
            dma,
            dma((4,)),
            dma((3,)),
            dma((3,)),
            dma,
            dma,
        ],
        compiler_params=pltpu.CompilerParams(
            collective_id=0, has_side_effects=True, vmem_limit_bytes=55000 * 1024
        ),
    )(tokens, w_query, w_key, w_value, w_out, chosen.T, cos_piece, sin_piece)
    return pl.pallas_call(
        finish,
        out_shape=(
            jax.ShapeDtypeStruct(mixed.shape, mixed.dtype),
            jax.ShapeDtypeStruct(log_sums.shape, log_sums.dtype),
        ),
        in_specs=[vmem, vmem],
        out_specs=(hbm, hbm),
        scratch_shapes=[dma((2,))],
        compiler_params=pltpu.CompilerParams(vmem_limit_bytes=1024 * 1024),
    )(mixed, log_sums)


def solution(mesh):
    placed = (P("kv", None), P(None, "tp"), P(None, "tp"), P(None, "tp"), P("tp", None), P())
    return jax.shard_map(
        functools.partial(local, mesh.shape["kv"], mesh.shape["tp"]),
        mesh=mesh,
        in_specs=placed,
        out_specs=(P(("kv", "tp"), None), P("tp", "kv")),
        check_vma=False,
    )
```

```python
import functools

import jax
import jax.numpy as jnp
from jax import lax
from jax.experimental import pallas as pl
from jax.experimental.pallas import tpu as pltpu
from jax.sharding import PartitionSpec as P

HEAD_DIM = 64
BLK = 64
SEL = 16
NY = 4
ROTARY_BASE = 500000.0
MASKED = -1e30
MESH = pl.DeviceIdType.MESH


def rotary_pieces(first, width):
    half = HEAD_DIM // 2
    lane = jnp.arange(width)
    inverse = ROTARY_BASE ** (-(lane % half).astype(jnp.float32) / half)
    row = jnp.arange(40)
    position = jnp.where(row < 16, 16 * row, jnp.where(row < 32, row - 16, first))
    angles = position.astype(jnp.float32)[:, None] * inverse[None, :]
    return jnp.cos(angles), jnp.sin(angles)


def rotary_tables(cos_piece, sin_piece, cos_ref, sin_ref):
    half = HEAD_DIM // 2
    cos_first, sin_first = cos_piece[32:33, :], sin_piece[32:33, :]
    cos_tens, sin_tens = cos_piece[:16, :], sin_piece[:16, :]
    cos_ones, sin_ones = cos_piece[16:32, :], sin_piece[16:32, :]
    lane = lax.broadcasted_iota(jnp.int32, cos_ones.shape, 1)
    sign = jnp.where(lane % HEAD_DIM < half, -1.0, 1.0)
    cos_row = cos_first * cos_tens - sin_first * sin_tens
    sin_row = sin_first * cos_tens + cos_first * sin_tens
    for t in range(cos_ref.shape[0] // 16):
        c, n = cos_row[t : t + 1, :], sin_row[t : t + 1, :]
        cos_ref[t * 16 : (t + 1) * 16, :] = c * cos_ones - n * sin_ones
        sin_ref[t * 16 : (t + 1) * 16, :] = (n * cos_ones + c * sin_ones) * sign


def turn(values, cos_part, sin_part):
    width = values.shape[1]
    half = HEAD_DIM // 2
    lane = lax.broadcasted_iota(jnp.int32, values.shape, 1)
    ahead = pltpu.roll(values, width - half, 1)
    behind = pltpu.roll(values, half, 1)
    partner = jnp.where(lane % HEAD_DIM < half, ahead, behind)
    return values * cos_part + partner * sin_part


def make_tables(nz, blocks, kv, dest_z, low, high, planes, chosen_ref, table, at):
    z, y = kv // NY, kv % NY
    lane = lax.broadcasted_iota(jnp.int32, table.shape[1:], 1)
    found = jnp.zeros(table.shape[1:], jnp.int32)
    target = lax.broadcasted_iota(jnp.int32, (nz, SEL), 0) * (NY * blocks) + y * blocks
    for ahead in range(1, NY):
        dest = dest_z * NY + (y + ahead) % NY
        rows = [chosen_ref[pl.ds(dest * blocks + r, 1), :] for r in range(blocks)]
        least = jnp.full((nz, 1), blocks - 1, jnp.int32)
        most = jnp.zeros((nz, 1), jnp.int32)
        hits = []
        for b in range(blocks):
            hit = jnp.zeros((nz, SEL), jnp.int32)
            for entries in rows:
                hit = jnp.where(entries == target + b, 1, hit)
            hits.append(jnp.max(hit, axis=1, keepdims=True))
        for b in range(blocks):
            most = jnp.where(hits[b] > 0, b, most)
            least = jnp.where(hits[blocks - 1 - b] > 0, blocks - 1 - b, least)
        found = jnp.where(lane == (ahead - 1) * 2, least, found)
        found = jnp.where(lane == (ahead - 1) * 2 + 1, most, found)
    table[at] = found
    size = blocks * SEL
    first_row = (dest_z * NY + y) * blocks
    mine = jnp.concatenate([chosen_ref[pl.ds(first_row + r, 1), :] for r in range(blocks)], axis=1)
    across = jnp.broadcast_to(mine, (size, size))
    diagonal = lax.broadcasted_iota(jnp.int32, (size, size), 0) == lax.broadcasted_iota(
        jnp.int32, (size, size), 1
    )
    down = jnp.sum(jnp.where(diagonal, across, 0), axis=1, keepdims=True)
    lower = (down // blocks == across // blocks) & (down >= 0) & (down < across)
    second = jnp.max(jnp.where(lower, 1, 0), axis=0, keepdims=True)
    source = jnp.maximum(mine, 0) // blocks
    from_z, ahead = source // NY, (source % NY - y + NY) % NY
    served = (mine >= 0) & (from_z >= low) & (from_z <= high)
    here = (ahead == 0) | (served == False)
    column = jnp.where(served, from_z * blocks + jnp.maximum(mine, 0) % blocks, z * blocks)
    column = jnp.where(here, column, 0)
    along = jnp.where(
        ahead == NY - 1,
        3 * from_z + second,
        jnp.where(
            ahead == 1,
            3 * planes + 3 * from_z + second,
            6 * planes + second * planes + from_z,
        ),
    )
    along = jnp.where(here, 0, along)
    blank = jnp.zeros((1, table.shape[2] - size), jnp.int32)
    full = [jnp.concatenate([v, blank], axis=1) for v in (column, along, here.astype(jnp.int32))]
    row = lax.broadcasted_iota(jnp.int32, table.shape[1:], 0)
    table[at + 1] = jnp.where(row == 0, full[0], jnp.where(row == 1, full[1], full[2]))


def attend(
    nz,
    ntp,
    tokens_hbm,
    wq_hbm,
    wk_hbm,
    wv_hbm,
    w_hbm,
    chosen_hbm,
    cos_piece,
    sin_piece,
    out_ref,
    lse_ref,
    tokens_ref,
    wq_ref,
    wkv_ref,
    q_ref,
    q_far,
    chosen_across,
    chosen_ref,
    cos_ref,
    sin_ref,
    table,
    sel_ref,
    idx_ref,
    far_sel_ref,
    far_idx_ref,
    pool,
    own_pool,
    far_pool,
    to_right,
    to_left,
    picked,
    wall,
    mixed_ref,
    wide_ref,
    help_out,
    help_log_out,
    help_in,
    help_log_in,
    att,
    abuf,
    acc_ref,
    local_sem,
    z_send,
    up_recv,
    down_recv,
    y_send,
    y_recv,
    far_recv,
    relay_recv,
    w_send,
    w_recv,
    help_send,
    help_recv,
    a_send,
    a_recv,
):
    kv = lax.axis_index("kv")
    tp = lax.axis_index("tp")
    z, y = kv // NY, kv % NY
    nx = ntp // 2
    x, core = tp // 2, tp % 2
    up = ((z + 1) % nz) * NY + y
    down = ((z + nz - 1) % nz) * NY + y
    mirror_z = nz - 1 - z
    mirror = mirror_z * NY + y
    right = z * NY + (y + 1) % NY
    left = z * NY + (y + NY - 1) % NY
    x_right = ((x + 1) % nx) * 2 + core
    x_left = ((x + nx - 1) % nx) * 2 + core
    partner = x * 2 + (1 - core)
    width = wq_ref.shape[1]
    blocks = att.shape[0] // BLK
    heads = width // HEAD_DIM
    rows = att.shape[0] // ntp
    ups = nz // 2
    last_far = ups - 2 - z

    def load(which, src, dst):
        return pltpu.make_async_copy(src, dst, local_sem.at[which])

    loads = [
        load(0, tokens_hbm, tokens_ref),
        load(1, wk_hbm, wkv_ref.at[:, pl.ds(0, width)]),
        load(2, wv_hbm, wkv_ref.at[:, pl.ds(width, width)]),
        load(3, w_hbm, wall.at[tp]),
        load(4, wq_hbm, wq_ref),
    ]
    listing = load(5, chosen_hbm, chosen_across)
    listing.start()
    for copy in loads:
        copy.start()

    barrier = pltpu.get_barrier_semaphore()
    for peer in (mirror, up, down, right, left):
        pl.semaphore_signal(barrier, inc=1, device_id=(peer, tp), device_id_type=MESH)
    for step in range(1, ntp):
        pl.semaphore_signal(barrier, inc=1, device_id=(kv, (tp + step) % ntp), device_id_type=MESH)
    rotary_tables(cos_piece, sin_piece, cos_ref, sin_ref)
    listing.wait()
    chosen_ref[...] = jnp.transpose(chosen_across[...])
    make_tables(nz, blocks, kv, z, z - ups, nz, nz, chosen_ref, table, 0)
    make_tables(nz, blocks, kv, mirror_z, 0, last_far, nz // 2, chosen_ref, table, 2)
    to_smem = [
        load(5, table.at[0], sel_ref),
        load(6, table.at[1, pl.ds(0, 8)], idx_ref),
        load(7, table.at[2], far_sel_ref),
        load(8, table.at[3, pl.ds(0, 8)], far_idx_ref),
    ]
    for copy in to_smem:
        copy.start()

    def remote(src, dst, send, recv, device):
        return pltpu.make_async_remote_copy(
            src_ref=src,
            dst_ref=dst,
            send_sem=send,
            recv_sem=recv,
            device_id=device,
            device_id_type=MESH,
        )

    parts = 2 * blocks

    def up_copy(step, b):
        at = pool.at[(z + nz - step) % nz * blocks + b // 2, pl.ds(b % 2 * (BLK // 2), BLK // 2)]
        return remote(at, at, z_send, up_recv.at[step * 2 * blocks + b], (up, tp))

    def down_copy(step, b):
        at = pool.at[(z + step) % nz * blocks + b // 2, pl.ds(b % 2 * (BLK // 2), BLK // 2)]
        return remote(at, at, z_send, down_recv.at[step * parts + b], (down, tp))

    def stretch(size):
        return own_pool.at[pl.ds(0, size)]

    def arrived(size, sem):
        remote(stretch(size), stretch(size), z_send, sem, (up, tp)).wait_recv()

    def left_off(size, sem):
        remote(stretch(size), stretch(size), sem, relay_recv.at[0], (up, tp)).wait_send()

    class Route:
        def __init__(self, kind):
            self.kind = kind
            self.pool = (own_pool, far_pool)[kind]
            self.planes = (nz, nz // 2)[kind]
            self.stage = (0, nz)[kind]
            self.sel = (sel_ref, far_sel_ref)[kind]
            self.recv = (y_recv, far_recv)[kind]

        def right_copy(self, p):
            src, dst = to_right.at[self.stage + p, pl.ds(0, 2)], self.pool.at[pl.ds(3 * p, 2)]
            return remote(src, dst, y_send, relay_recv.at[self.kind], (right, tp))

        def left_copy(self, p):
            src = to_left.at[self.stage + p, pl.ds(0, 2)]
            dst = self.pool.at[pl.ds(3 * self.planes + 3 * p, 2)]
            return remote(src, dst, y_send, relay_recv.at[self.kind], (left, tp))

        def right_ahead(self, k, p):
            src, dst = to_right.at[self.stage + p, 2], self.pool.at[3 * p + 2]
            return remote(src, dst, y_send, self.recv.at[k], (right, tp))

        def left_ahead(self, k, p):
            src, dst = to_left.at[self.stage + p, 2], self.pool.at[3 * self.planes + 3 * p + 2]
            return remote(src, dst, y_send, self.recv.at[k], (left, tp))

        def right_relay(self, p):
            src = self.pool.at[3 * p + 2]
            dst = self.pool.at[6 * self.planes + p]
            return remote(src, dst, y_send, relay_recv.at[self.kind], (right, tp))

        def left_relay(self, p):
            src = self.pool.at[3 * self.planes + 3 * p + 2]
            dst = self.pool.at[7 * self.planes + p]
            return remote(src, dst, y_send, relay_recv.at[self.kind], (left, tp))

        def exchange(self, k, p):
            here = [pool[p * blocks + b] for b in range(blocks)]
            at = self.stage + p

            def pick(ahead, c):
                which = self.sel[p, (ahead - 1) * 2 + c]
                found = here[blocks - 1]
                for b in range(blocks - 1):
                    found = jnp.where(which == b, here[b], found)
                return found

            to_right[at, 2] = pick(2, 0)
            self.right_ahead(k, p).start()
            to_left[at, 2] = pick(2, 1)
            self.left_ahead(k, p).start()
            to_right[at, 0] = pick(1, 0)
            to_right[at, 1] = pick(1, 1)
            self.right_copy(p).start()
            to_left[at, 0] = pick(3, 0)
            to_left[at, 1] = pick(3, 1)
            self.left_copy(p).start()

        def relay(self, k, p):
            arrived(2, self.recv.at[k])
            self.right_relay(p).start()
            self.left_relay(p).start()

    routes = (Route(0), Route(1))

    half = width // 2

    def w_ring(side):
        peer = x_right if side == 0 else x_left
        return remote(wall.at[tp], wall.at[tp], w_send, w_recv.at[side], (kv, peer))

    def w_half(side):
        origin = x_left if side == 0 else x_right
        peer = x_right if side == 0 else x_left
        piece = wall.at[origin, pl.ds(side * half, half)]
        return remote(piece, piece, w_send, w_recv.at[2], (kv, peer))

    def w_arrived(size, sem):
        at = wall.at[pl.ds(0, size)]
        remote(at, at, w_send, sem, (kv, partner)).wait_recv()

    def w_pair(which):
        far = ((x + 2) % nx) * 2 + core
        owner = (tp, x_left, x_right, far)[which]
        return remote(wall.at[owner], wall.at[owner], w_send, w_recv.at[3], (kv, partner))

    def w_first():
        w_ring(0).wait_recv()
        w_half(0).start()
        w_pair(1).start()
        w_ring(1).wait_recv()
        w_half(1).start()
        w_pair(2).start()

    def w_second():
        w_arrived(1, w_recv.at[2])
        w_pair(3).start()

    q_copy = remote(q_ref, q_far, help_send.at[0], help_recv.at[0], (mirror, tp))
    o_copy = remote(help_out, help_in, help_send.at[1], help_recv.at[1], (mirror, tp))
    log_copy = remote(help_log_out, help_log_in, help_send.at[2], help_recv.at[2], (mirror, tp))
    helper = last_far >= 0
    helped = mirror_z <= ups - 2

    loads[0].wait()
    loads[1].wait()
    cos_part, sin_part = cos_ref[...], sin_ref[...]
    loads[2].wait()
    both = jnp.dot(tokens_ref[...], wkv_ref[...], preferred_element_type=jnp.float32)
    keys = turn(both[:, :width], cos_part, sin_part).astype(jnp.bfloat16)
    pool[pl.ds(z * blocks, blocks), :, :width] = keys.reshape(blocks, BLK, width)
    values = both[:, width:].astype(jnp.bfloat16)
    pool[pl.ds(z * blocks, blocks), :, width:] = values.reshape(blocks, BLK, width)
    pl.semaphore_wait(barrier, 5 + ntp - 1)

    @pl.when(z < nz - 1)
    def _():
        for b in range(2 * blocks):
            up_copy(0, b).start()

    goes_down = (z >= 1) & (z <= ups - 2)

    @pl.when(goes_down)
    def _():
        for b in range(parts):
            down_copy(0, b).start()

    for copy in to_smem:
        copy.wait()
    pl.when(z <= last_far)(lambda: routes[1].exchange(0, z))
    routes[0].exchange(0, z)
    loads[4].wait()
    query = jnp.dot(tokens_ref[...], wq_ref[...], preferred_element_type=jnp.float32)
    query = turn(query, cos_part, sin_part).astype(jnp.bfloat16).astype(jnp.float32)
    q_ref[...] = (query * HEAD_DIM ** (-0.5)).astype(jnp.bfloat16)
    pl.when(helped)(lambda: q_copy.start())
    loads[3].wait()
    w_ring(0).start()
    w_ring(1).start()
    w_pair(0).start()

    def own_there(k):
        return z - k >= 0

    def far_below(k):
        return (z - k >= 0) & (z - k <= last_far)

    def far_above(step):
        return z + 1 + step <= last_far

    def relay_step(k):
        pl.when(far_below(k))(lambda: routes[1].relay(k, z - k))
        if 1 <= k <= ups - 2:
            pl.when(far_above(k - 1))(lambda: routes[1].relay(ups + k - 1, z + k))
        pl.when(own_there(k))(lambda: routes[0].relay(k, z - k))

    for step in range(ups):
        k = step + 1

        @pl.when(own_there(k))
        def _():
            for b in range(2 * blocks):
                up_copy(step, b).wait_recv()
                if step + 1 < ups:
                    pl.when(z < nz - 1)(lambda: up_copy(step + 1, b).start())
            pl.when(z - k <= last_far)(lambda: routes[1].exchange(k, z - k))
            routes[0].exchange(k, z - k)

        if step <= ups - 3:

            @pl.when(z + 1 + step <= ups - 2)
            def _():
                for b in range(parts):
                    down_copy(step, b).wait_recv()

                    if step <= ups - 4:

                        @pl.when(z >= 1)
                        def _():
                            down_copy(step + 1, b).start()

                pl.when(far_above(step))(lambda: routes[1].exchange(ups + step, z + k))

        if step == 3:
            w_first()
        if step == 5:
            w_second()
        if step >= 1:
            relay_step(step - 1)
    relay_step(ups - 1)
    relay_step(ups)

    def plane_counts(c):
        own = min(c, ups) + 1
        far = max(0, ups - 1 - c)
        ups_sent = min(c, ups - 1) + 1 if c < nz - 1 else 0
        downs_sent = ups - 1 - c if 1 <= c <= ups - 2 else 0
        return own, far, (ups_sent + downs_sent) * blocks

    lane = lax.broadcasted_iota(jnp.int32, (BLK, width), 1)
    wide_lane = lax.broadcasted_iota(jnp.int32, (heads * BLK, width), 1)
    wide_row = lax.broadcasted_iota(jnp.int32, (heads * BLK, width), 0)
    eye = lax.broadcasted_iota(jnp.int32, (heads * BLK, heads * BLK), 0) == lax.broadcasted_iota(
        jnp.int32, (heads * BLK, heads * BLK), 1
    )
    key_block = lax.broadcasted_iota(jnp.int32, (1, SEL * BLK), 1) // BLK

    def by_head(stacked):
        result = stacked[:BLK]
        for head in range(1, heads):
            result = jnp.where(lane // HEAD_DIM == head, stacked[head * BLK : (head + 1) * BLK], result)
        return result

    def attention(i, queries, places, along, dest, low, high):
        for j in range(SEL):
            n = i * SEL + j
            picked[i, j * BLK : (j + 1) * BLK, :] = jnp.where(
                places[2, n] > 0, pool[places[0, n]], along[places[1, n]]
            )
        rows_here = queries[i * BLK : (i + 1) * BLK, :].astype(jnp.float32)
        stacked = jnp.concatenate([rows_here] * heads, axis=0)
        stacked = jnp.where(wide_lane // HEAD_DIM == wide_row // BLK, stacked, 0.0)
        scores = lax.dot_general(
            stacked.astype(jnp.bfloat16),
            picked[i, :, :width],
            (((1,), (1,)), ((), ())),
            preferred_element_type=jnp.float32,
        )
        listed = chosen_ref[pl.ds(dest * blocks + i, 1), :]
        block_of = jnp.zeros((1, SEL * BLK), jnp.int32)
        for j in range(SEL):
            block_of = jnp.where(key_block == j, listed[:, j : j + 1], block_of)
        scores = jnp.where((block_of >= low) & (block_of < high), scores, MASKED)
        top = jnp.max(scores, axis=1, keepdims=True)
        weights = jnp.exp(scores - top)
        total = jnp.sum(weights, axis=1, keepdims=True)
        summed = jnp.dot(
            weights.astype(jnp.bfloat16), picked[i, :, width:], preferred_element_type=jnp.float32
        )
        return by_head(summed / total), top + jnp.log(total)

    first = jnp.maximum(z - ups, 0) * NY * blocks

    def own_attention():
        for c in range(nz):
            pl.when(z == c)(lambda: arrived(6 * plane_counts(c)[0], relay_recv.at[0]))
        for i in range(blocks):
            result, column = attention(i, q_ref, idx_ref, own_pool, kv, first, nz * NY * blocks)
            mixed_ref[i * BLK : (i + 1) * BLK, :] = result
            wide_ref[i * BLK : (i + 1) * BLK, :] = by_head(
                jnp.broadcast_to(column, (heads * BLK, width))
            )

    def part_copy(to, distant):
        src = att.at[pl.ds(to * rows, rows)]
        dst = abuf.at[:, pl.ds(pl.multiple_of(tp * width, width), width)]
        return remote(src, dst, a_send, a_recv.at[distant], (kv, to))

    def emit():
        per_block = ntp // blocks
        for i in range(blocks):
            at = slice(i * BLK, (i + 1) * BLK)
            att[at, :] = mixed_ref[at, :].astype(jnp.bfloat16)
            for to in range(i * per_block, (i + 1) * per_block):

                opposite = (to // 2 - x + nx) % nx == nx // 2

                @pl.when((to != tp) & opposite)
                def _():
                    part_copy(to, 1).start()

                @pl.when((to != tp) & jnp.logical_not(opposite))
                def _():
                    part_copy(to, 0).start()

                @pl.when(to == tp)
                def _():
                    abuf[:, pl.ds(pl.multiple_of(tp * width, width), width)] = att[
                        to * rows : (to + 1) * rows, :
                    ]

        for head in range(heads):
            cols = slice(head * HEAD_DIM, (head + 1) * HEAD_DIM)
            lse_ref[head : head + 1, :] = jnp.concatenate(
                [
                    jnp.sum(
                        jnp.where(
                            eye[:BLK, :HEAD_DIM], wide_ref[i * BLK : (i + 1) * BLK, cols], 0.0
                        ),
                        axis=0,
                        keepdims=True,
                    )
                    for i in range(blocks)
                ],
                axis=1,
            )

    early = z <= 1

    @pl.when(early)
    def _():
        own_attention()
        emit()

    @pl.when(helper)
    def _():
        for c in range(ups - 1):

            @pl.when(z == c)
            def _():
                arrived(6 * plane_counts(c)[1], relay_recv.at[1])

        q_copy.wait_recv()
        help_log_out[...] = jnp.zeros(help_log_out.shape, jnp.float32)
        limit = (last_far + 1) * NY * blocks
        for i in range(blocks):
            result, column = attention(i, q_far, far_idx_ref, far_pool, mirror, 0, limit)
            help_out[i * BLK : (i + 1) * BLK, :] = result.astype(jnp.bfloat16)
            help_log_out[i : i + 1, :] = jnp.sum(jnp.where(eye, column, 0.0), axis=0, keepdims=True)
        o_copy.start()
        log_copy.start()

    pl.when(z > 1)(own_attention)

    @pl.when(helped)
    def _():
        o_copy.wait_recv()
        log_copy.wait_recv()
        for i in range(blocks):
            at = slice(i * BLK, (i + 1) * BLK)
            row = jnp.broadcast_to(help_log_in[i : i + 1, :], (heads * BLK, width))
            column = jnp.sum(jnp.where(eye, row, 0.0), axis=1, keepdims=True)
            theirs = by_head(jnp.broadcast_to(column, (heads * BLK, width)))
            mine = wide_ref[at, :]
            top = jnp.maximum(mine, theirs)
            share, other = jnp.exp(mine - top), jnp.exp(theirs - top)
            total = share + other
            extra = help_in[at, :].astype(jnp.float32)
            mixed_ref[at, :] = (mixed_ref[at, :] * share + extra * other) / total
            wide_ref[at, :] = top + jnp.log(total)

    pl.when(z > 1)(emit)

    for c in range(nz):

        @pl.when(z == c)
        def _():
            own, far, sent = plane_counts(c)
            left_off(8 * (own + far), y_send)
            if sent:
                left_off(sent, z_send)

    @pl.when(helper)
    def _():
        o_copy.wait_send()
        log_copy.wait_send()

    pl.when(helped)(lambda: q_copy.wait_send())
    w_arrived(4, w_recv.at[3])
    sent_w = wall.at[pl.ds(0, ntp - 1)]
    remote(sent_w, sent_w, w_send, w_recv.at[3], (kv, partner)).wait_send()
    def parts_of(count):
        return abuf.at[:, pl.ds(0, count * width)]

    total_width = out_ref.shape[1]
    chunk = min(512, total_width)

    def product(chip, cols):
        lhs = abuf[:, pl.ds(pl.multiple_of(chip * 2 * width, 2 * width), 2 * width)]
        rhs = wall[pl.ds(2 * chip, 2), :, cols].reshape(2 * width, chunk)
        return jnp.dot(lhs, rhs, preferred_element_type=jnp.float32)

    remote(parts_of(ntp - 3), parts_of(ntp - 3), a_send, a_recv.at[0], (kv, partner)).wait_recv()
    for c in range(total_width // chunk):
        cols = slice(c * chunk, (c + 1) * chunk)
        near_sum = product(x, cols) + product((x + 1) % nx, cols) + product((x + 3) % nx, cols)
        acc_ref[:, cols] = near_sum
    remote(parts_of(2), parts_of(2), a_send, a_recv.at[1], (kv, partner)).wait_recv()
    for c in range(total_width // chunk):
        cols = slice(c * chunk, (c + 1) * chunk)
        out_ref[:, cols] = (acc_ref[:, cols] + product((x + 2) % nx, cols)).astype(jnp.bfloat16)
    remote(parts_of(ntp - 1), parts_of(ntp - 1), a_send, a_recv.at[0], (kv, partner)).wait_send()


def finish(mixed_ref, log_ref, mixed_out, log_out, sem):
    first = pltpu.make_async_copy(mixed_ref, mixed_out, sem.at[0])
    second = pltpu.make_async_copy(log_ref, log_out, sem.at[1])
    first.start()
    second.start()
    first.wait()
    second.wait()


def local(nkv, ntp, tokens, w_query, w_key, w_value, w_out, chosen):
    local_rows = tokens.shape[0]
    width = w_query.shape[1]
    heads = width // HEAD_DIM
    blocks = local_rows // BLK
    nz = nkv // NY
    device = lax.axis_index("kv")
    vmem = pl.BlockSpec(memory_space=pltpu.VMEM)
    hbm = pl.BlockSpec(memory_space=pltpu.HBM)
    cos_piece, sin_piece = rotary_pieces(device * local_rows, width)
    ups = nz // 2
    out_rows = local_rows // ntp
    dma = pltpu.SemaphoreType.DMA
    stage = (nz + ups, 3, BLK, 2 * width)
    bf16, f32, i32 = jnp.bfloat16, jnp.float32, jnp.int32
    mixed, log_sums = pl.pallas_call(
        functools.partial(attend, nz, ntp),
        out_shape=(
            jax.ShapeDtypeStruct((out_rows, w_out.shape[1]), bf16),
            jax.ShapeDtypeStruct((heads, local_rows), f32),
        ),
        in_specs=[hbm] * 6 + [vmem] * 2,
        out_specs=(vmem, vmem),
        scratch_shapes=[
            pltpu.VMEM(tokens.shape, bf16),
            pltpu.VMEM(w_query.shape, bf16),
            pltpu.VMEM((w_key.shape[0], 2 * width), bf16),
            pltpu.VMEM((local_rows, width), bf16),
            pltpu.VMEM((local_rows, width), bf16),
            pltpu.VMEM((SEL, chosen.shape[0]), i32),
            pltpu.VMEM((chosen.shape[0], SEL), i32),
            pltpu.VMEM((local_rows, width), f32),
            pltpu.VMEM((local_rows, width), f32),
            pltpu.VMEM((4, nz, 128), i32),
            pltpu.SMEM((nz, 128), i32),
            pltpu.SMEM((8, 128), i32),
            pltpu.SMEM((nz, 128), i32),
            pltpu.SMEM((8, 128), i32),
            pltpu.VMEM((nz * blocks, BLK, 2 * width), bf16),
            pltpu.VMEM((nz * 8, BLK, 2 * width), bf16),
            pltpu.VMEM((ups * 8, BLK, 2 * width), bf16),
            pltpu.VMEM(stage, bf16),
            pltpu.VMEM(stage, bf16),
            pltpu.VMEM((blocks, SEL * BLK, 2 * width), bf16),
            pltpu.VMEM((ntp, width, w_out.shape[1]), bf16),
            pltpu.VMEM((local_rows, width), f32),
            pltpu.VMEM((local_rows, width), f32),
            pltpu.VMEM((local_rows, width), bf16),
            pltpu.VMEM((8, heads * BLK), f32),
            pltpu.VMEM((local_rows, width), bf16),
            pltpu.VMEM((8, heads * BLK), f32),
            pltpu.VMEM((local_rows, width), bf16),
            pltpu.VMEM((out_rows, ntp * width), bf16),
            pltpu.VMEM((out_rows, w_out.shape[1]), f32),
            dma((9,)),
            dma,
            dma((2 * blocks * ups,)),
            dma((2 * blocks * (ups - 2),)),
            dma,
            dma((ups + 1,)),
            dma((2 * ups - 2,)),
            dma((2,)),
            dma,
            dma((4,)),
            dma((3,)),
            dma((3,)),
            dma,
            dma((2,)),
        ],
        compiler_params=pltpu.CompilerParams(
            collective_id=0, has_side_effects=True, vmem_limit_bytes=55000 * 1024
        ),
    )(tokens, w_query, w_key, w_value, w_out, chosen.T, cos_piece, sin_piece)
    return pl.pallas_call(
        finish,
        out_shape=(
            jax.ShapeDtypeStruct(mixed.shape, mixed.dtype),
            jax.ShapeDtypeStruct(log_sums.shape, log_sums.dtype),
        ),
        in_specs=[vmem, vmem],
        out_specs=(hbm, hbm),
        scratch_shapes=[dma((2,))],
        compiler_params=pltpu.CompilerParams(vmem_limit_bytes=1024 * 1024),
    )(mixed, log_sums)


def solution(mesh):
    placed = (P("kv", None), P(None, "tp"), P(None, "tp"), P(None, "tp"), P("tp", None), P())
    return jax.shard_map(
        functools.partial(local, mesh.shape["kv"], mesh.shape["tp"]),
        mesh=mesh,
        in_specs=placed,
        out_specs=(P(("kv", "tp"), None), P("tp", "kv")),
        check_vma=False,
    )
```
